256 devices in a mesh: kv: 32 (over z, x), tp: 8 (over y, core).
Axes of the slice: x: 4, y: 4, z: 8, core: 2. Of those that a mesh axis runs over, the one named last changes fastest.
Arguments:
- tokens: bfloat16 [256, 12, 4096], P(None, None, 'kv'), may hold values from -6 to 6
- parents: int32 [256, 12], P('kv'), may hold values from -1 to 10, as said below
- accepted: int32 [256], P('kv'), may hold values from 0 to 6
- state: float32 [256, 64, 64, 128], P('kv', 'tp'), may hold values from -4 to 4
- conv_x: bfloat16 [256, 3, 4096], P('kv', None, 'tp'), may hold values from -6 to 6
- conv_b: bfloat16 [256, 3, 2048], P('kv', None, 'tp'), may hold values from -6 to 6
- conv_c: bfloat16 [256, 3, 2048], P('kv', None, 'tp'), may hold values from -6 to 6
- path_x: bfloat16 [256, 6, 4096], P('kv', None, 'tp'), may hold values from -6 to 6
- path_b: bfloat16 [256, 6, 2048], P('kv', None, 'tp'), may hold values from -6 to 6
- path_c: bfloat16 [256, 6, 2048], P('kv', None, 'tp'), may hold values from -6 to 6
- path_dt: bfloat16 [256, 6, 64], P('kv', None, 'tp'), may hold values from -6 to 6
- gain_in: float32 [4096], replicated, may hold values from 0.1 to 1.9
- w_x: bfloat16 [4096, 4096], P('kv', 'tp'), may hold values from -0.09375 to 0.09375
- w_z: bfloat16 [4096, 4096], P('kv', 'tp'), may hold values from -0.09375 to 0.09375
- w_b: bfloat16 [4096, 2048], P('kv', 'tp'), may hold values from -0.09375 to 0.09375
- w_c: bfloat16 [4096, 2048], P('kv', 'tp'), may hold values from -0.09375 to 0.09375
- w_dt: bfloat16 [4096, 64], replicated, may hold values from -0.09375 to 0.09375
- dt_bias: float32 [64], P('tp'), may hold values from -2 to 1
- a_log: float32 [64], P('tp'), may hold values from -3 to 1.5
- d_skip: float32 [64], P('tp'), may hold values from 0.5 to 1.5
- conv_wx: bfloat16 [4, 4096], P(None, 'tp'), may hold values from -3 to 3
- conv_wb: bfloat16 [4, 2048], P(None, 'tp'), may hold values from -3 to 3
- conv_wc: bfloat16 [4, 2048], P(None, 'tp'), may hold values from -3 to 3
- gain_out: float32 [4096], P('tp'), may hold values from 0.1 to 1.9
- w_out: bfloat16 [4096, 4096], P('tp', 'kv'), may hold values from -0.09375 to 0.09375
Outputs:
- mixed: bfloat16 [256, 12, 4096], P('kv', None, 'tp')
- new_state: float32 [256, 64, 64, 128], P('kv', 'tp')
The draws below stay inside these ranges and needn't reach their ends.
Inputs may be any that keep to these rules, and one draw needn't show every extreme that they name: `parents`: each proposal's parent is -1 or an earlier proposal of the same sequence; the first proposal's parent is -1.
All inputs are finite; a program needn't handle non-finite values.
Results may differ from the reference program's by a relative error of at most 0.03.
Values may be sent and summed in bfloat16 or wider, within the bound.
A program may use at most 128 MiB of HBM per device.

```python
import jax
import jax.numpy as jnp
from jax import lax

D = 4096
G = 16
HPG = 4
H = 64
HD = 64
N = 128
INNER = 4096
CONV = 4
Q = 12
P_SIZE = 6
SEQS = 256
N_TP = 8


def draw_parents(key, part):
    jumps = jax.random.randint(key, (SEQS, Q), 0, 3)
    places = jnp.arange(Q, dtype=jnp.int32)[None, :]
    return jnp.maximum(places - 1 - jumps, -1).astype(jnp.int32)


def touch_ends(array, key, low, largest):
    longest = array.shape.index(max(array.shape))
    spots = []
    for shift in (0, 1):
        where = [jax.random.randint(jax.random.fold_in(key, axis), (), 0, length) for axis, length in enumerate(array.shape)]
        where[longest] = (where[longest] + shift) % array.shape[longest]
        spots.append(tuple(where))
    return array.at[spots[0]].set(low).at[spots[1]].set(largest)


def raised(values, stream_key, source, target, shards_of, factor):
    def block_of(position):
        return (jnp.arange(values.shape[position]) // (values.shape[position] // shards_of)).reshape((-1,) + (1,) * (values.ndim - 1 - position))

    near = jax.random.permutation(stream_key, shards_of)[block_of(target)]
    second = (block_of(target) + shards_of // 2) % shards_of
    return jnp.where((block_of(source) == near) | (block_of(source) == second), factor * values, values)


def block_scale(key, extent, split, smallest, high):
    gain = 1.0
    for dim, blocks in split:
        steps = jax.random.uniform(jax.random.fold_in(jax.random.fold_in(key, 6), dim), (blocks,), jnp.float32, smallest / len(split), high / len(split))
        gain = gain * jnp.repeat(jnp.exp(steps), extent[dim] // blocks).reshape((-1,) + (1,) * (len(extent) - 1 - dim))
    return gain


def noise(rng, dims, spread, bound, shards=(), kind=jnp.bfloat16):
    array = jax.random.normal(rng, dims, jnp.float32) * spread
    if len(shards) > 0:
        array = block_scale(rng, dims, shards, -0.22, 0.18) * array
    return jnp.clip(array, min=-bound, max=bound).astype(kind)


def heavy_noise(own_key, shape, deviation, reach, shards, heavy, kind=jnp.bfloat16):
    array = deviation * jax.random.normal(own_key, shape, jnp.float32)
    if shards:
        array = array * block_scale(own_key, shape, shards, -0.22, 0.18)
    return jnp.clip(raised(array, jax.random.fold_in(own_key, 3), *heavy), -reach, reach).astype(kind)


def setup_inputs(seed: int = 0) -> dict:
    key_list = jax.random.split(jax.random.key(seed), 26)
    tokens = heavy_noise(key_list[0], (SEQS, Q, D), 1.0, 6.0, ((2, 32),), (2, 0, 32, 2.75))
    parents = draw_parents(jax.random.fold_in(key_list[25], 71), 0)
    accepted = touch_ends(jax.random.randint(key_list[2], (SEQS,), 0, P_SIZE + 1), jax.random.fold_in(key_list[2], 1), 0, P_SIZE).astype(jnp.int32)
    state = noise(key_list[3], (SEQS, H, HD, N), 0.3, 4.0, ((0, 32), (1, 8)), jnp.float32)
    conv_x = noise(key_list[4], (SEQS, CONV - 1, INNER), 1.0, 6.0, ((0, 32), (2, 8)))
    conv_b = noise(key_list[5], (SEQS, CONV - 1, G * N), 1.0, 6.0, ((0, 32), (2, 8)))
    conv_c = noise(key_list[6], (SEQS, CONV - 1, G * N), 1.0, 6.0, ((0, 32), (2, 8)))
    path_x = noise(key_list[7], (SEQS, P_SIZE, INNER), 1.0, 6.0, ((0, 32), (2, 8)))
    path_b = noise(key_list[8], (SEQS, P_SIZE, G * N), 1.0, 6.0, ((0, 32), (2, 8)))
    path_c = noise(key_list[9], (SEQS, P_SIZE, G * N), 1.0, 6.0, ((0, 32), (2, 8)))
    path_dt = noise(key_list[10], (SEQS, P_SIZE, H), 1.0, 6.0, ((0, 32), (2, 8)))
    gain_in = jnp.clip(1.0 + 0.18 * jax.random.normal(key_list[11], (D,), jnp.float32), 0.1, 1.9)
    w_x = noise(key_list[12], (D, INNER), D ** -0.5, 0.09375, ((0, 32), (1, 8)))
    w_z = noise(key_list[13], (D, INNER), D ** -0.5, 0.09375, ((0, 32), (1, 8)))
    w_b = noise(key_list[14], (D, G * N), D ** -0.5, 0.09375, ((0, 32), (1, 8)))
    w_c = noise(key_list[15], (D, G * N), D ** -0.5, 0.09375, ((0, 32), (1, 8)))
    w_dt = noise(key_list[16], (D, H), D ** -0.5, 0.09375)
    dt_bias = jnp.clip(-2.0 + 3.0 * jax.random.uniform(key_list[17], (H,), jnp.float32) ** block_scale(key_list[17], (H,), ((0, 8),), -0.2, 0.2), -2.0, 1.0)
    a_log = jnp.clip(-3.0 + 4.5 * jax.random.uniform(key_list[18], (H,), jnp.float32) ** block_scale(key_list[18], (H,), ((0, 8),), -0.2, 0.2), -3.0, 1.5)
    d_skip = jnp.clip(0.5 + 1.0 * jax.random.uniform(key_list[19], (H,), jnp.float32) ** block_scale(key_list[19], (H,), ((0, 8),), -0.2, 0.2), 0.5, 1.5)
    conv_wx = noise(key_list[20], (CONV, INNER), 0.5, 3.0, ((1, 8),))
    conv_wb = noise(key_list[21], (CONV, G * N), 0.5, 3.0, ((1, 8),))
    conv_wc = noise(key_list[22], (CONV, G * N), 0.5, 3.0, ((1, 8),))
    gain_out = jnp.clip(1.0 + 0.18 * jax.random.normal(key_list[23], (INNER,), jnp.float32), 0.1, 1.9)
    w_out = noise(key_list[24], (INNER, D), INNER ** -0.5, 0.09375, ((0, 8), (1, 32)))
    return dict(tokens=tokens, parents=parents, accepted=accepted, state=state, conv_x=conv_x, conv_b=conv_b, conv_c=conv_c, path_x=path_x, path_b=path_b, path_c=path_c, path_dt=path_dt, gain_in=gain_in, w_x=w_x, w_z=w_z, w_b=w_b, w_c=w_c, w_dt=w_dt, dt_bias=dt_bias, a_log=a_log, d_skip=d_skip, conv_wx=conv_wx, conv_wb=conv_wb, conv_wc=conv_wc, gain_out=gain_out, w_out=w_out)


EPS = 1e-06
HIGH = lax.Precision.HIGHEST

def conv_window(history, taps, amount):
    values = history.astype(jnp.float32)
    weights = taps.astype(jnp.float32)
    summed = weights[0] * values[:, 0:amount, :]
    for distance in range(1, weights.shape[0]):
        summed = summed + weights[distance] * values[:, distance:distance + amount, :]
    return jax.nn.silu(summed)

def commit_rows(history, accepted, keep):
    picked = accepted[:, None].astype(jnp.int32) + jnp.arange(keep, dtype=jnp.int32)[None, :]
    select = (picked[:, :, None] == jnp.arange(history.shape[1], dtype=jnp.int32)[None, None, :]).astype(jnp.float32)
    return jnp.einsum('skl,slc->skc', select, history.astype(jnp.float32), precision=HIGH).astype(jnp.bfloat16)

def replay_state(state, history_x, history_b, path_dt, conv_wx, conv_wb, accepted, rate_bias, a_rate, per_group):
    seq_count, heads, head_dim, state_dim = state.shape
    path_len = path_dt.shape[1]
    path_xs = conv_window(history_x, conv_wx, path_len).reshape(seq_count, path_len, heads, head_dim)
    path_bs = conv_window(history_b, conv_wb, path_len).reshape(seq_count, path_len, heads // per_group, state_dim)
    path_bh = jnp.repeat(path_bs, per_group, axis=2)
    path_step = jax.nn.softplus(path_dt.astype(jnp.float32) + rate_bias)
    is_live = (jnp.arange(path_len, dtype=jnp.int32)[None, :] < accepted[:, None].astype(jnp.int32)).astype(jnp.float32)[:, :, None]
    log_decay = path_step * a_rate * is_live
    overall = lax.optimization_barrier(jnp.sum(log_decay, axis=1))
    tail_sum = overall[:, None, :] - jnp.cumsum(log_decay, axis=1)
    weights = is_live * jnp.exp(tail_sum) * path_step
    grown = jnp.einsum('sjh,sjhp,sjhn->shpn', weights, path_xs, path_bh, precision=HIGH)
    return jnp.exp(overall)[:, :, None, None] * state + grown

def tree_links(parents, keep):
    seq_count, prop_count = parents.shape
    front = jnp.broadcast_to(jnp.arange(-1, keep - 1, dtype=jnp.int32)[None, :], (seq_count, keep))
    parent_ids = jnp.concatenate([front, parents.astype(jnp.int32) + keep], axis=1)
    nodes = keep + prop_count
    links = (parent_ids[:, :, None] == jnp.arange(nodes, dtype=jnp.int32)[None, None, :]).astype(jnp.float32)
    identity = jnp.eye(prop_count, dtype=jnp.float32)[None, :, :]
    ancestry = identity + links[:, keep:, keep:]
    for turn in range(prop_count.bit_length()):
        ancestry = jnp.minimum(jnp.einsum('sij,sjk->sik', ancestry, ancestry, precision=HIGH), 1.0)
    return (links, ancestry)

def tree_conv(buffer, rows, taps, links, keep):
    values = jnp.concatenate([buffer, rows], axis=1).astype(jnp.float32)
    weights = taps.astype(jnp.float32)
    last_tap = weights.shape[0] - 1
    summed = weights[last_tap] * values
    reached = values
    for distance in range(1, last_tap + 1):
        reached = jnp.einsum('sij,sjc->sic', links, reached, precision=HIGH)
        summed = summed + weights[last_tap - distance] * reached
    return jax.nn.silu(summed[:, keep:, :])

def tree_mix(state, post_x, post_b, post_c, rate_rows, z_rows, ancestry, rate_bias, a_rate, d_skip, gain_out, per_group):
    seq_count, prop_count, _ = post_x.shape
    heads, head_dim, state_dim = (state.shape[1], state.shape[2], state.shape[3])
    groups = heads // per_group
    x_heads = post_x.reshape(seq_count, prop_count, heads, head_dim)
    b_groups = post_b.reshape(seq_count, prop_count, groups, state_dim)
    c_groups = post_c.reshape(seq_count, prop_count, groups, state_dim)
    step_size = jax.nn.softplus(rate_rows.astype(jnp.float32) + rate_bias)
    path_decay = jnp.einsum('sij,sjh->sih', ancestry, step_size * a_rate, precision=HIGH)
    c_heads = jnp.repeat(c_groups, per_group, axis=2)
    carried = jnp.einsum('sihn,shpn->sihp', c_heads, state, precision=HIGH) * jnp.exp(path_decay)[:, :, :, None]
    scores = jnp.einsum('sign,sjgn->sgij', c_groups, b_groups, precision=HIGH)
    scores = jnp.repeat(scores, per_group, axis=1)
    decay_t = jnp.transpose(path_decay, (0, 2, 1))
    decay_gap = decay_t[:, :, :, None] - decay_t[:, :, None, :]
    is_live = ancestry[:, None, :, :] > 0.5
    mixing = jnp.where(is_live, jnp.exp(jnp.where(is_live, decay_gap, 0.0)), 0.0)
    mixing = mixing * jnp.transpose(step_size, (0, 2, 1))[:, :, None, :]
    within = jnp.einsum('shij,sjhp->sihp', scores * mixing, x_heads, precision=HIGH)
    heads_out = carried + within + d_skip[None, None, :, None] * x_heads
    heads_out = heads_out.reshape(seq_count, prop_count, heads * head_dim) * jax.nn.silu(z_rows.astype(jnp.float32))
    grouped = heads_out.reshape(seq_count, prop_count, groups, per_group * head_dim)
    grouped = grouped * lax.rsqrt(lax.optimization_barrier(jnp.mean(grouped * grouped, axis=-1, keepdims=True)) + EPS)
    return (grouped.reshape(seq_count, prop_count, heads * head_dim) * gain_out).astype(jnp.bfloat16)

def reference(tokens, parents, accepted, state, conv_x, conv_b, conv_c, path_x, path_b, path_c, path_dt, gain_in, w_x, w_z, w_b, w_c, w_dt, dt_bias, a_log, d_skip, conv_wx, conv_wb, conv_wc, gain_out, w_out):
    seq_count, prop_count, width = tokens.shape
    keep = conv_wx.shape[0] - 1
    flat_rows = tokens.reshape(-1, width).astype(jnp.float32)
    row_scale = lax.rsqrt(lax.optimization_barrier(jnp.sum(flat_rows * flat_rows, axis=1)) / width + EPS)[:, None]
    scaled = (flat_rows * gain_in).astype(jnp.bfloat16)

    def project(weight):
        product = jnp.dot(scaled, weight, preferred_element_type=jnp.float32) * row_scale
        return product.astype(jnp.bfloat16).reshape(seq_count, prop_count, -1)
    x_rows = project(w_x)
    z_rows = project(w_z)
    b_rows = project(w_b)
    c_rows = project(w_c)
    rate_rows = project(w_dt)
    a_rate = -jnp.exp(a_log)
    history_x = jnp.concatenate([conv_x, path_x], axis=1)
    history_b = jnp.concatenate([conv_b, path_b], axis=1)
    history_c = jnp.concatenate([conv_c, path_c], axis=1)
    new_state = replay_state(state, history_x, history_b, path_dt, conv_wx, conv_wb, accepted, dt_bias, a_rate, HPG)
    links, ancestry = tree_links(parents, keep)
    post_x = tree_conv(commit_rows(history_x, accepted, keep), x_rows, conv_wx, links, keep)
    post_b = tree_conv(commit_rows(history_b, accepted, keep), b_rows, conv_wb, links, keep)
    post_c = tree_conv(commit_rows(history_c, accepted, keep), c_rows, conv_wc, links, keep)
    gated = tree_mix(new_state, post_x, post_b, post_c, rate_rows, z_rows, ancestry, dt_bias, a_rate, d_skip, gain_out, HPG)
    block = gated.shape[2] // N_TP
    gated_flat = gated.reshape(-1, gated.shape[2])
    running = jnp.zeros((gated_flat.shape[0], width), jnp.float32)
    for index in range(N_TP):
        term = jnp.dot(gated_flat[:, index * block:(index + 1) * block], w_out[index * block:(index + 1) * block, :], preferred_element_type=jnp.float32)
        rounded = lax.optimization_barrier(term.astype(jnp.bfloat16))
        running = running + rounded.astype(jnp.float32)
    mixed = running.astype(jnp.bfloat16).reshape(seq_count, prop_count, width)
    return (mixed, new_state)
```

```python
import functools

import jax
import jax.numpy as jnp
from jax import lax
from jax.experimental import pallas as pl
from jax.experimental.pallas import tpu as pltpu
from jax.sharding import Mesh
from jax.sharding import PartitionSpec as P

NZ, NX, NY, NC = 8, 4, 4, 2
NT = NY * NC
MESH = pl.DeviceIdType.MESH
KV = ("z", "x")
TP = ("y", "c")
EPS = 1e-06
HIGH = lax.Precision.HIGHEST
F32 = jnp.float32
BF16 = jnp.bfloat16
NQ, NS, NP, NH = 12, 8, 6, 8
VMEM_LIMIT = 60 * 1024 * 1024


def wrap(i, n):
    return lax.rem(i + n, n)


def remote(src, dst, send_sem, recv_sem, device):
    return pltpu.make_async_remote_copy(
        src_ref=src,
        dst_ref=dst,
        send_sem=send_sem,
        recv_sem=recv_sem,
        device_id=device,
        device_id_type=MESH,
    )


def greet(devices):
    barrier = pltpu.get_barrier_semaphore()
    for device in devices:
        pl.semaphore_signal(barrier, inc=1, device_id=device, device_id_type=MESH)
    pl.semaphore_wait(barrier, len(devices))


def hops_of(piece, way):
    return 4 if (piece % 2 == 0) == (way == 0) else 3


def inproj_kernel(
    tok,
    wx,
    wz,
    wb,
    wc,
    wr,
    gain,
    wo,
    rows_out,
    aux_out,
    wog,
    tg,
    ts,
    wg,
    prod,
    aprod,
    ring,
    aring,
    stage,
    astage,
    t_s,
    t_r,
    f_s,
    f_r,
    w_s,
    w_r,
    r_s,
    r_r,
    o_s,
    o_r,
):
    z, x, c = lax.axis_index("z"), lax.axis_index("x"), lax.axis_index("c")
    greet(
        [{"x": wrap(x + d, NX)} for d in (1, 2, 3)]
        + [{"z": wrap(z + 1, NZ)}, {"z": wrap(z - 1, NZ)}, {"c": 1 - c}]
    )
    half = pl.ds(4 * c, 4)

    def tok_copy(d):
        to = wrap(x + d, NX)
        return remote(
            tok.at[:, half, to], tg.at[x, :, half], t_s.at[d - 1], t_r.at[d - 1], {"x": to}
        )

    def tok_share(d):
        block = tg.at[wrap(x - d, NX), :, half]
        return remote(block, block, f_s.at[d - 1], f_r.at[d - 1], {"c": 1 - c})

    pieces = [
        wx.at[:, 0:256],
        wx.at[:, 256:512],
        wz.at[:, 0:256],
        wz.at[:, 256:512],
        wb,
        wc,
    ]

    def depth_of(owner):
        return pl.ds(pl.multiple_of(owner * 128, 128), 128)

    def w_own(p, way):
        to = wrap(x + (1 if way == 0 else -1), NX)
        return remote(
            pieces[p], wg.at[p, depth_of(x), :], w_s.at[p, way], w_r.at[p, way], {"x": to}
        )

    def w_pass(p):
        sign = 1 if p % 2 == 0 else -1
        block = wg.at[p, depth_of(wrap(x - sign, NX)), :]
        return remote(block, block, w_s.at[p, 2], w_r.at[p, 2], {"x": wrap(x + sign, NX)})

    def o_copy(way, hop):
        sign = 1 if way == 0 else -1
        owner = wrap(z - sign * (hop - 1), NZ)
        src = wo if hop == 1 else wog.at[owner]
        dst = wog.at[owner]
        if hop == 4:
            src, dst = src.at[pl.ds(256 * way, 256)], dst.at[pl.ds(256 * way, 256)]
        return remote(
            src, dst, o_s.at[way, hop - 1], o_r.at[way, hop - 1], {"z": wrap(z + sign, NZ)}
        )

    def r_copy(p, way, hop):
        sign = 1 if way == 0 else -1
        to = {"z": wrap(z + sign, NZ)}
        if p == 6:
            src = astage.at[way] if hop == 1 else aring.at[way, hop - 2]
            dst = aring.at[way, hop - 1]
        else:
            src = stage.at[p, way] if hop == 1 else ring.at[p, way, hop - 2]
            dst = ring.at[p, way, hop - 1]
        return remote(src, dst, r_s.at[p, way, hop - 1], r_r.at[p, way, hop - 1], to)

    def own_term(p, dest):
        if p == 6:
            return aprod[:, pl.ds(dest, 1)].reshape(NQ, NS, 128)
        return prod[p, :, pl.ds(dest, 1)].reshape(NQ, NS, 256)

    def r_step(p, hop):
        for way in (0, 1):
            hops = hops_of(p, way)
            if hop > hops:
                continue
            sign = 1 if way == 0 else -1
            term = own_term(p, wrap(z + sign * (hops + 1 - hop), NZ))
            if hop == 1:
                if p == 6:
                    astage[way] = term.astype(BF16)
                else:
                    stage[p, way] = term.astype(BF16)
            else:
                r_copy(p, way, hop - 1).wait_recv()
                if p == 6:
                    aring[way, hop - 2] = (aring[way, hop - 2].astype(F32) + term).astype(BF16)
                else:
                    ring[p, way, hop - 2] = (ring[p, way, hop - 2].astype(F32) + term).astype(BF16)
            r_copy(p, way, hop).start()

    def r_total(p):
        total = own_term(p, z)
        for way in (0, 1):
            hops = hops_of(p, way)
            r_copy(p, way, hops).wait_recv()
            arrived = aring[way, hops - 1] if p == 6 else ring[p, way, hops - 1]
            total = total + arrived.astype(F32)
        return total.reshape(NQ * NS, total.shape[2])

    order = (1, 3, 2)
    for d in order:
        tok_copy(d).start()
    for p in range(6):
        first = p % 2
        w_own(p, first).start()
        w_own(p, 1 - first).start()
    for way in (0, 1):
        o_copy(way, 1).start()
    tg[pl.ds(x, 1)] = tok[:, :, pl.ds(x, 1)].reshape(1, NQ, NZ, NS, 128)
    for p in range(6):
        wg[p, depth_of(x), :] = pieces[p][...]
    wog[pl.ds(z, 1)] = wo[...].reshape(1, 512, 128)
    for d in order:
        tok_copy(d).wait_recv()
        tok_share(d).start()
    for way in (0, 1):
        o_copy(way, 1).wait_recv()
        o_copy(way, 2).start()
    for d in order:
        tok_share(d).wait_recv()

    squares = jnp.zeros((NQ * NZ * NS, 128), F32)
    for xs in range(NX):
        values = tg[xs].reshape(NQ * NZ * NS, 128).astype(F32)
        squares = squares + values * values
        ts[:, xs * 128 : (xs + 1) * 128] = (values * gain[pl.ds(z * NX + xs, 1), :]).astype(BF16)
    lane = lax.broadcasted_iota(jnp.int32, (NQ * NZ * NS, 128), 1)
    rates = lax.dot_general(
        ts[...], wr[...], (((1,), (1,)), ((), ())), preferred_element_type=F32
    )
    sums = jnp.sum(squares, axis=1, keepdims=True)
    aprod[...] = jnp.where(lane == 8, sums, rates).reshape(NQ, NZ, NS, 128)
    r_step(6, 1)

    def forward(ch):
        for p in (2 * ch, 2 * ch + 1):
            w_own(p, p % 2).wait_recv()
            w_pass(p).start()

    def multiply(ch):
        for p in (2 * ch, 2 * ch + 1):
            w_own(p, 1 - p % 2).wait_recv()
            w_pass(p).wait_recv()
            prod[p] = jnp.dot(ts[...], wg[p], preferred_element_type=F32).reshape(
                NQ, NZ, NS, 256
            )
            r_step(p, 1)

    def advance(ch, hop):
        for p in (2 * ch, 2 * ch + 1):
            r_step(p, hop)

    forward(0)
    forward(1)
    multiply(0)
    for way in (0, 1):
        o_copy(way, 2).wait_recv()
        o_copy(way, 3).start()
    r_step(6, 2)
    advance(0, 2)
    forward(2)
    multiply(1)
    for way in (0, 1):
        o_copy(way, 3).wait_recv()
        o_copy(way, 4).start()
    r_step(6, 3)
    advance(0, 3)
    advance(1, 2)
    multiply(2)
    r_step(6, 4)
    advance(0, 4)
    advance(1, 3)
    advance(2, 2)
    advance(1, 4)
    advance(2, 3)
    advance(2, 4)

    total = r_total(6)
    scale = lax.rsqrt(total[:, 8:9] / (NZ * NX * 128.0) + EPS)
    aux_out[...] = (total * scale).astype(BF16).astype(F32)
    for p in range(6):
        rows_out[:, p * 256 : (p + 1) * 256] = (r_total(p) * scale).astype(BF16)

    for way in (0, 1):
        o_copy(way, 4).wait_recv()
        for hop in (1, 2, 3, 4):
            o_copy(way, hop).wait_send()
    for d in order:
        tok_copy(d).wait_send()
        tok_share(d).wait_send()
    for p in range(6):
        w_own(p, 0).wait_send()
        w_own(p, 1).wait_send()
        w_pass(p).wait_send()
    for p in range(7):
        for way in (0, 1):
            for hop in range(1, hops_of(p, way) + 1):
                r_copy(p, way, hop).wait_send()


def inproj(tok, wx, wz, wb, wc, wr, gain, wo):
    vmem = pl.BlockSpec(memory_space=pltpu.VMEM)
    dma = pltpu.SemaphoreType.DMA
    return pl.pallas_call(
        inproj_kernel,
        name="inproj",
        out_shape=(
            jax.ShapeDtypeStruct((NQ * NS, 1536), BF16),
            jax.ShapeDtypeStruct((NQ * NS, 128), F32),
            jax.ShapeDtypeStruct((NZ, 512, 128), BF16),
        ),
        in_specs=[vmem] * 8,
        out_specs=(vmem, vmem, vmem),
        scratch_shapes=[
            pltpu.VMEM((NX, NQ, NZ, NS, 128), BF16),
            pltpu.VMEM((NQ * NZ * NS, 512), BF16),
            pltpu.VMEM((6, 512, 256), BF16),
            pltpu.VMEM((6, NQ, NZ, NS, 256), F32),
            pltpu.VMEM((NQ, NZ, NS, 128), F32),
            pltpu.VMEM((6, 2, 4, NQ, NS, 256), BF16),
            pltpu.VMEM((2, 4, NQ, NS, 128), BF16),
            pltpu.VMEM((6, 2, NQ, NS, 256), BF16),
            pltpu.VMEM((2, NQ, NS, 128), BF16),
            dma((3,)),
            dma((3,)),
            dma((3,)),
            dma((3,)),
            dma((6, 3)),
            dma((6, 3)),
            dma((7, 2, 4)),
            dma((7, 2, 4)),
            dma((2, 4)),
            dma((2, 4)),
        ],
        compiler_params=pltpu.CompilerParams(
            collective_id=0, has_side_effects=True, vmem_limit_bytes=VMEM_LIMIT
        ),
    )(tok, wx, wz, wb, wc, wr, gain, wo)


def silu(v):
    return v * (1.0 / (1.0 + jnp.exp(-v)))


def softplus(v):
    return jnp.maximum(v, 0.0) + jnp.log1p(jnp.exp(-jnp.abs(v)))


def mix_kernel(
    idx,
    rows,
    aux,
    cx,
    px,
    cb,
    pb,
    cc,
    pc,
    pdt,
    state,
    bias,
    alog,
    dskip,
    wtx,
    wtb,
    wtc,
    gain,
    gated,
    new_state,
):
    count = NQ * NS

    def iota(shape, dim):
        return lax.broadcasted_iota(jnp.int32, shape, dim)

    def dot(a, b):
        return jnp.dot(a.astype(BF16), b.astype(BF16), preferred_element_type=F32)

    def dot_of(a, b, dims, precision=None):
        return lax.dot_general(
            a, b, ((dims[:1], dims[1:]), ((), ())), precision=precision, preferred_element_type=F32
        )

    def past(first, last):
        return jnp.concatenate([first[...].astype(F32), last[...].astype(F32)], axis=0)

    spread = (iota((NH, 512), 1) // 64 == iota((NH, 512), 0)).astype(F32)

    def widen(v):
        return dot_of(v, spread, (1, 0), HIGH)

    rate = -jnp.exp(alog[...])
    hist_x, hist_b, hist_c = past(cx, px), past(cb, pb), past(cc, pc)
    tx, tb, tc = wtx[...].astype(F32), wtb[...].astype(F32), wtc[...].astype(F32)

    def window(history, taps):
        summed = taps[0:1] * history[0 : NP * NS]
        for k in (1, 2, 3):
            summed = summed + taps[k : k + 1] * history[k * NS : (k + NP) * NS]
        return silu(summed)

    path_xs, path_bs = window(hist_x, tx), window(hist_b, tb)
    path_step = softplus(pdt[...].astype(F32) + bias[...])
    live = (iota((NP * NS, 1), 0) // NS < idx[0 : NP * NS, 4:5]).astype(F32)
    path_log = path_step * rate * live
    tails = [jnp.zeros((NS, NH), F32)]
    for j in range(NP - 1, 0, -1):
        tails.insert(0, tails[0] + path_log[j * NS : (j + 1) * NS])
    overall = jnp.exp(tails[0] + path_log[0:NS])
    weights = live * jnp.exp(jnp.concatenate(tails, axis=0)) * path_step
    weighted = (path_xs * widen(weights)).astype(BF16)

    step = softplus(aux[:, 0:NH] + bias[...])
    slope = step * rate
    links = (iota((count, count), 1) == idx[:, 3:4]).astype(F32)
    eye = (iota((count, count), 0) == iota((count, count), 1)).astype(F32)
    family = eye + links
    for _ in range(4):
        family = jnp.minimum(dot(family, family), 1.0)
    is_kin = family > 0.5
    nodes = iota((count, 9 * NS + count), 1)
    one = (nodes == idx[:, 0:1]).astype(F32)
    two = dot(links, one) + (nodes == idx[:, 1:2]).astype(F32)
    three = dot(links, two) + (nodes == idx[:, 2:3]).astype(F32)
    one, two, three = one.astype(BF16), two.astype(BF16), three.astype(BF16)

    def tree_conv(history, own, taps):
        own = own.astype(F32)
        values = jnp.concatenate([history, own], axis=0).astype(BF16)
        summed = taps[3:4] * own
        for k, reach in ((2, one), (1, two), (0, three)):
            summed = summed + taps[k : k + 1] * dot(reach, values)
        return silu(summed)

    post_x = tree_conv(hist_x, rows[:, 0:512], tx)
    post_b = tree_conv(hist_b, rows[:, 1024:1280], tb).astype(BF16)
    post_c = tree_conv(hist_c, rows[:, 1280:1536], tc).astype(BF16)

    decay = dot_of(family, slope, (1, 0), HIGH)
    decay_t = dot_of(slope, family, (0, 1), HIGH)
    step_t = dot_of(step, eye, (0, 1), HIGH)
    grown = widen(jnp.exp(decay))
    skip = widen(jnp.broadcast_to(dskip[...], (NS, NH)))[0:1]
    post_xb = post_x.astype(BF16)
    seq_of = lax.rem(iota((count, 128), 0), NS)
    path_seq = lax.rem(iota((NP * NS, 128), 0), NS)
    lane = iota((count, 128), 1)

    for g in range(2):
        wide, narrow = slice(256 * g, 256 * g + 256), slice(128 * g, 128 * g + 128)
        post_bg, post_cg = post_b[:, narrow], post_c[:, narrow]
        split_b = jnp.concatenate(
            [jnp.where(path_seq == s, path_bs[:, narrow], 0.0) for s in range(NS)], axis=1
        ).astype(BF16)
        gained = dot_of(weighted[:, wide], split_b, (0, 0))
        carried = jnp.zeros((count, 256), F32)
        for s in range(NS):
            fade = jnp.concatenate(
                [
                    jnp.broadcast_to(overall[s : s + 1, h : h + 1], (64, 128))
                    for h in range(4 * g, 4 * g + 4)
                ],
                axis=0,
            )
            fresh = fade * state[s, wide, :] + gained[:, 128 * s : 128 * s + 128]
            new_state[s, wide, :] = fresh
            mine = jnp.where(seq_of == s, post_cg.astype(F32), 0.0).astype(BF16)
            carried = carried + dot_of(mine, fresh.astype(BF16), (1, 1))
        scores = dot_of(post_cg, post_bg, (1, 1))
        within = []
        for pair in range(2):
            sides = []
            for h in (4 * g + 2 * pair, 4 * g + 2 * pair + 1):
                gap = decay[:, h : h + 1] - decay_t[h : h + 1, :]
                mixing = jnp.exp(jnp.where(is_kin, gap, 0.0)) * step_t[h : h + 1, :]
                mixing = jnp.where(is_kin, scores * mixing, 0.0)
                at = 256 * g + 128 * pair
                sides.append(dot(mixing, post_xb[:, at : at + 128]))
            within.append(jnp.where(lane < 64, sides[0], sides[1]))
        heads = carried * grown[:, wide] + jnp.concatenate(within, axis=1)
        heads = heads + skip[:, wide] * post_x[:, wide]
        heads = heads * silu(rows[:, 512 + 256 * g : 768 + 256 * g].astype(F32))
        spread_of = jnp.sum(heads * heads, axis=1, keepdims=True) / 256.0
        heads = heads * lax.rsqrt(spread_of + EPS) * gain[:, wide]
        gated[:, wide] = heads.astype(BF16)


def mix(*args):
    vmem = pl.BlockSpec(memory_space=pltpu.VMEM)
    return pl.pallas_call(
        mix_kernel,
        name="mix",
        out_shape=(
            jax.ShapeDtypeStruct((NQ * NS, 512), BF16),
            jax.ShapeDtypeStruct((NS, 512, 128), F32),
        ),
        in_specs=[vmem] * len(args),
        out_specs=(vmem, vmem),
        compiler_params=pltpu.CompilerParams(vmem_limit_bytes=VMEM_LIMIT),
    )(*args)


def outproj_kernel(gated, wog, mixed, gg, woc, part, terms, g_s, g_r, p_s, p_r):
    x, y, c = lax.axis_index("x"), lax.axis_index("y"), lax.axis_index("c")
    t = y * NC + c

    def place(xs, tt):
        return {"x": xs, "y": tt // NC, "c": lax.rem(tt, NC)}

    greet(
        [
            place(wrap(x + d, NX), wrap(t + e, NT))
            for d in range(NX)
            for e in range(NT)
            if d + e > 0
        ]
    )

    def g_copy(d):
        return remote(
            gated, gg.at[d - 1], g_s.at[d - 1], g_r.at[d - 1], {"x": wrap(x + d, NX)}
        )

    def p_copy(d, e):
        tt = wrap(t + e, NT)
        return remote(
            part.at[d, tt],
            terms.at[x * NT + t],
            p_s.at[d, e],
            p_r.at[d, e],
            place(wrap(x - d, NX), tt),
        )

    order = (1, 3, 2)
    for d in order:
        g_copy(d).start()
    for k in range(NZ):
        woc[:, k * 128 : (k + 1) * 128] = wog[k]
    for d in (0,) + order:
        if d > 0:
            g_copy(d).wait_recv()
        values = gated[...] if d == 0 else gg[d - 1]
        for pair in range(4):
            cols = slice(256 * pair, 256 * pair + 256)
            product = jnp.dot(values, woc[:, cols], preferred_element_type=F32).astype(BF16)
            part[d, 2 * pair] = product[:, 0:128]
            part[d, 2 * pair + 1] = product[:, 128:256]
        for e in range(NT):
            if d + e > 0:
                p_copy(d, e).start()
    terms[pl.ds(x * NT + t, 1)] = part[0, pl.ds(t, 1)]
    for d in (0,) + order:
        for e in range(NT):
            if d + e > 0:
                p_copy(d, e).wait_recv()
    for xs in range(NX):
        total = terms[xs * NT].astype(F32)
        for k in range(1, NT):
            total = total + terms[xs * NT + k].astype(F32)
        mixed[:, xs * 128 : (xs + 1) * 128] = total.astype(BF16)
    for d in range(NX):
        if d > 0:
            g_copy(d).wait_send()
        for e in range(NT):
            if d + e > 0:
                p_copy(d, e).wait_send()


def outproj(gated, wog):
    vmem = pl.BlockSpec(memory_space=pltpu.VMEM)
    dma = pltpu.SemaphoreType.DMA
    return pl.pallas_call(
        outproj_kernel,
        name="outproj",
        out_shape=jax.ShapeDtypeStruct((NQ * NS, 512), BF16),
        in_specs=[vmem, vmem],
        out_specs=vmem,
        scratch_shapes=[
            pltpu.VMEM((3, NQ * NS, 512), BF16),
            pltpu.VMEM((512, 1024), BF16),
            pltpu.VMEM((NX, NT, NQ * NS, 128), BF16),
            pltpu.VMEM((NX * NT, NQ * NS, 128), BF16),
            dma((3,)),
            dma((3,)),
            dma((NX, NT)),
            dma((NX, NT)),
        ],
        compiler_params=pltpu.CompilerParams(
            collective_id=1, has_side_effects=True, vmem_limit_bytes=VMEM_LIMIT
        ),
    )(gated, wog)


def by_place(v):
    v = jnp.transpose(v, (1, 0, 2))
    return v.reshape(v.shape[0] * v.shape[1], v.shape[2])


def shards(
    tokens,
    parents,
    accepted,
    state,
    conv_x,
    conv_b,
    conv_c,
    path_x,
    path_b,
    path_c,
    path_dt,
    gain_in,
    w_x,
    w_z,
    w_b,
    w_c,
    w_dt,
    dt_bias,
    a_log,
    d_skip,
    conv_wx,
    conv_wb,
    conv_wc,
    gain_out,
    w_out,
):
    z = lax.axis_index("z")
    t = lax.axis_index("y") * NC + lax.axis_index("c")
    tok = jnp.transpose(tokens, (1, 0, 2)).reshape(NQ, NZ, NX, NS, 128)
    wr = lax.dynamic_slice(w_dt.T, (t * NH, z * 512), (NH, 512))
    wr = jnp.pad(wr, ((0, 128 - NH), (0, 0)))
    rows, aux, wog = inproj(tok, w_x, w_z, w_b, w_c, wr, gain_in.reshape(32, 128), w_out)

    up = parents.T
    seq = jnp.arange(NS, dtype=jnp.int32)[None, :]
    acc = accepted[None, :]
    root = up < 0
    idx = jnp.stack(
        [
            jnp.where(root, (acc + 2) * NS + seq, 9 * NS + up * NS + seq),
            jnp.where(root, (acc + 1) * NS + seq, -1),
            jnp.where(root, acc * NS + seq, -1),
            jnp.where(root, -1, up * NS + seq),
            jnp.broadcast_to(acc, up.shape),
        ],
        axis=-1,
    ).reshape(NQ * NS, 5)
    gated, new_state = mix(
        idx,
        rows,
        aux,
        by_place(conv_x),
        by_place(path_x),
        by_place(conv_b),
        by_place(path_b),
        by_place(conv_c),
        by_place(path_c),
        by_place(path_dt),
        state.reshape(NS, 512, 128),
        dt_bias[None, :],
        a_log[None, :],
        d_skip[None, :],
        conv_wx,
        conv_wb,
        conv_wc,
        gain_out[None, :],
    )
    mixed = outproj(gated, wog)
    mixed = jnp.transpose(mixed.reshape(NQ, NS, 512), (1, 0, 2))
    return (mixed, new_state.reshape(NS, NH, 64, 128))


def solution(mesh):
    finer = Mesh(mesh.devices.reshape(NZ, NX, NY, NC), ("z", "x", "y", "c"))
    return jax.shard_map(
        shards,
        mesh=finer,
        in_specs=(
            P(None, None, KV),
            P(KV, None),
            P(KV),
            P(KV, TP, None, None),
            P(KV, None, TP),
            P(KV, None, TP),
            P(KV, None, TP),
            P(KV, None, TP),
            P(KV, None, TP),
            P(KV, None, TP),
            P(KV, None, TP),
            P(),
            P(KV, TP),
            P(KV, TP),
            P(KV, TP),
            P(KV, TP),
            P(),
            P(TP),
            P(TP),
            P(TP),
            P(None, TP),
            P(None, TP),
            P(None, TP),
            P(TP),
            P(TP, KV),
        ),
        out_specs=(P(KV, None, TP), P(KV, TP, None, None)),
        check_vma=False,
    )
```

```python
import functools

import jax
import jax.numpy as jnp
from jax import lax
from jax.experimental import pallas as pl
from jax.experimental.pallas import tpu as pltpu
from jax.sharding import Mesh
from jax.sharding import PartitionSpec as P

NZ, NX, NY, NC = 8, 4, 4, 2
NT = NY * NC
MESH = pl.DeviceIdType.MESH
KV = ("z", "x")
TP = ("y", "c")
EPS = 1e-06
HIGH = lax.Precision.HIGHEST
F32 = jnp.float32
BF16 = jnp.bfloat16
NQ, NS, NP, NH = 12, 8, 6, 8
VMEM_LIMIT = 60 * 1024 * 1024


def wrap(i, n):
    return lax.rem(i + n, n)


def remote(src, dst, send_sem, recv_sem, device):
    return pltpu.make_async_remote_copy(
        src_ref=src,
        dst_ref=dst,
        send_sem=send_sem,
        recv_sem=recv_sem,
        device_id=device,
        device_id_type=MESH,
    )


def greet(devices):
    barrier = pltpu.get_barrier_semaphore()
    for device in devices:
        pl.semaphore_signal(barrier, inc=1, device_id=device, device_id_type=MESH)
    pl.semaphore_wait(barrier, len(devices))


def hops_of(piece, way):
    return 4 if (piece % 2 == 0) == (way == 0) else 3


def silu(v):
    return v * (1.0 / (1.0 + jnp.exp(-v)))


def softplus(v):
    return jnp.maximum(v, 0.0) + jnp.log1p(jnp.exp(-jnp.abs(v)))


def iota(shape, dim):
    return lax.broadcasted_iota(jnp.int32, shape, dim)


def dot(a, b):
    return jnp.dot(a.astype(BF16), b.astype(BF16), preferred_element_type=F32)


def dot_of(a, b, dims, precision=None):
    return lax.dot_general(
        a, b, ((dims[:1], dims[1:]), ((), ())), precision=precision, preferred_element_type=F32
    )


def past(first, last):
    return jnp.concatenate([first[...].astype(F32), last[...].astype(F32)], axis=0)


def widen(v):
    spread = (iota((NH, 512), 1) // 64 == iota((NH, 512), 0)).astype(F32)
    return dot_of(v, spread, (1, 0), HIGH)


def upright(row):
    wide = jnp.broadcast_to(row[...].astype(F32), (NS, NS))
    return jnp.sum(
        jnp.where(iota((NS, NS), 0) == iota((NS, NS), 1), wide, 0.0), axis=1, keepdims=True
    )


def replay_kernel(
    accepted, cx, px, cb, pb, pdt, state, bias, alog, wtx, wtb, new_state, fresh_b, held, in_s, out_s
):
    def load(s):
        return pltpu.make_async_copy(state.at[s], held.at[s], in_s.at[s])

    def save(s):
        return pltpu.make_async_copy(held.at[s], new_state.at[s], out_s.at[s])

    for s in range(NS):
        load(s).start()

    def window(history, taps):
        summed = taps[0:1] * history[0 : NP * NS]
        for k in (1, 2, 3):
            summed = summed + taps[k : k + 1] * history[k * NS : (k + NP) * NS]
        return silu(summed)

    rate = -jnp.exp(alog[...])
    path_xs = window(past(cx, px), wtx[...].astype(F32))
    path_bs = window(past(cb, pb), wtb[...].astype(F32))
    path_step = softplus(pdt[...].astype(F32) + bias[...])
    count = jnp.concatenate([upright(accepted)] * NP, axis=0)
    live = ((iota((NP * NS, 1), 0) // NS).astype(F32) < count).astype(F32)
    path_log = path_step * rate * live
    tails = [jnp.zeros((NS, NH), F32)]
    for j in range(NP - 1, 0, -1):
        tails.insert(0, tails[0] + path_log[j * NS : (j + 1) * NS])
    overall = jnp.exp(tails[0] + path_log[0:NS])
    weights = live * jnp.exp(jnp.concatenate(tails, axis=0)) * path_step
    weighted = (path_xs * widen(weights)).astype(BF16)
    path_seq = lax.rem(iota((NP * NS, 128), 0), NS)
    gained = []
    for g in range(2):
        split_b = jnp.concatenate(
            [
                jnp.where(path_seq == s, path_bs[:, 128 * g : 128 * g + 128], 0.0)
                for s in range(NS)
            ],
            axis=1,
        ).astype(BF16)
        gained.append(dot_of(weighted[:, 256 * g : 256 * g + 256], split_b, (0, 0)))
    for s in range(NS):
        load(s).wait()
        at = slice(128 * s, 128 * s + 128)
        for g in range(2):
            wide = slice(256 * g, 256 * g + 256)
            fade = jnp.concatenate(
                [
                    jnp.broadcast_to(overall[s : s + 1, h : h + 1], (64, 128))
                    for h in range(4 * g, 4 * g + 4)
                ],
                axis=0,
            )
            fresh = fade * held[s, wide, :] + gained[g][:, at]
            held[s, wide, :] = fresh
            fresh_b[g, :, at] = fresh.astype(BF16)
        save(s).start()
    for s in range(NS):
        save(s).wait()


def replay(*args):
    vmem = pl.BlockSpec(memory_space=pltpu.VMEM)
    far = pl.BlockSpec(memory_space=pl.ANY)
    return pl.pallas_call(
        replay_kernel,
        name="replay",
        out_shape=(
            jax.ShapeDtypeStruct((NS, 512, 128), F32),
            jax.ShapeDtypeStruct((2, 256, 1024), BF16),
        ),
        in_specs=[vmem] * 6 + [far] + [vmem] * 4,
        out_specs=(far, vmem),
        scratch_shapes=[
            pltpu.VMEM((NS, 512, 128), F32),
            pltpu.SemaphoreType.DMA((NS,)),
            pltpu.SemaphoreType.DMA((NS,)),
        ],
        compiler_params=pltpu.CompilerParams(vmem_limit_bytes=VMEM_LIMIT),
    )(*args)


def mixer_kernel(
    tok_h,
    wx_h,
    wz_h,
    wb_h,
    wc_h,
    wdt_h,
    wo_h,
    fresh_h,
    gain,
    parents,
    accepted,
    cx,
    px,
    cb,
    pb,
    cc,
    pc,
    bias,
    alog,
    dskip,
    wtx,
    wtb,
    wtc,
    gain_out,
    mixed,
    tok,
    wown,
    wr,
    wo,
    fresh,
    tg,
    ts,
    wg,
    wog,
    prod,
    aprod,
    ring,
    aring,
    stage,
    astage,
    gated,
    gg,
    woc,
    kept,
    given,
    taken,
    part,
    terms,
    l_s,
    t_s,
    t_r,
    f_s,
    f_r,
    w_s,
    w_r,
    r_s,
    r_r,
    o_s,
    o_r,
    g_s,
    g_r,
    d_s,
    d_r,
    p_s,
    p_r,
):
    z, x = lax.axis_index("z"), lax.axis_index("x")
    y, c = lax.axis_index("y"), lax.axis_index("c")
    t = y * NC + c
    count = NQ * NS

    def depth_of(owner):
        return pl.ds(pl.multiple_of(owner * 128, 128), 128)

    sources = [
        wx_h.at[:, 0:256],
        wx_h.at[:, 256:512],
        wb_h,
        wc_h,
        wz_h.at[:, 0:256],
        wz_h.at[:, 256:512],
    ]
    loads = [(tok_h, tok)] + [(sources[p], wown.at[p]) for p in range(6)]
    loads.append((wo_h, wo))
    loads.append(
        (
            wdt_h.at[
                pl.ds(pl.multiple_of(t * NH, NH), NH), pl.ds(pl.multiple_of(z * 512, 512), 512)
            ],
            wr,
        )
    )
    loads.append((fresh_h, fresh))

    def load(k):
        return pltpu.make_async_copy(loads[k][0], loads[k][1], l_s.at[k])

    for k in range(len(loads)):
        load(k).start()
    plane = [(d, e) for d in range(NX) for e in range(NY) if d + e > 0]
    greet(
        [{"x": wrap(x + d, NX), "y": wrap(y + e, NY)} for d, e in plane]
        + [{"z": wrap(z + 1, NZ)}, {"z": wrap(z - 1, NZ)}, {"c": 1 - c}]
    )
    half = pl.ds(4 * c, 4)

    def tok_copy(d):
        to = wrap(x + d, NX)
        return remote(
            tok.at[:, half, to], tg.at[x, :, half], t_s.at[d - 1], t_r.at[d - 1], {"x": to}
        )

    def tok_share(d):
        block = tg.at[wrap(x - d, NX), :, half]
        return remote(block, block, f_s.at[d - 1], f_r.at[d - 1], {"c": 1 - c})

    def w_own(p, way):
        to = wrap(x + (1 if way == 0 else -1), NX)
        return remote(
            wown.at[p], wg.at[p, depth_of(x), :], w_s.at[p, way], w_r.at[p, way], {"x": to}
        )

    def w_pass(p):
        sign = 1 if p % 2 == 0 else -1
        block = wg.at[p, depth_of(wrap(x - sign, NX)), :]
        return remote(block, block, w_s.at[p, 2], w_r.at[p, 2], {"x": wrap(x + sign, NX)})

    def o_copy(way, hop):
        sign = 1 if way == 0 else -1
        owner = wrap(z - sign * (hop - 1), NZ)
        src = wo if hop == 1 else wog.at[owner]
        dst = wog.at[owner]
        if hop == 4:
            src, dst = src.at[pl.ds(256 * way, 256)], dst.at[pl.ds(256 * way, 256)]
        return remote(
            src, dst, o_s.at[way, hop - 1], o_r.at[way, hop - 1], {"z": wrap(z + sign, NZ)}
        )

    def r_copy(p, way, hop):
        to = {"z": wrap(z + (1 if way == 0 else -1), NZ)}
        if p == 6:
            src = astage.at[way] if hop == 1 else aring.at[way, hop - 2]
            dst = aring.at[way, hop - 1]
        else:
            src = stage.at[p, way] if hop == 1 else ring.at[p, way, hop - 2]
            dst = ring.at[p, way, hop - 1]
        return remote(src, dst, r_s.at[p, way, hop - 1], r_r.at[p, way, hop - 1], to)

    def own_term(p, dest):
        if p == 6:
            return aprod[:, pl.ds(dest, 1)].reshape(NQ, NS, 128)
        return prod[p, :, pl.ds(dest, 1)].reshape(NQ, NS, 256)

    def r_step(p, hop):
        for way in (0, 1):
            hops = hops_of(p, way)
            if hop > hops:
                continue
            sign = 1 if way == 0 else -1
            term = own_term(p, wrap(z + sign * (hops + 1 - hop), NZ))
            if hop == 1:
                if p == 6:
                    astage[way] = term.astype(BF16)
                else:
                    stage[p, way] = term.astype(BF16)
            else:
                r_copy(p, way, hop - 1).wait_recv()
                if p == 6:
                    aring[way, hop - 2] = (aring[way, hop - 2].astype(F32) + term).astype(BF16)
                else:
                    ring[p, way, hop - 2] = (ring[p, way, hop - 2].astype(F32) + term).astype(BF16)
            r_copy(p, way, hop).start()

    def r_total(p):
        total = own_term(p, z)
        for way in (0, 1):
            hops = hops_of(p, way)
            r_copy(p, way, hops).wait_recv()
            arrived = aring[way, hops - 1] if p == 6 else ring[p, way, hops - 1]
            total = total + arrived.astype(F32)
        return total.reshape(count, total.shape[2])

    order = (2, 1, 3)
    load(0).wait()
    for d in order:
        tok_copy(d).start()

    def w_send(ch):
        for p in (2 * ch, 2 * ch + 1):
            load(1 + p).wait()
            w_own(p, p % 2).start()
            w_own(p, 1 - p % 2).start()

    def o_send(hop):
        for way in (0, 1):
            if hop > 1:
                o_copy(way, hop - 1).wait_recv()
            o_copy(way, hop).start()

    w_send(0)
    w_send(1)
    load(7).wait()
    o_send(1)
    load(6).wait()
    load(5).wait()
    load(8).wait()
    load(9).wait()
    tg[pl.ds(x, 1)] = tok[:, :, pl.ds(x, 1)].reshape(1, NQ, NZ, NS, 128)
    for p in range(6):
        wg[p, depth_of(x), :] = wown[p]
    wog[pl.ds(z, 1)] = wo[...].reshape(1, 512, 128)

    up = jnp.concatenate([parents[:, q : q + 1] for q in range(NQ)], axis=0).astype(F32)
    taken_in = jnp.concatenate([upright(accepted)] * NQ, axis=0)
    seq = lax.rem(iota((count, 1), 0), NS).astype(F32)
    is_root = up < 0.0
    nodes = iota((count, 9 * NS + count), 1).astype(F32)

    def reach(back, other):
        return jnp.where(is_root, (taken_in + back) * NS + seq, other)

    at_kin = up * NS + seq
    kin = iota((count, count), 1).astype(F32)
    links = (kin == jnp.where(is_root, -1.0, at_kin)).astype(F32)
    eye = (iota((count, count), 0) == iota((count, count), 1)).astype(F32)
    family = eye + links
    for _ in range(4):
        family = jnp.minimum(dot(family, family), 1.0)
    is_kin = family > 0.5
    one = (nodes == reach(2.0, 9.0 * NS + at_kin)).astype(F32)
    two = dot(links, one) + (nodes == reach(1.0, -1.0)).astype(F32)
    three = dot(links, two) + (nodes == reach(0.0, -1.0)).astype(F32)
    one, two, three = one.astype(BF16), two.astype(BF16), three.astype(BF16)

    def tree_conv(first, last, own, taps):
        values = jnp.concatenate([past(first, last), own], axis=0).astype(BF16)
        summed = taps[3:4] * own
        for k, far in ((2, one), (1, two), (0, three)):
            summed = summed + taps[k : k + 1] * dot(far, values)
        return silu(summed)

    for d in order:
        tok_copy(d).wait_recv()
        tok_share(d).start()
    o_send(2)

    def forward(ch):
        for p in (2 * ch, 2 * ch + 1):
            w_own(p, p % 2).wait_recv()
            w_pass(p).start()

    def multiply(ch):
        for p in (2 * ch, 2 * ch + 1):
            w_own(p, 1 - p % 2).wait_recv()
            w_pass(p).wait_recv()
            prod[p] = jnp.dot(ts[...], wg[p], preferred_element_type=F32).reshape(
                NQ, NZ, NS, 256
            )
            r_step(p, 1)

    def advance(ch, hop):
        for p in (2 * ch, 2 * ch + 1):
            r_step(p, hop)

    forward(0)
    w_own(4, 0).start()
    w_own(4, 1).start()
    w_own(5, 1).start()
    w_own(5, 0).start()
    for d in order:
        tok_share(d).wait_recv()
    squares = jnp.zeros((NQ * NZ * NS, 128), F32)
    for xs in range(NX):
        values = tg[xs].reshape(NQ * NZ * NS, 128).astype(F32)
        squares = squares + values * values
        ts[:, xs * 128 : (xs + 1) * 128] = (values * gain[pl.ds(z * NX + xs, 1), :]).astype(BF16)
    lane = iota((NQ * NZ * NS, 128), 1)
    tall = jnp.concatenate([wr[...].astype(F32), jnp.zeros((120, 512), F32)], axis=0).astype(BF16)
    rates = dot_of(ts[...], tall, (1, 1))
    sums = jnp.sum(squares, axis=1, keepdims=True)
    aprod[...] = jnp.where(lane == 8, sums, rates).reshape(NQ, NZ, NS, 128)
    r_step(6, 1)
    multiply(0)
    forward(1)
    o_send(3)
    r_step(6, 2)
    advance(0, 2)
    multiply(1)
    forward(2)
    r_step(6, 3)
    advance(0, 3)
    advance(1, 2)
    multiply(2)
    o_send(4)
    r_step(6, 4)
    advance(0, 4)
    advance(1, 3)
    advance(2, 2)

    total = r_total(6)
    scale = lax.rsqrt(total[:, 8:9] / (NZ * NX * 128.0) + EPS)
    rate = -jnp.exp(alog[...])
    step = softplus((total[:, 0:NH] * scale).astype(BF16).astype(F32) + bias[...])
    slope = step * rate
    decay = dot_of(family, slope, (1, 0), HIGH)
    decay_t = dot_of(slope, family, (0, 1), HIGH)
    step_t = dot_of(step, eye, (0, 1), HIGH)
    grown = widen(jnp.exp(decay))
    skip = widen(jnp.broadcast_to(dskip[...], (NS, NH)))[0:1]

    def scaled_rows(p):
        return (r_total(p) * scale).astype(BF16).astype(F32)

    advance(1, 4)
    advance(2, 3)
    post_x = tree_conv(
        cx,
        px,
        jnp.concatenate([scaled_rows(0), scaled_rows(1)], axis=1),
        wtx[...].astype(F32),
    )
    post_xb = post_x.astype(BF16)
    advance(2, 4)
    post_b = tree_conv(cb, pb, scaled_rows(2), wtb[...].astype(F32)).astype(BF16)
    post_c = tree_conv(cc, pc, scaled_rows(3), wtc[...].astype(F32)).astype(BF16)
    seq_of = lax.rem(iota((count, 128), 0), NS)
    side = iota((count, 128), 1)
    heads_of = []
    for g in range(2):
        wide, narrow = slice(256 * g, 256 * g + 256), slice(128 * g, 128 * g + 128)
        post_bg, post_cg = post_b[:, narrow], post_c[:, narrow]
        split_c = jnp.concatenate(
            [jnp.where(seq_of == s, post_cg.astype(F32), 0.0) for s in range(NS)], axis=1
        ).astype(BF16)
        carried = dot_of(split_c, fresh[g], (1, 1))
        scores = dot_of(post_cg, post_bg, (1, 1))
        within = []
        for pair in range(2):
            sides = []
            at = 256 * g + 128 * pair
            for h in (4 * g + 2 * pair, 4 * g + 2 * pair + 1):
                gap = decay[:, h : h + 1] - decay_t[h : h + 1, :]
                mixing = jnp.exp(jnp.where(is_kin, gap, 0.0)) * step_t[h : h + 1, :]
                mixing = jnp.where(is_kin, scores * mixing, 0.0)
                sides.append(dot(mixing, post_xb[:, at : at + 128]))
            within.append(jnp.where(side < 64, sides[0], sides[1]))
        heads = carried * grown[:, wide] + jnp.concatenate(within, axis=1)
        heads_of.append(heads + skip[:, wide] * post_x[:, wide])
    for way in (0, 1):
        o_copy(way, 4).wait_recv()
    for k in range(NZ):
        at = 512 * (k % 2) + 128 * (k // 2)
        woc[:, at : at + 128] = wog[k]
    for g in range(2):
        wide = slice(256 * g, 256 * g + 256)
        heads = heads_of[g] * silu(scaled_rows(4 + g))
        spread_of = jnp.sum(heads * heads, axis=1, keepdims=True) / 256.0
        heads = heads * lax.rsqrt(spread_of + EPS) * gain_out[:, wide]
        gated[:, wide] = heads.astype(BF16)

    def g_copy(d):
        return remote(
            gated, gg.at[d - 1], g_s.at[d - 1], g_r.at[d - 1], {"x": wrap(x + d, NX)}
        )

    def d_copy(d):
        return remote(given.at[d], taken.at[d], d_s.at[d], d_r.at[d], {"c": 1 - c})

    def p_copy(d, e):
        to_y = wrap(y + e, NY)
        return remote(
            part.at[d, to_y],
            terms.at[x * NY + y],
            p_s.at[d, e],
            p_r.at[d, e],
            {"x": wrap(x - d, NX), "y": to_y},
        )

    for d in order:
        g_copy(d).start()

    def product(d):
        if d > 0:
            g_copy(d).wait_recv()
        values = gated[...] if d == 0 else gg[d - 1]
        mine = pl.ds(pl.multiple_of(512 * c, 512), 512)
        other = pl.ds(pl.multiple_of(512 * (1 - c), 512), 512)
        given[d] = jnp.dot(values, woc[:, other], preferred_element_type=F32).astype(BF16)
        d_copy(d).start()
        kept[d] = jnp.dot(values, woc[:, mine], preferred_element_type=F32)

    def deliver(d):
        d_copy(d).wait_recv()
        both = (kept[d] + taken[d].astype(F32)).astype(BF16)
        for to in range(NY):
            part[d, to] = both[:, 128 * to : 128 * to + 128]
        for e in (2, 1, 3, 0):
            if d + e > 0:
                p_copy(d, e).start()

    product(0)
    deliver(0)
    terms[pl.ds(x * NY + y, 1)] = part[0, pl.ds(y, 1)]
    product(2)
    deliver(2)
    product(1)
    product(3)
    deliver(1)
    deliver(3)
    for d, e in plane:
        p_copy(d, e).wait_recv()
    for xs in range(NX):
        total = terms[xs * NY].astype(F32)
        for k in range(1, NY):
            total = total + terms[xs * NY + k].astype(F32)
        mixed[:, xs * 128 : (xs + 1) * 128] = total

    for way in (0, 1):
        for hop in (1, 2, 3, 4):
            o_copy(way, hop).wait_send()
    for d in order:
        tok_copy(d).wait_send()
        tok_share(d).wait_send()
        g_copy(d).wait_send()
    for p in range(6):
        w_own(p, 0).wait_send()
        w_own(p, 1).wait_send()
        w_pass(p).wait_send()
    for p in range(7):
        for way in (0, 1):
            for hop in range(1, hops_of(p, way) + 1):
                r_copy(p, way, hop).wait_send()
    for d in range(NX):
        d_copy(d).wait_send()
    for d, e in plane:
        p_copy(d, e).wait_send()


def mixer(*args):
    vmem = pl.BlockSpec(memory_space=pltpu.VMEM)
    far = pl.BlockSpec(memory_space=pl.ANY)
    dma = pltpu.SemaphoreType.DMA
    rows = NQ * NS
    return pl.pallas_call(
        mixer_kernel,
        name="mixer",
        out_shape=jax.ShapeDtypeStruct((rows, 512), F32),
        in_specs=[far] * 8 + [vmem] * (len(args) - 8),
        out_specs=vmem,
        scratch_shapes=[
            pltpu.VMEM((NQ, NZ, NX, NS, 128), BF16),
            pltpu.VMEM((6, 128, 256), BF16),
            pltpu.VMEM((NH, 512), BF16),
            pltpu.VMEM((512, 128), BF16),
            pltpu.VMEM((2, 256, 1024), BF16),
            pltpu.VMEM((NX, NQ, NZ, NS, 128), BF16),
            pltpu.VMEM((NZ * rows, 512), BF16),
            pltpu.VMEM((6, 512, 256), BF16),
            pltpu.VMEM((NZ, 512, 128), BF16),
            pltpu.VMEM((6, NQ, NZ, NS, 256), F32),
            pltpu.VMEM((NQ, NZ, NS, 128), F32),
            pltpu.VMEM((6, 2, 4, NQ, NS, 256), BF16),
            pltpu.VMEM((2, 4, NQ, NS, 128), BF16),
            pltpu.VMEM((6, 2, NQ, NS, 256), BF16),
            pltpu.VMEM((2, NQ, NS, 128), BF16),
            pltpu.VMEM((rows, 512), BF16),
            pltpu.VMEM((3, rows, 512), BF16),
            pltpu.VMEM((512, 1024), BF16),
            pltpu.VMEM((NX, rows, 512), F32),
            pltpu.VMEM((NX, rows, 512), BF16),
            pltpu.VMEM((NX, rows, 512), BF16),
            pltpu.VMEM((NX, NY, rows, 128), BF16),
            pltpu.VMEM((NX * NY, rows, 128), BF16),
            dma((10,)),
            dma((3,)),
            dma((3,)),
            dma((3,)),
            dma((3,)),
            dma((6, 3)),
            dma((6, 3)),
            dma((7, 2, 4)),
            dma((7, 2, 4)),
            dma((2, 4)),
            dma((2, 4)),
            dma((3,)),
            dma((3,)),
            dma((NX,)),
            dma((NX,)),
            dma((NX, NY)),
            dma((NX, NY)),
        ],
        compiler_params=pltpu.CompilerParams(
            collective_id=0, has_side_effects=True, vmem_limit_bytes=VMEM_LIMIT
        ),
    )(*args)


def by_place(v):
    v = jnp.transpose(v, (1, 0, 2))
    return v.reshape(v.shape[0] * v.shape[1], v.shape[2])


def shards(
    tokens,
    parents,
    accepted,
    state,
    conv_x,
    conv_b,
    conv_c,
    path_x,
    path_b,
    path_c,
    path_dt,
    gain_in,
    w_x,
    w_z,
    w_b,
    w_c,
    w_dt,
    dt_bias,
    a_log,
    d_skip,
    conv_wx,
    conv_wb,
    conv_wc,
    gain_out,
    w_out,
):
    tok = jnp.transpose(tokens, (1, 0, 2)).reshape(NQ, NZ, NX, NS, 128)
    conv_x, path_x = by_place(conv_x), by_place(path_x)
    conv_b, path_b = by_place(conv_b), by_place(path_b)
    conv_c, path_c = by_place(conv_c), by_place(path_c)
    accepted, dt_bias, a_log = accepted[None, :], dt_bias[None, :], a_log[None, :]
    new_state, fresh = replay(
        accepted,
        conv_x,
        path_x,
        conv_b,
        path_b,
        by_place(path_dt),
        state.reshape(NS, 512, 128),
        dt_bias,
        a_log,
        conv_wx,
        conv_wb,
    )
    mixed = mixer(
        tok,
        w_x,
        w_z,
        w_b,
        w_c,
        w_dt.T,
        w_out,
        fresh,
        gain_in.reshape(32, 128),
        parents,
        accepted,
        conv_x,
        path_x,
        conv_b,
        path_b,
        conv_c,
        path_c,
        dt_bias,
        a_log,
        d_skip[None, :],
        conv_wx,
        conv_wb,
        conv_wc,
        gain_out[None, :],
    )
    mixed = jnp.transpose(mixed.reshape(NQ, NS, 512).astype(BF16), (1, 0, 2))
    return (mixed, new_state.reshape(NS, NH, 64, 128))


def solution(mesh):
    finer = Mesh(mesh.devices.reshape(NZ, NX, NY, NC), ("z", "x", "y", "c"))
    return jax.shard_map(
        shards,
        mesh=finer,
        in_specs=(
            P(None, None, KV),
            P(KV, None),
            P(KV),
            P(KV, TP, None, None),
            P(KV, None, TP),
            P(KV, None, TP),
            P(KV, None, TP),
            P(KV, None, TP),
            P(KV, None, TP),
            P(KV, None, TP),
            P(KV, None, TP),
            P(),
            P(KV, TP),
            P(KV, TP),
            P(KV, TP),
            P(KV, TP),
            P(),
            P(TP),
            P(TP),
            P(TP),
            P(None, TP),
            P(None, TP),
            P(None, TP),
            P(TP),
            P(TP, KV),
        ),
        out_specs=(P(KV, None, TP), P(KV, TP, None, None)),
        check_vma=False,
    )
```

```python
import functools

import jax
import jax.numpy as jnp
from jax import lax
from jax.experimental import pallas as pl
from jax.experimental.pallas import tpu as pltpu
from jax.sharding import Mesh
from jax.sharding import PartitionSpec as P

NZ, NX, NY, NC = 8, 4, 4, 2
NT = NY * NC
MESH = pl.DeviceIdType.MESH
KV = ("z", "x")
TP = ("y", "c")
EPS = 1e-06
HIGH = lax.Precision.HIGHEST
F32 = jnp.float32
BF16 = jnp.bfloat16
NQ, NS, NP, NH = 12, 8, 6, 8
VMEM_LIMIT = 60 * 1024 * 1024


def wrap(i, n):
    return lax.rem(i + n, n)


def remote(src, dst, send_sem, recv_sem, device):
    return pltpu.make_async_remote_copy(
        src_ref=src,
        dst_ref=dst,
        send_sem=send_sem,
        recv_sem=recv_sem,
        device_id=device,
        device_id_type=MESH,
    )


def greet(devices):
    barrier = pltpu.get_barrier_semaphore()
    for device in devices:
        pl.semaphore_signal(barrier, inc=1, device_id=device, device_id_type=MESH)
    pl.semaphore_wait(barrier, len(devices))


def hops_of(piece, way):
    return 4 if (piece % 2 == 0) == (way == 0) else 3


def silu(v):
    return v * (1.0 / (1.0 + jnp.exp(-v)))


def softplus(v):
    return jnp.maximum(v, 0.0) + jnp.log1p(jnp.exp(-jnp.abs(v)))


def iota(shape, dim):
    return lax.broadcasted_iota(jnp.int32, shape, dim)


def dot(a, b):
    return jnp.dot(a.astype(BF16), b.astype(BF16), preferred_element_type=F32)


def dot_of(a, b, dims, precision=None):
    return lax.dot_general(
        a, b, ((dims[:1], dims[1:]), ((), ())), precision=precision, preferred_element_type=F32
    )


def past(first, last):
    return jnp.concatenate([first[...].astype(F32), last[...].astype(F32)], axis=0)


def widen(v):
    spread = (iota((NH, 512), 1) // 64 == iota((NH, 512), 0)).astype(F32)
    return dot_of(v, spread, (1, 0), HIGH)


def upright(row):
    wide = jnp.broadcast_to(row[...].astype(F32), (NS, NS))
    return jnp.sum(
        jnp.where(iota((NS, NS), 0) == iota((NS, NS), 1), wide, 0.0), axis=1, keepdims=True
    )


def mixer_kernel(
    tok_h,
    wx_h,
    wz_h,
    wb_h,
    wc_h,
    wdt_h,
    wo_h,
    state_h,
    gain,
    parents,
    accepted,
    cx,
    px,
    cb,
    pb,
    cc,
    pc,
    pdt,
    bias,
    alog,
    dskip,
    wtx,
    wtb,
    wtc,
    gain_out,
    mixed,
    new_state,
    tok,
    wown,
    wr,
    wo,
    held,
    fresh,
    tg,
    ts,
    wg,
    wog,
    prod,
    aprod,
    ring,
    aring,
    stage,
    astage,
    gated,
    gg,
    woc,
    kept,
    given,
    taken,
    part,
    terms,
    l_s,
    s_s,
    n_s,
    t_s,
    t_r,
    f_s,
    f_r,
    w_s,
    w_r,
    r_s,
    r_r,
    o_s,
    o_r,
    g_s,
    g_r,
    d_s,
    d_r,
    p_s,
    p_r,
):
    z, x = lax.axis_index("z"), lax.axis_index("x")
    y, c = lax.axis_index("y"), lax.axis_index("c")
    t = y * NC + c
    count = NQ * NS

    def depth_of(owner):
        return pl.ds(pl.multiple_of(owner * 128, 128), 128)

    sources = [
        wx_h.at[:, 0:256],
        wx_h.at[:, 256:512],
        wb_h,
        wc_h,
        wz_h.at[:, 0:256],
        wz_h.at[:, 256:512],
    ]
    loads = [(tok_h, tok)] + [(sources[p], wown.at[p]) for p in range(6)]
    loads.append((wo_h, wo))
    loads.append(
        (
            wdt_h.at[
                pl.ds(pl.multiple_of(t * NH, NH), NH), pl.ds(pl.multiple_of(z * 512, 512), 512)
            ],
            wr,
        )
    )

    def load(k):
        return pltpu.make_async_copy(loads[k][0], loads[k][1], l_s.at[k])

    def load_state(s):
        return pltpu.make_async_copy(state_h.at[s], held.at[s], s_s.at[s])

    def save_state(s):
        return pltpu.make_async_copy(held.at[s], new_state.at[s], n_s.at[s])

    for k in (1, 2, 0, 3, 4, 7, 5, 6, 8):
        load(k).start()
    for s in range(NS):
        load_state(s).start()
    plane = [(d, e) for d in range(NX) for e in range(NY) if d + e > 0]
    greet(
        [{"x": wrap(x + d, NX), "y": wrap(y + e, NY)} for d, e in plane]
        + [{"z": wrap(z + 1, NZ)}, {"z": wrap(z - 1, NZ)}, {"c": 1 - c}]
    )
    half = pl.ds(4 * c, 4)

    def tok_copy(d):
        to = wrap(x + d, NX)
        return remote(
            tok.at[:, half, to], tg.at[x, :, half], t_s.at[d - 1], t_r.at[d - 1], {"x": to}
        )

    def tok_share(d):
        block = tg.at[wrap(x - d, NX), :, half]
        return remote(block, block, f_s.at[d - 1], f_r.at[d - 1], {"c": 1 - c})

    def w_own(p, way):
        to = wrap(x + (1 if way == 0 else -1), NX)
        return remote(
            wown.at[p], wg.at[p, depth_of(x), :], w_s.at[p, way], w_r.at[p, way], {"x": to}
        )

    def w_pass(p):
        sign = 1 if p % 2 == 0 else -1
        block = wg.at[p, depth_of(wrap(x - sign, NX)), :]
        return remote(block, block, w_s.at[p, 2], w_r.at[p, 2], {"x": wrap(x + sign, NX)})

    def o_copy(way, hop):
        sign = 1 if way == 0 else -1
        owner = wrap(z - sign * (hop - 1), NZ)
        src = wo if hop == 1 else wog.at[owner]
        dst = wog.at[owner]
        if hop == 4:
            src, dst = src.at[pl.ds(256 * way, 256)], dst.at[pl.ds(256 * way, 256)]
        return remote(
            src, dst, o_s.at[way, hop - 1], o_r.at[way, hop - 1], {"z": wrap(z + sign, NZ)}
        )

    def r_copy(p, way, hop):
        to = {"z": wrap(z + (1 if way == 0 else -1), NZ)}
        if p == 6:
            src = astage.at[way] if hop == 1 else aring.at[way, hop - 2]
            dst = aring.at[way, hop - 1]
        else:
            src = stage.at[p, way] if hop == 1 else ring.at[p, way, hop - 2]
            dst = ring.at[p, way, hop - 1]
        return remote(src, dst, r_s.at[p, way, hop - 1], r_r.at[p, way, hop - 1], to)

    def own_term(p, dest):
        if p == 6:
            return aprod[pl.ds(dest, 1)].reshape(16, count)
        return prod[p, :, pl.ds(dest, 1)].reshape(NQ, NS, 256)

    def r_step(p, hop):
        for way in (0, 1):
            hops = hops_of(p, way)
            if hop > hops:
                continue
            sign = 1 if way == 0 else -1
            term = own_term(p, wrap(z + sign * (hops + 1 - hop), NZ))
            if hop == 1:
                if p == 6:
                    astage[way] = term.astype(BF16)
                else:
                    stage[p, way] = term.astype(BF16)
            else:
                r_copy(p, way, hop - 1).wait_recv()
                if p == 6:
                    aring[way, hop - 2] = (aring[way, hop - 2].astype(F32) + term).astype(BF16)
                else:
                    ring[p, way, hop - 2] = (ring[p, way, hop - 2].astype(F32) + term).astype(BF16)
            r_copy(p, way, hop).start()

    def r_total(p):
        total = own_term(p, z)
        for way in (0, 1):
            hops = hops_of(p, way)
            r_copy(p, way, hops).wait_recv()
            arrived = aring[way, hops - 1] if p == 6 else ring[p, way, hops - 1]
            total = total + arrived.astype(F32)
        return total if p == 6 else total.reshape(count, 256)

    order = (2, 1, 3)

    def w_send(ch):
        for p in (2 * ch, 2 * ch + 1):
            load(1 + p).wait()
            w_own(p, p % 2).start()
            w_own(p, 1 - p % 2).start()

    def o_send(hop):
        for way in (0, 1):
            if hop > 1:
                o_copy(way, hop - 1).wait_recv()
            o_copy(way, hop).start()

    w_send(0)
    load(0).wait()
    for d in order:
        tok_copy(d).start()
    load(7).wait()
    o_send(1)

    up = jnp.concatenate([parents[:, q : q + 1] for q in range(NQ)], axis=0).astype(F32)
    taken_in = jnp.concatenate([upright(accepted)] * NQ, axis=0)
    seq = lax.rem(iota((count, 1), 0), NS).astype(F32)
    is_root = up < 0.0
    nodes = iota((count, 9 * NS + count), 1).astype(F32)

    def reach(back, other):
        return jnp.where(is_root, (taken_in + back) * NS + seq, other)

    at_kin = up * NS + seq
    kin = iota((count, count), 1).astype(F32)
    links = (kin == jnp.where(is_root, -1.0, at_kin)).astype(F32)
    eye = (iota((count, count), 0) == iota((count, count), 1)).astype(F32)
    family = eye + links
    for _ in range(4):
        family = jnp.minimum(dot(family, family), 1.0)
    is_kin = family > 0.5
    one = (nodes == reach(2.0, 9.0 * NS + at_kin)).astype(F32)
    two = dot(links, one) + (nodes == reach(1.0, -1.0)).astype(F32)
    three = dot(links, two) + (nodes == reach(0.0, -1.0)).astype(F32)
    one, two, three = one.astype(BF16), two.astype(BF16), three.astype(BF16)

    def window(history, taps):
        summed = taps[0:1] * history[0 : NP * NS]
        for k in (1, 2, 3):
            summed = summed + taps[k : k + 1] * history[k * NS : (k + NP) * NS]
        return silu(summed)

    rate = -jnp.exp(alog[...])
    path_xs = window(past(cx, px), wtx[...].astype(F32))
    path_bs = window(past(cb, pb), wtb[...].astype(F32))
    path_step = softplus(pdt[...].astype(F32) + bias[...])
    live = ((iota((NP * NS, 1), 0) // NS).astype(F32) < taken_in[0 : NP * NS]).astype(F32)
    path_log = path_step * rate * live
    tails = [jnp.zeros((NS, NH), F32)]
    for j in range(NP - 1, 0, -1):
        tails.insert(0, tails[0] + path_log[j * NS : (j + 1) * NS])
    overall = jnp.exp(tails[0] + path_log[0:NS])
    weights = live * jnp.exp(jnp.concatenate(tails, axis=0)) * path_step
    weighted = (path_xs * widen(weights)).astype(BF16)
    path_seq = lax.rem(iota((NP * NS, 128), 0), NS)

    def forward(ch):
        for p in (2 * ch, 2 * ch + 1):
            w_own(p, p % 2).wait_recv()
            w_pass(p).start()

    forward(0)
    w_send(1)
    w_send(2)
    o_send(2)
    tg[pl.ds(x, 1)] = tok[:, :, pl.ds(x, 1)].reshape(1, NQ, NZ, NS, 128)
    for p in range(6):
        wg[p, depth_of(x), :] = wown[p]
    wog[pl.ds(z, 1)] = wo[...].reshape(1, 512, 128)
    load(8).wait()

    gained = []
    for g in range(2):
        split_b = jnp.concatenate(
            [
                jnp.where(path_seq == s, path_bs[:, 128 * g : 128 * g + 128], 0.0)
                for s in range(NS)
            ],
            axis=1,
        ).astype(BF16)
        gained.append(dot_of(weighted[:, 256 * g : 256 * g + 256], split_b, (0, 0)))
    for s in range(NS):
        load_state(s).wait()
        at = slice(128 * s, 128 * s + 128)
        for g in range(2):
            wide = slice(256 * g, 256 * g + 256)
            fade = jnp.concatenate(
                [
                    jnp.broadcast_to(overall[s : s + 1, h : h + 1], (64, 128))
                    for h in range(4 * g, 4 * g + 4)
                ],
                axis=0,
            )
            now = fade * held[s, wide, :] + gained[g][:, at]
            held[s, wide, :] = now
            fresh[g, :, at] = now.astype(BF16)
        save_state(s).start()

    def tree_conv(first, last, own, taps):
        values = jnp.concatenate([past(first, last), own], axis=0).astype(BF16)
        summed = taps[3:4] * own
        for k, far in ((2, one), (1, two), (0, three)):
            summed = summed + taps[k : k + 1] * dot(far, values)
        return silu(summed)

    for d in order:
        tok_copy(d).wait_recv()
        tok_share(d).start()

    def multiply(ch):
        for p in (2 * ch, 2 * ch + 1):
            w_own(p, 1 - p % 2).wait_recv()
            w_pass(p).wait_recv()
            prod[p] = jnp.dot(
                ts[...].reshape(NQ * NZ * NS, 512), wg[p], preferred_element_type=F32
            ).reshape(NQ, NZ, NS, 256)
            r_step(p, 1)

    def advance(ch, hop):
        for p in (2 * ch, 2 * ch + 1):
            r_step(p, hop)

    squares = jnp.zeros((NQ * NZ * NS, 128), F32)
    for d in (0,) + order:
        if d > 0:
            tok_share(d).wait_recv()
        xs = wrap(x - d, NX)
        values = tg[pl.ds(xs, 1)].reshape(NQ * NZ * NS, 128).astype(F32)
        squares = squares + values * values
        scaled = (values * gain[pl.ds(z * NX + xs, 1), :]).astype(BF16)
        ts[:, :, :, depth_of(xs)] = scaled.reshape(NQ, NZ, NS, 128)
    multiply(0)
    tall = jnp.concatenate([wr[...].astype(F32), jnp.zeros((8, 512), F32)], axis=0).astype(BF16)
    squares = squares.reshape(NQ, NZ, NS, 128)
    for dest in range(NZ):
        rates = dot_of(tall, ts[:, dest].reshape(count, 512), (1, 1))
        sums = dot_of(
            jnp.ones((16, 128), F32), squares[:, dest].reshape(count, 128), (1, 1), HIGH
        )
        aprod[dest] = jnp.where(iota((16, count), 0) == NH, sums, rates)
    r_step(6, 1)
    o_send(3)
    forward(1)
    advance(0, 2)
    r_step(6, 2)
    forward(2)
    o_send(4)
    multiply(1)
    advance(0, 3)
    r_step(6, 3)
    multiply(2)
    advance(1, 2)
    advance(0, 4)
    r_step(6, 4)
    advance(2, 2)
    advance(1, 3)

    total = r_total(6)
    scale = lax.rsqrt(dot_of(eye, total, (1, 1), HIGH)[:, NH : NH + 1] / (NZ * NX * 128.0) + EPS)
    scale_t = lax.rsqrt(total[NH : NH + 1] / (NZ * NX * 128.0) + EPS)
    step_t = softplus((total[0:NH] * scale_t).astype(BF16).astype(F32) + upright(bias))
    slope_t = step_t * -jnp.exp(upright(alog))
    decay = dot_of(family, slope_t, (1, 1), HIGH)
    decay_t = dot_of(slope_t, family, (1, 1), HIGH)
    grown = widen(jnp.exp(decay))
    skip = widen(jnp.broadcast_to(dskip[...], (NS, NH)))[0:1]

    def scaled_rows(p):
        return (r_total(p) * scale).astype(BF16).astype(F32)

    advance(2, 3)
    advance(1, 4)
    post_x = tree_conv(
        cx,
        px,
        jnp.concatenate([scaled_rows(0), scaled_rows(1)], axis=1),
        wtx[...].astype(F32),
    )
    post_xb = post_x.astype(BF16)
    advance(2, 4)
    post_b = tree_conv(cb, pb, scaled_rows(2), wtb[...].astype(F32)).astype(BF16)
    post_c = tree_conv(cc, pc, scaled_rows(3), wtc[...].astype(F32)).astype(BF16)
    seq_of = lax.rem(iota((count, 128), 0), NS)
    side = iota((count, 128), 1)
    heads_of = []
    for g in range(2):
        wide, narrow = slice(256 * g, 256 * g + 256), slice(128 * g, 128 * g + 128)
        post_bg, post_cg = post_b[:, narrow], post_c[:, narrow]
        split_c = jnp.concatenate(
            [jnp.where(seq_of == s, post_cg.astype(F32), 0.0) for s in range(NS)], axis=1
        ).astype(BF16)
        carried = dot_of(split_c, fresh[g], (1, 1))
        scores = dot_of(post_cg, post_bg, (1, 1))
        within = []
        for pair in range(2):
            sides = []
            at = 256 * g + 128 * pair
            for h in (4 * g + 2 * pair, 4 * g + 2 * pair + 1):
                gap = decay[:, h : h + 1] - decay_t[h : h + 1, :]
                mixing = jnp.exp(jnp.where(is_kin, gap, 0.0)) * step_t[h : h + 1, :]
                mixing = jnp.where(is_kin, scores * mixing, 0.0)
                sides.append(dot(mixing, post_xb[:, at : at + 128]))
            within.append(jnp.where(side < 64, sides[0], sides[1]))
        heads = carried * grown[:, wide] + jnp.concatenate(within, axis=1)
        heads_of.append(heads + skip[:, wide] * post_x[:, wide])
    for way in (0, 1):
        o_copy(way, 4).wait_recv()
    for k in range(NZ):
        at = 512 * (k % 2) + 128 * (k // 2)
        woc[:, at : at + 128] = wog[k]
    for g in range(2):
        wide = slice(256 * g, 256 * g + 256)
        heads = heads_of[g] * silu(scaled_rows(4 + g))
        spread_of = jnp.sum(heads * heads, axis=1, keepdims=True) / 256.0
        heads = heads * lax.rsqrt(spread_of + EPS) * gain_out[:, wide]
        gated[:, wide] = heads.astype(BF16)

    def g_copy(d):
        return remote(
            gated, gg.at[d - 1], g_s.at[d - 1], g_r.at[d - 1], {"x": wrap(x + d, NX)}
        )

    def d_copy(d):
        return remote(given.at[d], taken.at[d], d_s.at[d], d_r.at[d], {"c": 1 - c})

    def p_copy(d, e):
        to_y = wrap(y + e, NY)
        return remote(
            part.at[d, to_y],
            terms.at[x * NY + y],
            p_s.at[d, e],
            p_r.at[d, e],
            {"x": wrap(x - d, NX), "y": to_y},
        )

    for d in order:
        g_copy(d).start()

    def product(d):
        if d > 0:
            g_copy(d).wait_recv()
        values = gated[...] if d == 0 else gg[d - 1]
        mine = pl.ds(pl.multiple_of(512 * c, 512), 512)
        other = pl.ds(pl.multiple_of(512 * (1 - c), 512), 512)
        given[d] = jnp.dot(values, woc[:, other], preferred_element_type=F32).astype(BF16)
        d_copy(d).start()
        kept[d] = jnp.dot(values, woc[:, mine], preferred_element_type=F32)

    def deliver(d):
        d_copy(d).wait_recv()
        both = (kept[d] + taken[d].astype(F32)).astype(BF16)
        for to in range(NY):
            part[d, to] = both[:, 128 * to : 128 * to + 128]
        for e in (2, 1, 3, 0):
            if d + e > 0:
                p_copy(d, e).start()

    product(0)
    deliver(0)
    terms[pl.ds(x * NY + y, 1)] = part[0, pl.ds(y, 1)]
    product(2)
    deliver(2)
    product(1)
    product(3)
    deliver(1)
    deliver(3)
    for d, e in plane:
        p_copy(d, e).wait_recv()
    for xs in range(NX):
        total = terms[xs * NY].astype(F32)
        for k in range(1, NY):
            total = total + terms[xs * NY + k].astype(F32)
        mixed[:, xs * 128 : (xs + 1) * 128] = total

    for s in range(NS):
        save_state(s).wait()
    for way in (0, 1):
        for hop in (1, 2, 3, 4):
            o_copy(way, hop).wait_send()
    for d in order:
        tok_copy(d).wait_send()
        tok_share(d).wait_send()
        g_copy(d).wait_send()
    for p in range(6):
        w_own(p, 0).wait_send()
        w_own(p, 1).wait_send()
        w_pass(p).wait_send()
    for p in range(7):
        for way in (0, 1):
            for hop in range(1, hops_of(p, way) + 1):
                r_copy(p, way, hop).wait_send()
    for d in range(NX):
        d_copy(d).wait_send()
    for d, e in plane:
        p_copy(d, e).wait_send()


def mixer(*args):
    vmem = pl.BlockSpec(memory_space=pltpu.VMEM)
    far = pl.BlockSpec(memory_space=pl.ANY)
    dma = pltpu.SemaphoreType.DMA
    rows = NQ * NS
    return pl.pallas_call(
        mixer_kernel,
        name="mixer",
        out_shape=(
            jax.ShapeDtypeStruct((rows, 512), F32),
            jax.ShapeDtypeStruct((NS, 512, 128), F32),
        ),
        in_specs=[far] * 8 + [vmem] * (len(args) - 8),
        out_specs=(vmem, far),
        scratch_shapes=[
            pltpu.VMEM((NQ, NZ, NX, NS, 128), BF16),
            pltpu.VMEM((6, 128, 256), BF16),
            pltpu.VMEM((NH, 512), BF16),
            pltpu.VMEM((512, 128), BF16),
            pltpu.VMEM((NS, 512, 128), F32),
            pltpu.VMEM((2, 256, 1024), BF16),
            pltpu.VMEM((NX, NQ, NZ, NS, 128), BF16),
            pltpu.VMEM((NQ, NZ, NS, 512), BF16),
            pltpu.VMEM((6, 512, 256), BF16),
            pltpu.VMEM((NZ, 512, 128), BF16),
            pltpu.VMEM((6, NQ, NZ, NS, 256), F32),
            pltpu.VMEM((NZ, 16, rows), F32),
            pltpu.VMEM((6, 2, 4, NQ, NS, 256), BF16),
            pltpu.VMEM((2, 4, 16, rows), BF16),
            pltpu.VMEM((6, 2, NQ, NS, 256), BF16),
            pltpu.VMEM((2, 16, rows), BF16),
            pltpu.VMEM((rows, 512), BF16),
            pltpu.VMEM((3, rows, 512), BF16),
            pltpu.VMEM((512, 1024), BF16),
            pltpu.VMEM((NX, rows, 512), F32),
            pltpu.VMEM((NX, rows, 512), BF16),
            pltpu.VMEM((NX, rows, 512), BF16),
            pltpu.VMEM((NX, NY, rows, 128), BF16),
            pltpu.VMEM((NX * NY, rows, 128), BF16),
            dma((9,)),
            dma((NS,)),
            dma((NS,)),
            dma((3,)),
            dma((3,)),
            dma((3,)),
            dma((3,)),
            dma((6, 3)),
            dma((6, 3)),
            dma((7, 2, 4)),
            dma((7, 2, 4)),
            dma((2, 4)),
            dma((2, 4)),
            dma((3,)),
            dma((3,)),
            dma((NX,)),
            dma((NX,)),
            dma((NX, NY)),
            dma((NX, NY)),
        ],
        compiler_params=pltpu.CompilerParams(
            collective_id=0, has_side_effects=True, vmem_limit_bytes=VMEM_LIMIT
        ),
    )(*args)


def by_place(v):
    v = jnp.transpose(v, (1, 0, 2))
    return v.reshape(v.shape[0] * v.shape[1], v.shape[2])


def shards(
    tokens,
    parents,
    accepted,
    state,
    conv_x,
    conv_b,
    conv_c,
    path_x,
    path_b,
    path_c,
    path_dt,
    gain_in,
    w_x,
    w_z,
    w_b,
    w_c,
    w_dt,
    dt_bias,
    a_log,
    d_skip,
    conv_wx,
    conv_wb,
    conv_wc,
    gain_out,
    w_out,
):
    tok = jnp.transpose(tokens, (1, 0, 2)).reshape(NQ, NZ, NX, NS, 128)
    conv_x, path_x = by_place(conv_x), by_place(path_x)
    conv_b, path_b = by_place(conv_b), by_place(path_b)
    conv_c, path_c = by_place(conv_c), by_place(path_c)
    accepted, dt_bias, a_log = accepted[None, :], dt_bias[None, :], a_log[None, :]
    mixed, new_state = mixer(
        tok,
        w_x,
        w_z,
        w_b,
        w_c,
        w_dt.T,
        w_out,
        state.reshape(NS, 512, 128),
        gain_in.reshape(32, 128),
        parents,
        accepted,
        conv_x,
        path_x,
        conv_b,
        path_b,
        conv_c,
        path_c,
        by_place(path_dt),
        dt_bias,
        a_log,
        d_skip[None, :],
        conv_wx,
        conv_wb,
        conv_wc,
        gain_out[None, :],
    )
    mixed = jnp.transpose(mixed.reshape(NQ, NS, 512).astype(BF16), (1, 0, 2))
    return (mixed, new_state.reshape(NS, NH, 64, 128))


def solution(mesh):
    finer = Mesh(mesh.devices.reshape(NZ, NX, NY, NC), ("z", "x", "y", "c"))
    return jax.shard_map(
        shards,
        mesh=finer,
        in_specs=(
            P(None, None, KV),
            P(KV, None),
            P(KV),
            P(KV, TP, None, None),
            P(KV, None, TP),
            P(KV, None, TP),
            P(KV, None, TP),
            P(KV, None, TP),
            P(KV, None, TP),
            P(KV, None, TP),
            P(KV, None, TP),
            P(),
            P(KV, TP),
            P(KV, TP),
            P(KV, TP),
            P(KV, TP),
            P(),
            P(TP),
            P(TP),
            P(TP),
            P(None, TP),
            P(None, TP),
            P(None, TP),
            P(TP),
            P(TP, KV),
        ),
        out_specs=(P(KV, None, TP), P(KV, TP, None, None)),
        check_vma=False,
    )
```

```python
import functools

import jax
import jax.numpy as jnp
from jax import lax
from jax.experimental import pallas as pl
from jax.experimental.pallas import tpu as pltpu
from jax.sharding import Mesh
from jax.sharding import PartitionSpec as P

NZ, NX, NY, NC = 8, 4, 4, 2
NT = NY * NC
MESH = pl.DeviceIdType.MESH
KV = ("z", "x")
TP = ("y", "c")
EPS = 1e-06
HIGH = lax.Precision.HIGHEST
F32 = jnp.float32
BF16 = jnp.bfloat16
NQ, NS, NP, NH = 12, 8, 6, 8
VMEM_LIMIT = 60 * 1024 * 1024


def wrap(i, n):
    return lax.rem(i + n, n)


def remote(src, dst, send_sem, recv_sem, device):
    return pltpu.make_async_remote_copy(
        src_ref=src,
        dst_ref=dst,
        send_sem=send_sem,
        recv_sem=recv_sem,
        device_id=device,
        device_id_type=MESH,
    )


def greet(devices):
    barrier = pltpu.get_barrier_semaphore()
    for device in devices:
        pl.semaphore_signal(barrier, inc=1, device_id=device, device_id_type=MESH)
    pl.semaphore_wait(barrier, len(devices))


def settle(view, sem):
    pltpu.make_async_copy(view, view, sem).wait()


def hops_of(piece, way):
    return 4 if (piece % 2 == 0) == (way == 0) else 3


def slot_of(piece, way, hop):
    return (0, 2, 4, 5)[hop - 1] if hops_of(piece, way) == 4 else (1, 3, 6)[hop - 1]


def sem_of(piece, way, hop):
    return hop - 1 if hop < hops_of(piece, way) else 3


def silu(v):
    return v * (1.0 / (1.0 + jnp.exp(-v)))


def softplus(v):
    return jnp.maximum(v, 0.0) + jnp.log1p(jnp.exp(-jnp.abs(v)))


def iota(shape, dim):
    return lax.broadcasted_iota(jnp.int32, shape, dim)


def dot(a, b):
    return jnp.dot(a.astype(BF16), b.astype(BF16), preferred_element_type=F32)


def dot_of(a, b, dims, precision=None):
    return lax.dot_general(
        a, b, ((dims[:1], dims[1:]), ((), ())), precision=precision, preferred_element_type=F32
    )


def past(first, last):
    return jnp.concatenate([first[...].astype(F32), last[...].astype(F32)], axis=0)


def widen(v):
    spread = (iota((NH, 512), 1) // 64 == iota((NH, 512), 0)).astype(F32)
    return dot_of(v, spread, (1, 0), HIGH)


def upright(row):
    wide = jnp.broadcast_to(row[...].astype(F32), (NS, NS))
    return jnp.sum(
        jnp.where(iota((NS, NS), 0) == iota((NS, NS), 1), wide, 0.0), axis=1, keepdims=True
    )


def mixer_kernel(
    tok_h,
    wx_h,
    wz_h,
    wb_h,
    wc_h,
    wdt_h,
    wo_h,
    state_h,
    gain,
    parents,
    accepted,
    cx,
    px,
    cb,
    pb,
    cc,
    pc,
    pdt,
    bias,
    alog,
    dskip,
    wtx,
    wtb,
    wtc,
    gain_out,
    mixed,
    new_state,
    tok,
    wown,
    wr,
    wo,
    held,
    fresh,
    tg,
    ts,
    wg,
    wog,
    prod,
    aprod,
    ring,
    aring,
    stage,
    astage,
    gated,
    gg,
    woc,
    kept,
    hold,
    given,
    taken,
    part,
    terms,
    l_s,
    s_s,
    n_s,
    t_s,
    t_r,
    f_r,
    w_s,
    w_r,
    r_s,
    a_s,
    r_r,
    o_s,
    o_r,
    g_s,
    g_r,
    d_s,
    d_r,
    p_s,
    p_r,
):
    z, x = lax.axis_index("z"), lax.axis_index("x")
    y, c = lax.axis_index("y"), lax.axis_index("c")
    t = y * NC + c
    count = NQ * NS

    def depth_of(owner):
        return pl.ds(pl.multiple_of(owner * 128, 128), 128)

    lower, upper = slice(0, 128), slice(128, 256)
    loads = [(tok_h, tok, 0), (wo_h, wo, 1)]
    loads.append(
        (
            wdt_h.at[
                pl.ds(pl.multiple_of(t * NH, NH), NH), pl.ds(pl.multiple_of(z * 512, 512), 512)
            ],
            wr,
            2,
        )
    )
    for g in range(2):
        wide, narrow = slice(256 * g, 256 * g + 256), slice(128 * g, 128 * g + 128)
        loads.append((wx_h.at[:, wide], wown.at[3 * g], 3 + g))
        loads.append((wb_h.at[:, narrow], wown.at[3 * g + 1, :, lower], 4))
        loads.append((wc_h.at[:, narrow], wown.at[3 * g + 1, :, upper], 4))
        loads.append((wz_h.at[:, wide], wown.at[3 * g + 2], 4))

    def load(k):
        return pltpu.make_async_copy(loads[k][0], loads[k][1], l_s.at[loads[k][2]])

    def load_state(s):
        return pltpu.make_async_copy(state_h.at[s], held.at[s], s_s.at[s // 4])

    def save_state(s):
        return pltpu.make_async_copy(held.at[s], new_state.at[s], n_s)

    for k in (3, 0, 1, 4, 5, 6, 2, 7, 8, 9, 10):
        load(k).start()
    for s in range(NS):
        load_state(s).start()
    plane = [(d, e) for d in range(NX) for e in range(NY) if d + e > 0]
    greet(
        [{"x": wrap(x + d, NX), "y": wrap(y + e, NY)} for d, e in plane]
        + [{"z": wrap(z + 1, NZ)}, {"z": wrap(z - 1, NZ)}, {"c": 1 - c}]
    )
    half = pl.ds(4 * c, 4)

    def tok_copy(d):
        to = wrap(x + d, NX)
        return remote(
            tok.at[:, half, to], tg.at[x, :, half], t_s, t_r.at[d - 1], {"x": to}
        )

    def tok_share(d):
        block = tg.at[wrap(x - d, NX), :, half]
        return remote(block, block, t_s, f_r.at[d - 1], {"c": 1 - c})

    def w_own(p, way):
        to = wrap(x + (1 if way == 0 else -1), NX)
        last = 0 if way == p % 2 else 1
        return remote(wown.at[p], wg.at[4 * p + x], w_s, w_r.at[p, last], {"x": to})

    def w_pass(p):
        sign = 1 if p % 2 == 0 else -1
        block = wg.at[4 * p + wrap(x - sign, NX)]
        return remote(block, block, w_s, w_r.at[p, 1], {"x": wrap(x + sign, NX)})

    def o_step(hop, side):
        for way in (0, 1):
            if hop == 4:
                side = way
            if hop == 4 or (hop > 1 and way == 0):
                settle(wog.at[0], o_r.at[2 * (hop - 2) + side])
            sign = 1 if way == 0 else -1
            owner = wrap(z - sign * (hop - 1), NZ)
            part = pl.ds(256 * side, 256)
            src = wo.at[part] if hop == 1 else wog.at[owner, part]
            to = {"z": wrap(z + sign, NZ)}
            at = 6 if hop == 4 else 2 * (hop - 1) + side
            sends.append(remote(src, wog.at[owner, part], o_s, o_r.at[at], to))
        for copy in sends[-2:]:
            copy.start()

    sends = []

    def r_copy(p, way, hop):
        to = {"z": wrap(z + (1 if way == 0 else -1), NZ)}
        buffer = aring if p == 6 else ring.at[p]
        dst = buffer.at[slot_of(p, way, hop)]
        if hop > 1:
            src = buffer.at[slot_of(p, way, hop - 1)]
        else:
            src = astage.at[way] if p == 6 else stage.at[p, way]
        return remote(src, dst, a_s if p == 6 else r_s, r_r.at[p, sem_of(p, way, hop)], to)

    def r_wait(p, index):
        buffer = aring if p == 6 else ring.at[p]
        first, many = ((0, 2), (2, 2), (4, 1), (5, 2))[index]
        settle(buffer.at[pl.ds(first, many)], r_r.at[p, index])

    def own_term(p, dest):
        if p == 6:
            return aprod[pl.ds(dest, 1)].reshape(16, count)
        return prod[p, :, pl.ds(dest, 1)].reshape(NQ, NS, 256)

    def r_step(p, hop):
        if hop > 1:
            r_wait(p, hop - 2)
        for way in (0, 1):
            hops = hops_of(p, way)
            if hop > hops:
                continue
            sign = 1 if way == 0 else -1
            term = own_term(p, wrap(z + sign * (hops + 1 - hop), NZ))
            if hop == 1:
                if p == 6:
                    astage[way] = term.astype(BF16)
                else:
                    stage[p, way] = term.astype(BF16)
            else:
                at = slot_of(p, way, hop - 1)
                if p == 6:
                    aring[at] = (aring[at].astype(F32) + term).astype(BF16)
                else:
                    ring[p, at] = (ring[p, at].astype(F32) + term).astype(BF16)
            r_copy(p, way, hop).start()

    def r_total(p):
        r_wait(p, 3)
        if p == 6:
            return own_term(p, z) + aring[5].astype(F32) + aring[6].astype(F32)
        total = own_term(p, z) + ring[p, 5].astype(F32) + ring[p, 6].astype(F32)
        return total.reshape(count, 256)

    order = (2, 1, 3)

    def w_send(p):
        w_own(p, p % 2).start()
        w_own(p, 1 - p % 2).start()

    load(3).wait()
    w_send(0)
    load(0).wait()
    for d in order:
        tok_copy(d).start()
    load(1).wait()
    o_step(1, 0)
    o_step(1, 1)

    up = jnp.concatenate([parents[:, q : q + 1] for q in range(NQ)], axis=0).astype(F32)
    taken_in = jnp.concatenate([upright(accepted)] * NQ, axis=0)
    seq = lax.rem(iota((count, 1), 0), NS).astype(F32)
    is_root = up < 0.0
    nodes = iota((count, 9 * NS + count), 1).astype(F32)

    def reach(back, other):
        return jnp.where(is_root, (taken_in + back) * NS + seq, other)

    at_kin = up * NS + seq
    kin = iota((count, count), 1).astype(F32)
    links = (kin == jnp.where(is_root, -1.0, at_kin)).astype(F32)
    eye = (iota((count, count), 0) == iota((count, count), 1)).astype(F32)
    family = eye + links
    for _ in range(4):
        family = jnp.minimum(dot(family, family), 1.0)
    is_kin = family > 0.5
    one = (nodes == reach(2.0, 9.0 * NS + at_kin)).astype(F32)
    two = dot(links, one) + (nodes == reach(1.0, -1.0)).astype(F32)
    three = dot(links, two) + (nodes == reach(0.0, -1.0)).astype(F32)
    one, two, three = one.astype(BF16), two.astype(BF16), three.astype(BF16)

    def window(history, taps):
        summed = taps[0:1] * history[0 : NP * NS]
        for k in (1, 2, 3):
            summed = summed + taps[k : k + 1] * history[k * NS : (k + NP) * NS]
        return silu(summed)

    rate = -jnp.exp(alog[...])
    path_xs = window(past(cx, px), wtx[...].astype(F32))
    path_bs = window(past(cb, pb), wtb[...].astype(F32))
    path_step = softplus(pdt[...].astype(F32) + bias[...])
    live = ((iota((NP * NS, 1), 0) // NS).astype(F32) < taken_in[0 : NP * NS]).astype(F32)
    path_log = path_step * rate * live
    tails = [jnp.zeros((NS, NH), F32)]
    for j in range(NP - 1, 0, -1):
        tails.insert(0, tails[0] + path_log[j * NS : (j + 1) * NS])
    overall = jnp.exp(tails[0] + path_log[0:NS])
    weights = live * jnp.exp(jnp.concatenate(tails, axis=0)) * path_step
    weighted = (path_xs * widen(weights)).astype(BF16)
    path_seq = lax.rem(iota((NP * NS, 128), 0), NS)

    def forward(p):
        settle(wg.at[0], w_r.at[p, 0])
        w_pass(p).start()

    forward(0)
    settle(wown.at[pl.ds(1, 5)], l_s.at[4])
    w_send(1)
    w_send(2)
    tg[pl.ds(x, 1)] = tok[:, :, pl.ds(x, 1)].reshape(1, NQ, NZ, NS, 128)
    for p in range(6):
        wg[pl.ds(4 * p + x, 1)] = wown[pl.ds(p, 1)]
    wog[pl.ds(z, 1)] = wo[...].reshape(1, 512, 128)
    load(2).wait()

    def rescale(d):
        xs = wrap(x - d, NX)
        values = tg[pl.ds(xs, 1)].reshape(NQ * NZ * NS, 128).astype(F32)
        scaled = (values * gain[pl.ds(z * NX + xs, 1), :]).astype(BF16)
        ts[:, :, :, depth_of(xs)] = scaled.reshape(NQ, NZ, NS, 128)
        return values * values

    squares = rescale(0)
    o_step(2, 0)

    gained = []
    for g in range(2):
        split_b = jnp.concatenate(
            [
                jnp.where(path_seq == s, path_bs[:, 128 * g : 128 * g + 128], 0.0)
                for s in range(NS)
            ],
            axis=1,
        ).astype(BF16)
        gained.append(dot_of(weighted[:, 256 * g : 256 * g + 256], split_b, (0, 0)))
    o_step(2, 1)
    for s in range(NS):
        if s % 4 == 0:
            settle(held.at[pl.ds(s, 4)], s_s.at[s // 4])
        at = slice(128 * s, 128 * s + 128)
        for g in range(2):
            wide = slice(256 * g, 256 * g + 256)
            fade = jnp.concatenate(
                [
                    jnp.broadcast_to(overall[s : s + 1, h : h + 1], (64, 128))
                    for h in range(4 * g, 4 * g + 4)
                ],
                axis=0,
            )
            now = fade * held[s, wide, :] + gained[g][:, at]
            held[s, wide, :] = now
            fresh[g, :, at] = now.astype(BF16)
        save_state(s).start()

    def tree_conv(history, own, taps):
        values = jnp.concatenate([history, own], axis=0).astype(BF16)
        summed = taps[3:4] * own
        for k, far in ((2, one), (1, two), (0, three)):
            summed = summed + taps[k : k + 1] * dot(far, values)
        return silu(summed)

    for d in order:
        settle(tg.at[0, :, half], t_r.at[d - 1])
        tok_share(d).start()
    o_step(3, 0)

    def multiply(p):
        settle(wg.at[pl.ds(0, 2)], w_r.at[p, 1])
        prod[p] = jnp.dot(
            ts[...].reshape(NQ * NZ * NS, 512),
            wg[4 * p : 4 * p + 4].reshape(512, 256),
            preferred_element_type=F32,
        ).reshape(NQ, NZ, NS, 256)
        r_step(p, 1)

    for d in order:
        if d == 3:
            forward(1)
            w_send(3)
        settle(tg.at[0, :, half], f_r.at[d - 1])
        squares = squares + rescale(d)
    multiply(0)
    o_step(3, 1)
    forward(2)
    w_send(4)
    multiply(1)
    forward(3)
    w_send(5)
    tall = jnp.concatenate([wr[...].astype(F32), jnp.zeros((8, 512), F32)], axis=0).astype(BF16)
    squares = squares.reshape(NQ, NZ, NS, 128)
    for dest in range(NZ):
        rates = dot_of(tall, ts[:, dest].reshape(count, 512), (1, 1))
        square = squares[:, dest].reshape(count, 128)
        above = square.astype(BF16)
        both = jnp.concatenate([above, (square - above.astype(F32)).astype(BF16)], axis=1)
        sums = dot_of(jnp.ones((16, 256), BF16), both, (1, 1))
        aprod[dest] = jnp.where(iota((16, count), 0) == NH, sums, rates)
    r_step(6, 1)
    r_step(0, 2)
    multiply(2)
    forward(4)
    r_step(1, 2)
    multiply(3)
    forward(5)
    o_step(4, 0)
    r_step(2, 2)
    r_step(6, 2)
    multiply(4)
    r_step(3, 2)
    multiply(5)
    r_step(0, 3)
    r_step(4, 2)
    r_step(6, 3)
    r_step(1, 3)
    r_step(5, 2)
    r_step(2, 3)
    settle(wog.at[0], o_r.at[6])
    for k in range(NZ):
        at = 512 * (k % 2) + 128 * (k // 2)
        woc[:, at : at + 128] = wog[k]
    r_step(3, 3)
    r_step(6, 4)
    r_step(4, 3)
    r_step(0, 4)
    r_step(5, 3)
    r_step(1, 4)
    r_step(2, 4)

    total = r_total(6)
    scale = lax.rsqrt(dot_of(eye, total, (1, 1), HIGH)[:, NH : NH + 1] / (NZ * NX * 128.0) + EPS)
    scale_t = lax.rsqrt(total[NH : NH + 1] / (NZ * NX * 128.0) + EPS)
    step_t = softplus((total[0:NH] * scale_t).astype(BF16).astype(F32) + upright(bias))
    slope_t = step_t * -jnp.exp(upright(alog))
    decay = dot_of(family, slope_t, (1, 1), HIGH)
    decay_t = dot_of(slope_t, family, (1, 1), HIGH)
    grown = widen(jnp.exp(decay))
    skip = widen(jnp.broadcast_to(dskip[...], (NS, NH)))[0:1]

    seq_of = lax.rem(iota((count, 128), 0), NS)
    side = iota((count, 128), 1)

    def scaled_rows(p):
        return (r_total(p) * scale).astype(BF16).astype(F32)

    def heads_of(g):
        wide, narrow = slice(256 * g, 256 * g + 256), slice(128 * g, 128 * g + 128)
        history = jnp.concatenate(
            [past(cx, px)[:, wide], past(cb, pb)[:, narrow], past(cc, pc)[:, narrow]], axis=1
        )
        taps = jnp.concatenate([wtx[:, wide], wtb[:, narrow], wtc[:, narrow]], axis=1)
        own = jnp.concatenate([scaled_rows(3 * g), scaled_rows(3 * g + 1)], axis=1)
        post = tree_conv(history, own, taps.astype(F32))
        post_b, post_c = post[:, 256:384].astype(BF16), post[:, 384:512].astype(BF16)
        post_x = post[:, 0:256].astype(BF16)
        split_c = jnp.concatenate(
            [jnp.where(seq_of == s, post_c.astype(F32), 0.0) for s in range(NS)], axis=1
        ).astype(BF16)
        carried = dot_of(split_c, fresh[g], (1, 1))
        scores = dot_of(post_c, post_b, (1, 1))
        within = []
        for pair in range(2):
            sides = []
            for h in (4 * g + 2 * pair, 4 * g + 2 * pair + 1):
                gap = decay[:, h : h + 1] - decay_t[h : h + 1, :]
                mixing = jnp.exp(jnp.where(is_kin, gap, 0.0)) * step_t[h : h + 1, :]
                mixing = jnp.where(is_kin, scores * mixing, 0.0)
                sides.append(dot(mixing, post_x[:, 128 * pair : 128 * pair + 128]))
            within.append(jnp.where(side < 64, sides[0], sides[1]))
        heads = carried * grown[:, wide] + jnp.concatenate(within, axis=1)
        return heads + skip[:, wide] * post[:, 0:256]

    def gate(g, heads):
        heads = heads * silu(scaled_rows(3 * g + 2))
        spread_of = jnp.sum(heads * heads, axis=1, keepdims=True) / 256.0
        heads = heads * lax.rsqrt(spread_of + EPS) * gain_out[:, 256 * g : 256 * g + 256]
        gated[g] = heads.astype(BF16)

    def g_copy(g, d):
        return remote(
            gated.at[g],
            gg.at[g, d - 1],
            g_s,
            g_r.at[0 if g == 0 else d],
            {"x": wrap(x + d, NX)},
        )

    def product(g, d, columns):
        values = gated[g] if d == 0 else gg[g, d - 1]
        return jnp.dot(
            values, woc[256 * g : 256 * g + 256, columns], preferred_element_type=F32
        )

    def d_copy(d):
        return remote(given.at[d], taken.at[d], d_s, d_r.at[d], {"c": 1 - c})

    def p_copy(d, e):
        to_y = wrap(y + e, NY)
        return remote(
            part.at[d, to_y],
            terms.at[x * NY + y],
            p_s,
            p_r,
            {"x": wrap(x - d, NX), "y": to_y},
        )

    mine = pl.ds(pl.multiple_of(512 * c, 512), 512)
    other = pl.ds(pl.multiple_of(512 * (1 - c), 512), 512)

    r_step(3, 4)
    r_step(4, 4)
    first = heads_of(0)
    r_step(5, 4)
    gate(0, first)
    for d in order:
        g_copy(0, d).start()
    gate(1, heads_of(1))
    for d in order:
        g_copy(1, d).start()
    def begin(d):
        hold[d] = product(0, d, other)
        kept[d] = product(0, d, mine)

    def finish(d):
        if d > 0:
            settle(gg.at[1, d - 1], g_r.at[d])
        given[d] = (hold[d] + product(1, d, other)).astype(BF16)
        d_copy(d).start()
        kept[d] = kept[d] + product(1, d, mine)

    def deliver(d):
        settle(taken.at[d], d_r.at[d])
        both = (kept[d] + taken[d].astype(F32)).astype(BF16)
        for to in range(NY):
            part[d, to] = both[:, 128 * to : 128 * to + 128]
        for e in (2, 1, 3, 0):
            if d + e > 0:
                p_copy(d, e).start()

    begin(0)
    finish(0)
    settle(gg.at[0], g_r.at[0])
    for d in order:
        begin(d)
    deliver(0)
    terms[pl.ds(x * NY + y, 1)] = part[0, pl.ds(y, 1)]
    finish(2)
    finish(1)
    deliver(2)
    finish(3)
    deliver(1)
    deliver(3)
    settle(terms.at[pl.ds(0, 15)], p_r)
    for xs in range(NX):
        total = terms[xs * NY].astype(F32)
        for k in range(1, NY):
            total = total + terms[xs * NY + k].astype(F32)
        mixed[:, xs * 128 : (xs + 1) * 128] = total.astype(BF16)

    settle(held, n_s)
    settle(wog.at[pl.ds(0, 7)], o_s)
    settle(tg.at[pl.ds(0, 3)], t_s)
    settle(wg.at[pl.ds(0, 18)], w_s)
    settle(ring, r_s)
    settle(aring, a_s)
    settle(gg, g_s)
    settle(given, d_s)
    settle(terms.at[pl.ds(0, 15)], p_s)


def mixer(*args):
    vmem = pl.BlockSpec(memory_space=pltpu.VMEM)
    far = pl.BlockSpec(memory_space=pl.ANY)
    dma = pltpu.SemaphoreType.DMA
    rows = NQ * NS
    return pl.pallas_call(
        mixer_kernel,
        name="mixer",
        out_shape=(
            jax.ShapeDtypeStruct((rows, 512), BF16),
            jax.ShapeDtypeStruct((NS, 512, 128), F32),
        ),
        in_specs=[far] * 8 + [vmem] * (len(args) - 8),
        out_specs=(vmem, far),
        scratch_shapes=[
            pltpu.VMEM((NQ, NZ, NX, NS, 128), BF16),
            pltpu.VMEM((6, 128, 256), BF16),
            pltpu.VMEM((NH, 512), BF16),
            pltpu.VMEM((512, 128), BF16),
            pltpu.VMEM((NS, 512, 128), F32),
            pltpu.VMEM((2, 256, 1024), BF16),
            pltpu.VMEM((NX, NQ, NZ, NS, 128), BF16),
            pltpu.VMEM((NQ, NZ, NS, 512), BF16),
            pltpu.VMEM((24, 128, 256), BF16),
            pltpu.VMEM((NZ, 512, 128), BF16),
            pltpu.VMEM((6, NQ, NZ, NS, 256), F32),
            pltpu.VMEM((NZ, 16, rows), F32),
            pltpu.VMEM((6, 7, NQ, NS, 256), BF16),
            pltpu.VMEM((7, 16, rows), BF16),
            pltpu.VMEM((6, 2, NQ, NS, 256), BF16),
            pltpu.VMEM((2, 16, rows), BF16),
            pltpu.VMEM((2, rows, 256), BF16),
            pltpu.VMEM((2, 3, rows, 256), BF16),
            pltpu.VMEM((512, 1024), BF16),
            pltpu.VMEM((NX, rows, 512), F32),
            pltpu.VMEM((NX, rows, 512), F32),
            pltpu.VMEM((NX, rows, 512), BF16),
            pltpu.VMEM((NX, rows, 512), BF16),
            pltpu.VMEM((NX, NY, rows, 128), BF16),
            pltpu.VMEM((NX * NY, rows, 128), BF16),
            dma((5,)),
            dma((2,)),
            dma,
            dma,
            dma((3,)),
            dma((3,)),
            dma,
            dma((6, 2)),
            dma,
            dma,
            dma((7, 4)),
            dma,
            dma((7,)),
            dma,
            dma((4,)),
            dma,
            dma((NX,)),
            dma,
            dma,
        ],
        compiler_params=pltpu.CompilerParams(
            collective_id=0, has_side_effects=True, vmem_limit_bytes=VMEM_LIMIT
        ),
    )(*args)


def finish_kernel(mixed_h, state_h, mixed_o, state_o, small, large, in_s, out_s):
    def steps(k):
        if k == NS:
            return mixed_h, small, mixed_o
        return state_h.at[k], large.at[k], state_o.at[k]

    def load(k):
        return pltpu.make_async_copy(steps(k)[0], steps(k)[1], in_s.at[k])

    def save(k):
        return pltpu.make_async_copy(steps(k)[1], steps(k)[2], out_s.at[k])

    for k in range(NS + 1):
        load(k).start()
    for k in range(NS + 1):
        load(k).wait()
        save(k).start()
    for k in range(NS + 1):
        save(k).wait()


def finish(mixed, new_state):
    far = pl.BlockSpec(memory_space=pltpu.HBM)
    return pl.pallas_call(
        finish_kernel,
        name="finish",
        out_shape=(
            jax.ShapeDtypeStruct(mixed.shape, mixed.dtype),
            jax.ShapeDtypeStruct(new_state.shape, new_state.dtype),
        ),
        in_specs=[far, far],
        out_specs=(far, far),
        scratch_shapes=[
            pltpu.VMEM(mixed.shape, mixed.dtype),
            pltpu.VMEM(new_state.shape, new_state.dtype),
            pltpu.SemaphoreType.DMA((NS + 1,)),
            pltpu.SemaphoreType.DMA((NS + 1,)),
        ],
        compiler_params=pltpu.CompilerParams(vmem_limit_bytes=VMEM_LIMIT),
    )(mixed, new_state)


def by_place(v):
    v = jnp.transpose(v, (1, 0, 2))
    return v.reshape(v.shape[0] * v.shape[1], v.shape[2])


def shards(
    tokens,
    parents,
    accepted,
    state,
    conv_x,
    conv_b,
    conv_c,
    path_x,
    path_b,
    path_c,
    path_dt,
    gain_in,
    w_x,
    w_z,
    w_b,
    w_c,
    w_dt,
    dt_bias,
    a_log,
    d_skip,
    conv_wx,
    conv_wb,
    conv_wc,
    gain_out,
    w_out,
):
    tok = jnp.transpose(tokens, (1, 0, 2)).reshape(NQ, NZ, NX, NS, 128)
    conv_x, path_x = by_place(conv_x), by_place(path_x)
    conv_b, path_b = by_place(conv_b), by_place(path_b)
    conv_c, path_c = by_place(conv_c), by_place(path_c)
    accepted, dt_bias, a_log = accepted[None, :], dt_bias[None, :], a_log[None, :]
    mixed, new_state = mixer(
        tok,
        w_x,
        w_z,
        w_b,
        w_c,
        w_dt.T,
        w_out,
        state.reshape(NS, 512, 128),
        gain_in.reshape(32, 128),
        parents,
        accepted,
        conv_x,
        path_x,
        conv_b,
        path_b,
        conv_c,
        path_c,
        by_place(path_dt),
        dt_bias,
        a_log,
        d_skip[None, :],
        conv_wx,
        conv_wb,
        conv_wc,
        gain_out[None, :],
    )
    mixed, new_state = finish(mixed, new_state)
    mixed = jnp.transpose(mixed.reshape(NQ, NS, 512), (1, 0, 2))
    return (mixed, new_state.reshape(NS, NH, 64, 128))


def solution(mesh):
    finer = Mesh(mesh.devices.reshape(NZ, NX, NY, NC), ("z", "x", "y", "c"))
    return jax.shard_map(
        shards,
        mesh=finer,
        in_specs=(
            P(None, None, KV),
            P(KV, None),
            P(KV),
            P(KV, TP, None, None),
            P(KV, None, TP),
            P(KV, None, TP),
            P(KV, None, TP),
            P(KV, None, TP),
            P(KV, None, TP),
            P(KV, None, TP),
            P(KV, None, TP),
            P(),
            P(KV, TP),
            P(KV, TP),
            P(KV, TP),
            P(KV, TP),
            P(),
            P(TP),
            P(TP),
            P(TP),
            P(None, TP),
            P(None, TP),
            P(None, TP),
            P(TP),
            P(TP, KV),
        ),
        out_specs=(P(KV, None, TP), P(KV, TP, None, None)),
        check_vma=False,
    )
```

```python
import functools

import jax
import jax.numpy as jnp
from jax import lax
from jax.experimental import pallas as pl
from jax.experimental.pallas import tpu as pltpu
from jax.sharding import Mesh
from jax.sharding import PartitionSpec as P

NZ, NX, NY, NC = 8, 4, 4, 2
NT = NY * NC
MESH = pl.DeviceIdType.MESH
KV = ("z", "x")
TP = ("y", "c")
EPS = 1e-06
HIGH = lax.Precision.HIGHEST
F32 = jnp.float32
BF16 = jnp.bfloat16
NQ, NS, NP, NH = 12, 8, 6, 8
VMEM_LIMIT = 40 * 1024 * 1024


def wrap(i, n):
    return lax.rem(i + n, n)


def remote(src, dst, send_sem, recv_sem, device):
    return pltpu.make_async_remote_copy(
        src_ref=src,
        dst_ref=dst,
        send_sem=send_sem,
        recv_sem=recv_sem,
        device_id=device,
        device_id_type=MESH,
    )


def greet(devices):
    barrier = pltpu.get_barrier_semaphore()
    for device in devices:
        pl.semaphore_signal(barrier, inc=1, device_id=device, device_id_type=MESH)
    pl.semaphore_wait(barrier, len(devices))


def settle(view, sem):
    pltpu.make_async_copy(view, view, sem).wait()


def hops_of(piece, way):
    return 4 if (piece % 2 == 0) == (way == 0) else 3


def slot_of(piece, way, hop):
    return (0, 2, 4, 5)[hop - 1] if hops_of(piece, way) == 4 else (1, 3, 6)[hop - 1]


def sem_of(piece, way, hop):
    return hop - 1 if hop < hops_of(piece, way) else 3


def silu(v):
    return v * (1.0 / (1.0 + jnp.exp(-v)))


def softplus(v):
    return jnp.maximum(v, 0.0) + jnp.log1p(jnp.exp(-jnp.abs(v)))


def iota(shape, dim):
    return lax.broadcasted_iota(jnp.int32, shape, dim)


def dot(a, b):
    return jnp.dot(a.astype(BF16), b.astype(BF16), preferred_element_type=F32)


def dot_of(a, b, dims, precision=None):
    return lax.dot_general(
        a, b, ((dims[:1], dims[1:]), ((), ())), precision=precision, preferred_element_type=F32
    )


def past(first, last):
    return jnp.concatenate([first[...].astype(F32), last[...].astype(F32)], axis=0)


def widen(v):
    spread = (iota((NH, 512), 1) // 64 == iota((NH, 512), 0)).astype(F32)
    return dot_of(v, spread, (1, 0), HIGH)


def upright(row):
    wide = jnp.broadcast_to(row[...].astype(F32), (NS, NS))
    return jnp.sum(
        jnp.where(iota((NS, NS), 0) == iota((NS, NS), 1), wide, 0.0), axis=1, keepdims=True
    )


def mixer_kernel(
    tok_h,
    wx_h,
    wz_h,
    wb_h,
    wc_h,
    wdt_h,
    wo_h,
    state_h,
    gain,
    parents,
    accepted,
    cx,
    px,
    cb,
    pb,
    cc,
    pc,
    pdt,
    bias,
    alog,
    dskip,
    wtx,
    wtb,
    wtc,
    gain_out,
    mixed,
    new_state,
    tok,
    wown,
    wr,
    wo,
    held,
    fresh,
    tg,
    ts,
    wg,
    wog,
    prod,
    aprod,
    ring,
    aring,
    stage,
    astage,
    gated,
    gg,
    woc,
    kept,
    hold,
    given,
    taken,
    part,
    terms,
    l_s,
    s_s,
    t_s,
    t_r,
    f_r,
    w_s,
    w_r,
    r_s,
    a_s,
    r_r,
    o_s,
    o_r,
    g_s,
    g_r,
    d_s,
    d_r,
    p_s,
    p_r,
):
    z, x = lax.axis_index("z"), lax.axis_index("x")
    y, c = lax.axis_index("y"), lax.axis_index("c")
    t = y * NC + c
    count = NQ * NS

    def depth_of(owner):
        return pl.ds(pl.multiple_of(owner * 128, 128), 128)

    lower, upper = slice(0, 128), slice(128, 256)
    loads = [(tok_h, tok, 0), (wo_h, wo, 1)]
    loads.append(
        (
            wdt_h.at[
                pl.ds(pl.multiple_of(t * NH, NH), NH), pl.ds(pl.multiple_of(z * 512, 512), 512)
            ],
            wr,
            2,
        )
    )
    for g in range(2):
        wide, narrow = slice(256 * g, 256 * g + 256), slice(128 * g, 128 * g + 128)
        loads.append((wx_h.at[:, wide], wown.at[3 * g], 3 + g))
        loads.append((wb_h.at[:, narrow], wown.at[3 * g + 1, :, lower], 4))
        loads.append((wc_h.at[:, narrow], wown.at[3 * g + 1, :, upper], 4))
        loads.append((wz_h.at[:, wide], wown.at[3 * g + 2], 4))

    def load(k):
        return pltpu.make_async_copy(loads[k][0], loads[k][1], l_s.at[loads[k][2]])

    def load_state(s):
        return pltpu.make_async_copy(state_h.at[s], held.at[s], s_s.at[s // 4])

    for k in (3, 0, 1, 4, 5, 6, 2, 7, 8, 9, 10):
        load(k).start()
    for s in range(NS):
        load_state(s).start()
    plane = [(d, e) for d in range(NX) for e in range(NY) if d + e > 0]
    greet(
        [{"x": wrap(x + d, NX), "y": wrap(y + e, NY)} for d, e in plane]
        + [{"z": wrap(z + 1, NZ)}, {"z": wrap(z - 1, NZ)}, {"c": 1 - c}]
    )
    half = pl.ds(4 * c, 4)

    def tok_copy(d):
        to = wrap(x + d, NX)
        return remote(
            tok.at[:, half, to], tg.at[x, :, half], t_s, t_r.at[d - 1], {"x": to}
        )

    def tok_share(d):
        block = tg.at[wrap(x - d, NX), :, half]
        return remote(block, block, t_s, f_r.at[d - 1], {"c": 1 - c})

    def w_own(p, way):
        to = wrap(x + (1 if way == 0 else -1), NX)
        last = 0 if way == p % 2 else 1
        return remote(wown.at[p], wg.at[4 * p + x], w_s, w_r.at[p, last], {"x": to})

    def w_pass(p):
        sign = 1 if p % 2 == 0 else -1
        block = wg.at[4 * p + wrap(x - sign, NX)]
        return remote(block, block, w_s, w_r.at[p, 1], {"x": wrap(x + sign, NX)})

    def o_step(hop, side):
        for way in (0, 1):
            if hop == 4:
                side = way
            if hop == 4 or (hop > 1 and way == 0):
                settle(wog.at[0], o_r.at[2 * (hop - 2) + side])
            sign = 1 if way == 0 else -1
            owner = wrap(z - sign * (hop - 1), NZ)
            part = pl.ds(256 * side, 256)
            src = wo.at[part] if hop == 1 else wog.at[owner, part]
            to = {"z": wrap(z + sign, NZ)}
            at = 6 if hop == 4 else 2 * (hop - 1) + side
            sends.append(remote(src, wog.at[owner, part], o_s, o_r.at[at], to))
        for copy in sends[-2:]:
            copy.start()

    sends = []

    def r_copy(p, way, hop):
        to = {"z": wrap(z + (1 if way == 0 else -1), NZ)}
        buffer = aring if p == 6 else ring.at[p]
        dst = buffer.at[slot_of(p, way, hop)]
        if hop > 1:
            src = buffer.at[slot_of(p, way, hop - 1)]
        else:
            src = astage.at[way] if p == 6 else stage.at[p, way]
        return remote(src, dst, a_s if p == 6 else r_s, r_r.at[p, sem_of(p, way, hop)], to)

    def r_wait(p, index):
        buffer = aring if p == 6 else ring.at[p]
        first, many = ((0, 2), (2, 2), (4, 1), (5, 2))[index]
        settle(buffer.at[pl.ds(first, many)], r_r.at[p, index])

    def own_term(p, dest):
        if p == 6:
            return aprod[pl.ds(dest, 1)].reshape(16, count)
        return prod[p, :, pl.ds(dest, 1)].reshape(NQ, NS, 256)

    def r_step(p, hop):
        if hop > 1:
            r_wait(p, hop - 2)
        for way in (0, 1):
            hops = hops_of(p, way)
            if hop > hops:
                continue
            sign = 1 if way == 0 else -1
            term = own_term(p, wrap(z + sign * (hops + 1 - hop), NZ))
            if hop == 1:
                if p == 6:
                    astage[way] = term.astype(BF16)
                else:
                    stage[p, way] = term.astype(BF16)
            else:
                at = slot_of(p, way, hop - 1)
                if p == 6:
                    aring[at] = (aring[at].astype(F32) + term).astype(BF16)
                else:
                    ring[p, at] = (ring[p, at].astype(F32) + term).astype(BF16)
            r_copy(p, way, hop).start()

    def r_total(p):
        r_wait(p, 3)
        if p == 6:
            return own_term(p, z) + aring[5].astype(F32) + aring[6].astype(F32)
        total = own_term(p, z) + ring[p, 5].astype(F32) + ring[p, 6].astype(F32)
        return total.reshape(count, 256)

    order = (2, 1, 3)

    def w_send(p):
        w_own(p, p % 2).start()
        w_own(p, 1 - p % 2).start()

    load(3).wait()
    w_send(0)
    load(0).wait()
    for d in order:
        tok_copy(d).start()
    load(1).wait()
    o_step(1, 0)
    o_step(1, 1)

    up = jnp.concatenate([parents[:, q : q + 1] for q in range(NQ)], axis=0).astype(F32)
    taken_in = jnp.concatenate([upright(accepted)] * NQ, axis=0)
    seq = lax.rem(iota((count, 1), 0), NS).astype(F32)
    is_root = up < 0.0
    nodes = iota((count, 9 * NS + count), 1).astype(F32)

    def reach(back, other):
        return jnp.where(is_root, (taken_in + back) * NS + seq, other)

    at_kin = up * NS + seq
    kin = iota((count, count), 1).astype(F32)
    links = (kin == jnp.where(is_root, -1.0, at_kin)).astype(F32)
    eye = (iota((count, count), 0) == iota((count, count), 1)).astype(F32)
    family = eye + links
    for _ in range(4):
        family = jnp.minimum(dot(family, family), 1.0)
    is_kin = family > 0.5
    one = (nodes == reach(2.0, 9.0 * NS + at_kin)).astype(F32)
    two = dot(links, one) + (nodes == reach(1.0, -1.0)).astype(F32)
    three = dot(links, two) + (nodes == reach(0.0, -1.0)).astype(F32)
    one, two, three = one.astype(BF16), two.astype(BF16), three.astype(BF16)

    def window(history, taps):
        summed = taps[0:1] * history[0 : NP * NS]
        for k in (1, 2, 3):
            summed = summed + taps[k : k + 1] * history[k * NS : (k + NP) * NS]
        return silu(summed)

    rate = -jnp.exp(alog[...])
    path_xs = window(past(cx, px), wtx[...].astype(F32))
    path_bs = window(past(cb, pb), wtb[...].astype(F32))
    path_step = softplus(pdt[...].astype(F32) + bias[...])
    live = ((iota((NP * NS, 1), 0) // NS).astype(F32) < taken_in[0 : NP * NS]).astype(F32)
    path_log = path_step * rate * live
    tails = [jnp.zeros((NS, NH), F32)]
    for j in range(NP - 1, 0, -1):
        tails.insert(0, tails[0] + path_log[j * NS : (j + 1) * NS])
    overall = jnp.exp(tails[0] + path_log[0:NS])
    weights = live * jnp.exp(jnp.concatenate(tails, axis=0)) * path_step
    weighted = (path_xs * widen(weights)).astype(BF16)
    path_seq = lax.rem(iota((NP * NS, 128), 0), NS)

    def forward(p):
        settle(wg.at[0], w_r.at[p, 0])
        w_pass(p).start()

    forward(0)
    settle(wown.at[pl.ds(1, 5)], l_s.at[4])
    w_send(1)
    w_send(2)
    tg[pl.ds(x, 1)] = tok[:, :, pl.ds(x, 1)].reshape(1, NQ, NZ, NS, 128)
    for p in range(6):
        wg[pl.ds(4 * p + x, 1)] = wown[pl.ds(p, 1)]
    wog[pl.ds(z, 1)] = wo[...].reshape(1, 512, 128)
    load(2).wait()

    def rescale(d):
        xs = wrap(x - d, NX)
        values = tg[pl.ds(xs, 1)].reshape(NQ * NZ * NS, 128).astype(F32)
        scaled = (values * gain[pl.ds(z * NX + xs, 1), :]).astype(BF16)
        ts[:, :, :, depth_of(xs)] = scaled.reshape(NQ, NZ, NS, 128)
        return values * values

    squares = rescale(0)
    o_step(2, 0)

    gained = []
    for g in range(2):
        split_b = jnp.concatenate(
            [
                jnp.where(path_seq == s, path_bs[:, 128 * g : 128 * g + 128], 0.0)
                for s in range(NS)
            ],
            axis=1,
        ).astype(BF16)
        gained.append(dot_of(weighted[:, 256 * g : 256 * g + 256], split_b, (0, 0)))
    o_step(2, 1)
    for s in range(NS):
        if s % 4 == 0:
            settle(held.at[pl.ds(s, 4)], s_s.at[s // 4])
        at = slice(128 * s, 128 * s + 128)
        for g in range(2):
            wide = slice(256 * g, 256 * g + 256)
            fade = jnp.concatenate(
                [
                    jnp.broadcast_to(overall[s : s + 1, h : h + 1], (64, 128))
                    for h in range(4 * g, 4 * g + 4)
                ],
                axis=0,
            )
            now = fade * held[s, wide, :] + gained[g][:, at]
            new_state[s, wide, :] = now
            fresh[g, :, at] = now.astype(BF16)

    def tree_conv(history, own, taps):
        values = jnp.concatenate([history, own], axis=0).astype(BF16)
        summed = taps[3:4] * own
        for k, far in ((2, one), (1, two), (0, three)):
            summed = summed + taps[k : k + 1] * dot(far, values)
        return silu(summed)

    for d in order:
        settle(tg.at[0, :, half], t_r.at[d - 1])
        tok_share(d).start()

    def multiply(p):
        settle(wg.at[pl.ds(0, 2)], w_r.at[p, 1])
        prod[p] = jnp.dot(
            ts[...].reshape(NQ * NZ * NS, 512),
            wg[4 * p : 4 * p + 4].reshape(512, 256),
            preferred_element_type=F32,
        ).reshape(NQ, NZ, NS, 256)
        r_step(p, 1)

    for d in order:
        if d == 3:
            forward(1)
            w_send(3)
            o_step(3, 0)
        settle(tg.at[0, :, half], f_r.at[d - 1])
        squares = squares + rescale(d)
    multiply(0)
    o_step(3, 1)
    forward(2)
    w_send(4)
    multiply(1)
    forward(3)
    w_send(5)
    tall = jnp.concatenate([wr[...].astype(F32), jnp.zeros((8, 512), F32)], axis=0).astype(BF16)
    squares = squares.reshape(NQ, NZ, NS, 128)
    for dest in range(NZ):
        rates = dot_of(tall, ts[:, dest].reshape(count, 512), (1, 1))
        square = squares[:, dest].reshape(count, 128)
        above = square.astype(BF16)
        both = jnp.concatenate([above, (square - above.astype(F32)).astype(BF16)], axis=1)
        sums = dot_of(jnp.ones((16, 256), BF16), both, (1, 1))
        aprod[dest] = jnp.where(iota((16, count), 0) == NH, sums, rates)
    r_step(6, 1)
    r_step(0, 2)
    multiply(2)
    forward(4)
    r_step(1, 2)
    multiply(3)
    forward(5)
    o_step(4, 0)
    r_step(2, 2)
    r_step(6, 2)
    multiply(4)
    r_step(3, 2)
    multiply(5)
    r_step(6, 3)
    r_step(0, 3)
    r_step(4, 2)
    r_step(1, 3)
    r_step(5, 2)
    r_step(6, 4)
    r_step(2, 3)
    settle(wog.at[0], o_r.at[6])
    for k in range(NZ):
        at = 512 * (k % 2) + 128 * (k // 2)
        woc[:, at : at + 128] = wog[k]
    r_step(3, 3)
    r_step(4, 3)
    r_step(0, 4)
    r_step(5, 3)
    r_step(1, 4)
    r_step(2, 4)

    seq_of = lax.rem(iota((count, 128), 0), NS)
    side = iota((count, 128), 1)

    def scaled_rows(p):
        return (r_total(p) * scale).astype(BF16).astype(F32)

    def heads_of(g):
        wide, narrow = slice(256 * g, 256 * g + 256), slice(128 * g, 128 * g + 128)
        history = jnp.concatenate(
            [past(cx, px)[:, wide], past(cb, pb)[:, narrow], past(cc, pc)[:, narrow]], axis=1
        )
        taps = jnp.concatenate([wtx[:, wide], wtb[:, narrow], wtc[:, narrow]], axis=1)
        own = jnp.concatenate([scaled_rows(3 * g), scaled_rows(3 * g + 1)], axis=1)
        post = tree_conv(history, own, taps.astype(F32))
        post_b, post_c = post[:, 256:384].astype(BF16), post[:, 384:512].astype(BF16)
        post_x = post[:, 0:256].astype(BF16)
        split_c = jnp.concatenate(
            [jnp.where(seq_of == s, post_c.astype(F32), 0.0) for s in range(NS)], axis=1
        ).astype(BF16)
        carried = dot_of(split_c, fresh[g], (1, 1))
        scores = dot_of(post_c, post_b, (1, 1))
        within = []
        for pair in range(2):
            sides = []
            for h in (4 * g + 2 * pair, 4 * g + 2 * pair + 1):
                gap = decay[:, h : h + 1] - decay_t[h : h + 1, :]
                mixing = jnp.exp(jnp.where(is_kin, gap, 0.0)) * step_t[h : h + 1, :]
                mixing = jnp.where(is_kin, scores * mixing, 0.0)
                sides.append(dot(mixing, post_x[:, 128 * pair : 128 * pair + 128]))
            within.append(jnp.where(side < 64, sides[0], sides[1]))
        heads = carried * grown[:, wide] + jnp.concatenate(within, axis=1)
        return heads + skip[:, wide] * post[:, 0:256]

    def gate(g, heads):
        heads = heads * silu(scaled_rows(3 * g + 2))
        spread_of = jnp.sum(heads * heads, axis=1, keepdims=True) / 256.0
        heads = heads * lax.rsqrt(spread_of + EPS) * gain_out[:, 256 * g : 256 * g + 256]
        gated[g] = heads.astype(BF16)

    def g_copy(g, d):
        return remote(
            gated.at[g],
            gg.at[g, d - 1],
            g_s,
            g_r.at[0 if g == 0 else d],
            {"x": wrap(x + d, NX)},
        )

    def product(g, d, columns):
        values = gated[g] if d == 0 else gg[g, d - 1]
        return jnp.dot(
            values, woc[256 * g : 256 * g + 256, columns], preferred_element_type=F32
        )

    def d_copy(d):
        return remote(given.at[d], taken.at[d], d_s, d_r.at[d], {"c": 1 - c})

    def p_copy(d, e):
        to_y = wrap(y + e, NY)
        return remote(
            part.at[d, to_y],
            terms.at[x * NY + y],
            p_s,
            p_r,
            {"x": wrap(x - d, NX), "y": to_y},
        )

    mine = pl.ds(pl.multiple_of(512 * c, 512), 512)
    other = pl.ds(pl.multiple_of(512 * (1 - c), 512), 512)

    r_step(3, 4)
    r_step(4, 4)
    total = r_total(6)
    scale = lax.rsqrt(dot_of(eye, total, (1, 1), HIGH)[:, NH : NH + 1] / (NZ * NX * 128.0) + EPS)
    scale_t = lax.rsqrt(total[NH : NH + 1] / (NZ * NX * 128.0) + EPS)
    step_t = softplus((total[0:NH] * scale_t).astype(BF16).astype(F32) + upright(bias))
    slope_t = step_t * -jnp.exp(upright(alog))
    decay = dot_of(family, slope_t, (1, 1), HIGH)
    decay_t = dot_of(slope_t, family, (1, 1), HIGH)
    grown = widen(jnp.exp(decay))
    skip = widen(jnp.broadcast_to(dskip[...], (NS, NH)))[0:1]
    first = heads_of(0)
    r_step(5, 4)
    gate(0, first)
    for d in order:
        g_copy(0, d).start()
    gate(1, heads_of(1))
    for d in order:
        g_copy(1, d).start()
    def begin(d):
        hold[d] = product(0, d, other)
        kept[d] = product(0, d, mine)

    def finish(d):
        if d > 0:
            settle(gg.at[1, d - 1], g_r.at[d])
        given[d] = (hold[d] + product(1, d, other)).astype(BF16)
        d_copy(d).start()
        kept[d] = kept[d] + product(1, d, mine)

    def deliver(d):
        settle(taken.at[d], d_r.at[d])
        both = (kept[d] + taken[d].astype(F32)).astype(BF16)
        for to in range(NY):
            part[d, to] = both[:, 128 * to : 128 * to + 128]
        for e in (2, 1, 3, 0):
            if d + e > 0:
                p_copy(d, e).start()

    begin(0)
    finish(0)
    settle(gg.at[0], g_r.at[0])
    for d in order:
        begin(d)
    deliver(0)
    terms[pl.ds(x * NY + y, 1)] = part[0, pl.ds(y, 1)]
    finish(2)
    finish(1)
    deliver(2)
    finish(3)
    deliver(1)
    deliver(3)
    settle(terms.at[pl.ds(0, 15)], p_r)
    for xs in range(NX):
        total = terms[xs * NY].astype(F32)
        for k in range(1, NY):
            total = total + terms[xs * NY + k].astype(F32)
        mixed[:, xs * 128 : (xs + 1) * 128] = total.astype(BF16)

    settle(wog.at[pl.ds(0, 7)], o_s)
    settle(tg.at[pl.ds(0, 3)], t_s)
    settle(wg.at[pl.ds(0, 18)], w_s)
    settle(ring, r_s)
    settle(aring, a_s)
    settle(gg, g_s)
    settle(given, d_s)
    settle(terms.at[pl.ds(0, 15)], p_s)


def mixer(*args):
    vmem = pl.BlockSpec(memory_space=pltpu.VMEM)
    far = pl.BlockSpec(memory_space=pltpu.HBM)
    dma = pltpu.SemaphoreType.DMA
    rows = NQ * NS
    return pl.pallas_call(
        mixer_kernel,
        name="mixer",
        out_shape=(
            jax.ShapeDtypeStruct((rows, 512), BF16),
            jax.ShapeDtypeStruct((NS, 512, 128), F32),
        ),
        in_specs=[far] * 8 + [vmem] * (len(args) - 8),
        out_specs=(vmem, vmem),
        scratch_shapes=[
            pltpu.VMEM((NQ, NZ, NX, NS, 128), BF16),
            pltpu.VMEM((6, 128, 256), BF16),
            pltpu.VMEM((NH, 512), BF16),
            pltpu.VMEM((512, 128), BF16),
            pltpu.VMEM((NS, 512, 128), F32),
            pltpu.VMEM((2, 256, 1024), BF16),
            pltpu.VMEM((NX, NQ, NZ, NS, 128), BF16),
            pltpu.VMEM((NQ, NZ, NS, 512), BF16),
            pltpu.VMEM((24, 128, 256), BF16),
            pltpu.VMEM((NZ, 512, 128), BF16),
            pltpu.VMEM((6, NQ, NZ, NS, 256), F32),
            pltpu.VMEM((NZ, 16, rows), F32),
            pltpu.VMEM((6, 7, NQ, NS, 256), BF16),
            pltpu.VMEM((7, 16, rows), BF16),
            pltpu.VMEM((6, 2, NQ, NS, 256), BF16),
            pltpu.VMEM((2, 16, rows), BF16),
            pltpu.VMEM((2, rows, 256), BF16),
            pltpu.VMEM((2, 3, rows, 256), BF16),
            pltpu.VMEM((512, 1024), BF16),
            pltpu.VMEM((NX, rows, 512), F32),
            pltpu.VMEM((NX, rows, 512), F32),
            pltpu.VMEM((NX, rows, 512), BF16),
            pltpu.VMEM((NX, rows, 512), BF16),
            pltpu.VMEM((NX, NY, rows, 128), BF16),
            pltpu.VMEM((NX * NY, rows, 128), BF16),
            dma((5,)),
            dma((2,)),
            dma,
            dma((3,)),
            dma((3,)),
            dma,
            dma((6, 2)),
            dma,
            dma,
            dma((7, 4)),
            dma,
            dma((7,)),
            dma,
            dma((4,)),
            dma,
            dma((NX,)),
            dma,
            dma,
        ],
        compiler_params=pltpu.CompilerParams(
            collective_id=0, has_side_effects=True, vmem_limit_bytes=VMEM_LIMIT
        ),
    )(*(pltpu.with_memory_space_constraint(a, pltpu.HBM) for a in args))


def finish_kernel(mixed, state, mixed_o, state_o, out_s):
    def save(k):
        if k == NS:
            return pltpu.make_async_copy(mixed, mixed_o, out_s.at[1])
        return pltpu.make_async_copy(state.at[k], state_o.at[k], out_s.at[0])

    for k in range(NS + 1):
        save(k).start()
    settle(state, out_s.at[0])
    save(NS).wait()


def finish(mixed, new_state):
    far = pl.BlockSpec(memory_space=pltpu.HBM)
    near = pl.BlockSpec(memory_space=pltpu.VMEM)
    return pl.pallas_call(
        finish_kernel,
        name="finish",
        out_shape=(
            jax.ShapeDtypeStruct(mixed.shape, mixed.dtype),
            jax.ShapeDtypeStruct(new_state.shape, new_state.dtype),
        ),
        in_specs=[near, near],
        out_specs=(far, far),
        scratch_shapes=[pltpu.SemaphoreType.DMA((2,))],
        compiler_params=pltpu.CompilerParams(vmem_limit_bytes=8 * 1024 * 1024),
    )(mixed, new_state)


def by_place(v):
    v = jnp.transpose(v, (1, 0, 2))
    return v.reshape(v.shape[0] * v.shape[1], v.shape[2])


def shards(
    tokens,
    parents,
    accepted,
    state,
    conv_x,
    conv_b,
    conv_c,
    path_x,
    path_b,
    path_c,
    path_dt,
    gain_in,
    w_x,
    w_z,
    w_b,
    w_c,
    w_dt,
    dt_bias,
    a_log,
    d_skip,
    conv_wx,
    conv_wb,
    conv_wc,
    gain_out,
    w_out,
):
    tok = jnp.transpose(tokens, (1, 0, 2)).reshape(NQ, NZ, NX, NS, 128)
    conv_x, path_x = by_place(conv_x), by_place(path_x)
    conv_b, path_b = by_place(conv_b), by_place(path_b)
    conv_c, path_c = by_place(conv_c), by_place(path_c)
    accepted, dt_bias, a_log = accepted[None, :], dt_bias[None, :], a_log[None, :]
    mixed, new_state = mixer(
        tok,
        w_x,
        w_z,
        w_b,
        w_c,
        w_dt.T,
        w_out,
        state.reshape(NS, 512, 128),
        gain_in.reshape(32, 128),
        parents,
        accepted,
        conv_x,
        path_x,
        conv_b,
        path_b,
        conv_c,
        path_c,
        by_place(path_dt),
        dt_bias,
        a_log,
        d_skip[None, :],
        conv_wx,
        conv_wb,
        conv_wc,
        gain_out[None, :],
    )
    mixed, new_state = finish(mixed, new_state)
    mixed = jnp.transpose(mixed.reshape(NQ, NS, 512), (1, 0, 2))
    return (mixed, new_state.reshape(NS, NH, 64, 128))


def solution(mesh):
    finer = Mesh(mesh.devices.reshape(NZ, NX, NY, NC), ("z", "x", "y", "c"))
    return jax.shard_map(
        shards,
        mesh=finer,
        in_specs=(
            P(None, None, KV),
            P(KV, None),
            P(KV),
            P(KV, TP, None, None),
            P(KV, None, TP),
            P(KV, None, TP),
            P(KV, None, TP),
            P(KV, None, TP),
            P(KV, None, TP),
            P(KV, None, TP),
            P(KV, None, TP),
            P(),
            P(KV, TP),
            P(KV, TP),
            P(KV, TP),
            P(KV, TP),
            P(),
            P(TP),
            P(TP),
            P(TP),
            P(None, TP),
            P(None, TP),
            P(None, TP),
            P(TP),
            P(TP, KV),
        ),
        out_specs=(P(KV, None, TP), P(KV, TP, None, None)),
        check_vma=False,
    )
```

```python
import functools

import jax
import jax.numpy as jnp
from jax import lax
from jax.experimental import pallas as pl
from jax.experimental.pallas import tpu as pltpu
from jax.sharding import Mesh
from jax.sharding import PartitionSpec as P

NZ, NX, NY, NC = 8, 4, 4, 2
NT = NY * NC
MESH = pl.DeviceIdType.MESH
KV = ("z", "x")
TP = ("y", "c")
EPS = 1e-06
HIGH = lax.Precision.HIGHEST
F32 = jnp.float32
BF16 = jnp.bfloat16
NQ, NS, NP, NH = 12, 8, 6, 8
VMEM_LIMIT = 40 * 1024 * 1024


def wrap(i, n):
    return lax.rem(i + n, n)


def remote(src, dst, send_sem, recv_sem, device):
    return pltpu.make_async_remote_copy(
        src_ref=src,
        dst_ref=dst,
        send_sem=send_sem,
        recv_sem=recv_sem,
        device_id=device,
        device_id_type=MESH,
    )


def greet(devices):
    barrier = pltpu.get_barrier_semaphore()
    for device in devices:
        pl.semaphore_signal(barrier, inc=1, device_id=device, device_id_type=MESH)
    pl.semaphore_wait(barrier, len(devices))


def settle(view, sem):
    pltpu.make_async_copy(view, view, sem).wait()


def hops_of(piece, way):
    return 4 if (piece % 2 == 0) == (way == 0) else 3


def slot_of(piece, way, hop):
    return (0, 2, 4, 5)[hop - 1] if hops_of(piece, way) == 4 else (1, 3, 6)[hop - 1]


def sem_of(piece, way, hop):
    return hop - 1 if hop < hops_of(piece, way) else 3


def silu(v):
    return v * (1.0 / (1.0 + jnp.exp(-v)))


def softplus(v):
    return jnp.maximum(v, 0.0) + jnp.log1p(jnp.exp(-jnp.abs(v)))


def iota(shape, dim):
    return lax.broadcasted_iota(jnp.int32, shape, dim)


def dot(a, b):
    return jnp.dot(a.astype(BF16), b.astype(BF16), preferred_element_type=F32)


def dot_of(a, b, dims, precision=None):
    return lax.dot_general(
        a, b, ((dims[:1], dims[1:]), ((), ())), precision=precision, preferred_element_type=F32
    )


def past(first, last):
    return jnp.concatenate([first[...].astype(F32), last[...].astype(F32)], axis=0)


def widen(v):
    spread = (iota((NH, 512), 1) // 64 == iota((NH, 512), 0)).astype(F32)
    return dot_of(v, spread, (1, 0), HIGH)


def upright(row):
    wide = jnp.broadcast_to(row[...].astype(F32), (NS, NS))
    return jnp.sum(
        jnp.where(iota((NS, NS), 0) == iota((NS, NS), 1), wide, 0.0), axis=1, keepdims=True
    )


def mixer_kernel(
    tok_h,
    wx_h,
    wz_h,
    wb_h,
    wc_h,
    wdt_h,
    wo_h,
    state_h,
    gain,
    parents,
    accepted,
    cx,
    px,
    cb,
    pb,
    cc,
    pc,
    pdt,
    bias,
    alog,
    dskip,
    wtx,
    wtb,
    wtc,
    gain_out,
    mixed,
    new_state,
    tok,
    wown,
    wr,
    wo,
    held,
    fresh,
    tg,
    ts,
    wg,
    wog,
    prod,
    aprod,
    ring,
    aring,
    stage,
    astage,
    gated,
    gg,
    woc,
    kept,
    hold,
    given,
    taken,
    part,
    terms,
    l_s,
    s_s,
    t_s,
    t_r,
    f_r,
    w_s,
    w_r,
    r_s,
    a_s,
    r_r,
    o_s,
    o_r,
    g_s,
    g_r,
    d_s,
    d_r,
    p_s,
    p_r,
):
    z, x = lax.axis_index("z"), lax.axis_index("x")
    y, c = lax.axis_index("y"), lax.axis_index("c")
    t = y * NC + c
    count = NQ * NS

    def depth_of(owner):
        return pl.ds(pl.multiple_of(owner * 128, 128), 128)

    lower, upper = slice(0, 128), slice(128, 256)
    loads = [(tok_h, tok, 0), (wo_h, wo, 1)]
    loads.append(
        (
            wdt_h.at[
                pl.ds(pl.multiple_of(t * NH, NH), NH), pl.ds(pl.multiple_of(z * 512, 512), 512)
            ],
            wr,
            2,
        )
    )
    for g in range(2):
        wide, narrow = slice(256 * g, 256 * g + 256), slice(128 * g, 128 * g + 128)
        loads.append((wx_h.at[:, wide], wown.at[3 * g], 3 + g))
        loads.append((wb_h.at[:, narrow], wown.at[3 * g + 1, :, lower], 4))
        loads.append((wc_h.at[:, narrow], wown.at[3 * g + 1, :, upper], 4))
        loads.append((wz_h.at[:, wide], wown.at[3 * g + 2], 4))

    def load(k):
        return pltpu.make_async_copy(loads[k][0], loads[k][1], l_s.at[loads[k][2]])

    def load_state(s):
        return pltpu.make_async_copy(state_h.at[s], held.at[s], s_s.at[s // 4])

    for k in (3, 0, 1, 4, 5, 6, 2, 7, 8, 9, 10):
        load(k).start()
    for s in range(NS):
        load_state(s).start()
    plane = [(d, e) for d in range(NX) for e in range(NY) if d + e > 0]
    greet(
        [{"x": wrap(x + d, NX), "y": wrap(y + e, NY)} for d, e in plane]
        + [{"z": wrap(z + 1, NZ)}, {"z": wrap(z - 1, NZ)}, {"c": 1 - c}]
    )
    half = pl.ds(4 * c, 4)

    def tok_copy(d):
        to = wrap(x + d, NX)
        return remote(
            tok.at[:, half, to], tg.at[x, :, half], t_s, t_r.at[d - 1], {"x": to}
        )

    def tok_share(d):
        block = tg.at[wrap(x - d, NX), :, half]
        return remote(block, block, t_s, f_r.at[d - 1], {"c": 1 - c})

    def w_own(p, way):
        to = wrap(x + (1 if way == 0 else -1), NX)
        last = 0 if way == p % 2 else 1
        return remote(wown.at[p], wg.at[4 * p + x], w_s, w_r.at[p, last], {"x": to})

    def w_pass(p):
        sign = 1 if p % 2 == 0 else -1
        block = wg.at[4 * p + wrap(x - sign, NX)]
        return remote(block, block, w_s, w_r.at[p, 1], {"x": wrap(x + sign, NX)})

    def o_step(hop, side):
        for way in (0, 1):
            if hop == 4:
                side = way
            if hop == 4 or (hop > 1 and way == 0):
                settle(wog.at[0], o_r.at[2 * (hop - 2) + side])
            sign = 1 if way == 0 else -1
            owner = wrap(z - sign * (hop - 1), NZ)
            part = pl.ds(256 * side, 256)
            src = wo.at[part] if hop == 1 else wog.at[owner, part]
            to = {"z": wrap(z + sign, NZ)}
            at = 6 if hop == 4 else 2 * (hop - 1) + side
            sends.append(remote(src, wog.at[owner, part], o_s, o_r.at[at], to))
        for copy in sends[-2:]:
            copy.start()

    sends = []

    def r_copy(p, way, hop):
        to = {"z": wrap(z + (1 if way == 0 else -1), NZ)}
        buffer = aring if p == 6 else ring.at[p]
        dst = buffer.at[slot_of(p, way, hop)]
        if hop > 1:
            src = buffer.at[slot_of(p, way, hop - 1)]
        else:
            src = astage.at[way] if p == 6 else stage.at[p, way]
        return remote(src, dst, a_s if p == 6 else r_s, r_r.at[p, sem_of(p, way, hop)], to)

    def r_wait(p, index):
        buffer = aring if p == 6 else ring.at[p]
        first, many = ((0, 2), (2, 2), (4, 1), (5, 2))[index]
        settle(buffer.at[pl.ds(first, many)], r_r.at[p, index])

    def own_term(p, dest):
        if p == 6:
            return aprod[pl.ds(dest, 1)].reshape(16, count)
        return prod[p, :, pl.ds(dest, 1)].reshape(NQ, NS, 256)

    def r_step(p, hop):
        if hop > 1:
            r_wait(p, hop - 2)
        for way in (0, 1):
            hops = hops_of(p, way)
            if hop > hops:
                continue
            sign = 1 if way == 0 else -1
            term = own_term(p, wrap(z + sign * (hops + 1 - hop), NZ))
            if hop == 1:
                if p == 6:
                    astage[way] = term.astype(BF16)
                else:
                    stage[p, way] = term.astype(BF16)
            else:
                at = slot_of(p, way, hop - 1)
                if p == 6:
                    aring[at] = (aring[at].astype(F32) + term).astype(BF16)
                else:
                    ring[p, at] = (ring[p, at].astype(F32) + term).astype(BF16)
            r_copy(p, way, hop).start()

    def r_total(p):
        r_wait(p, 3)
        if p == 6:
            return own_term(p, z) + aring[5].astype(F32) + aring[6].astype(F32)
        total = own_term(p, z) + ring[p, 5].astype(F32) + ring[p, 6].astype(F32)
        return total.reshape(count, 256)

    order = (2, 1, 3)

    def w_send(p):
        w_own(p, p % 2).start()
        w_own(p, 1 - p % 2).start()

    load(3).wait()
    w_send(0)
    load(0).wait()
    for d in order:
        tok_copy(d).start()
    load(1).wait()
    o_step(1, 0)
    o_step(1, 1)

    up = jnp.concatenate([parents[:, q : q + 1] for q in range(NQ)], axis=0).astype(F32)
    taken_in = jnp.concatenate([upright(accepted)] * NQ, axis=0)
    seq = lax.rem(iota((count, 1), 0), NS).astype(F32)
    is_root = up < 0.0
    nodes = iota((count, 9 * NS + count), 1).astype(F32)

    def reach(back, other):
        return jnp.where(is_root, (taken_in + back) * NS + seq, other)

    at_kin = up * NS + seq
    kin = iota((count, count), 1).astype(F32)
    links = (kin == jnp.where(is_root, -1.0, at_kin)).astype(F32)
    eye = (iota((count, count), 0) == iota((count, count), 1)).astype(F32)
    family = eye + links
    for _ in range(4):
        family = jnp.minimum(dot(family, family), 1.0)
    is_kin = family > 0.5
    one = (nodes == reach(2.0, 9.0 * NS + at_kin)).astype(F32)
    two = dot(links, one) + (nodes == reach(1.0, -1.0)).astype(F32)
    three = dot(links, two) + (nodes == reach(0.0, -1.0)).astype(F32)
    one, two, three = one.astype(BF16), two.astype(BF16), three.astype(BF16)

    def window(history, taps):
        summed = taps[0:1] * history[0 : NP * NS]
        for k in (1, 2, 3):
            summed = summed + taps[k : k + 1] * history[k * NS : (k + NP) * NS]
        return silu(summed)

    rate = -jnp.exp(alog[...])
    path_xs = window(past(cx, px), wtx[...].astype(F32))
    path_bs = window(past(cb, pb), wtb[...].astype(F32))
    path_step = softplus(pdt[...].astype(F32) + bias[...])
    live = ((iota((NP * NS, 1), 0) // NS).astype(F32) < taken_in[0 : NP * NS]).astype(F32)
    path_log = path_step * rate * live
    tails = [jnp.zeros((NS, NH), F32)]
    for j in range(NP - 1, 0, -1):
        tails.insert(0, tails[0] + path_log[j * NS : (j + 1) * NS])
    overall = jnp.exp(tails[0] + path_log[0:NS])
    weights = live * jnp.exp(jnp.concatenate(tails, axis=0)) * path_step
    weighted = (path_xs * widen(weights)).astype(BF16)
    path_seq = lax.rem(iota((NP * NS, 128), 0), NS)

    def forward(p):
        settle(wg.at[0], w_r.at[p, 0])
        w_pass(p).start()

    forward(0)
    settle(wown.at[pl.ds(1, 5)], l_s.at[4])
    w_send(1)
    w_send(2)
    tg[pl.ds(x, 1)] = tok[:, :, pl.ds(x, 1)].reshape(1, NQ, NZ, NS, 128)
    for p in range(6):
        wg[pl.ds(4 * p + x, 1)] = wown[pl.ds(p, 1)]
    wog[pl.ds(z, 1)] = wo[...].reshape(1, 512, 128)
    load(2).wait()

    def rescale(d):
        xs = wrap(x - d, NX)
        values = tg[pl.ds(xs, 1)].reshape(NQ * NZ * NS, 128).astype(F32)
        scaled = (values * gain[pl.ds(z * NX + xs, 1), :]).astype(BF16)
        ts[:, :, :, depth_of(xs)] = scaled.reshape(NQ, NZ, NS, 128)
        return values * values

    squares = rescale(0)
    o_step(2, 0)

    gained = []
    for g in range(2):
        split_b = jnp.concatenate(
            [
                jnp.where(path_seq == s, path_bs[:, 128 * g : 128 * g + 128], 0.0)
                for s in range(NS)
            ],
            axis=1,
        ).astype(BF16)
        gained.append(dot_of(weighted[:, 256 * g : 256 * g + 256], split_b, (0, 0)))
    o_step(2, 1)
    for s in range(NS):
        if s % 4 == 0:
            settle(held.at[pl.ds(s, 4)], s_s.at[s // 4])
        at = slice(128 * s, 128 * s + 128)
        for g in range(2):
            wide = slice(256 * g, 256 * g + 256)
            fade = jnp.concatenate(
                [
                    jnp.broadcast_to(overall[s : s + 1, h : h + 1], (64, 128))
                    for h in range(4 * g, 4 * g + 4)
                ],
                axis=0,
            )
            now = fade * held[s, wide, :] + gained[g][:, at]
            new_state[s, wide, :] = now
            fresh[g, :, at] = now.astype(BF16)

    def tree_conv(history, own, taps):
        values = jnp.concatenate([history, own], axis=0).astype(BF16)
        summed = taps[3:4] * own
        for k, far in ((2, one), (1, two), (0, three)):
            summed = summed + taps[k : k + 1] * dot(far, values)
        return silu(summed)

    for d in order:
        settle(tg.at[0, :, half], t_r.at[d - 1])
        tok_share(d).start()

    def multiply(p):
        settle(wg.at[pl.ds(0, 2)], w_r.at[p, 1])
        prod[p] = jnp.dot(
            ts[...].reshape(NQ * NZ * NS, 512),
            wg[4 * p : 4 * p + 4].reshape(512, 256),
            preferred_element_type=F32,
        ).reshape(NQ, NZ, NS, 256)
        r_step(p, 1)

    for d in order:
        if d == 3:
            forward(1)
            w_send(3)
            o_step(3, 0)
        settle(tg.at[0, :, half], f_r.at[d - 1])
        squares = squares + rescale(d)
    multiply(0)
    o_step(3, 1)
    forward(2)
    w_send(4)
    multiply(1)
    forward(3)
    w_send(5)
    tall = jnp.concatenate([wr[...].astype(F32), jnp.zeros((8, 512), F32)], axis=0).astype(BF16)
    squares = squares.reshape(NQ, NZ, NS, 128)
    for dest in range(NZ):
        rates = dot_of(tall, ts[:, dest].reshape(count, 512), (1, 1))
        square = squares[:, dest].reshape(count, 128)
        above = square.astype(BF16)
        both = jnp.concatenate([above, (square - above.astype(F32)).astype(BF16)], axis=1)
        sums = dot_of(jnp.ones((16, 256), BF16), both, (1, 1))
        aprod[dest] = jnp.where(iota((16, count), 0) == NH, sums, rates)
    r_step(6, 1)
    r_step(0, 2)
    multiply(2)
    forward(4)
    r_step(1, 2)
    multiply(3)
    forward(5)
    o_step(4, 0)
    r_step(2, 2)
    r_step(6, 2)
    multiply(4)
    r_step(3, 2)
    multiply(5)
    r_step(6, 3)
    r_step(0, 3)
    r_step(4, 2)
    r_step(1, 3)
    r_step(5, 2)
    r_step(6, 4)
    r_step(2, 3)
    settle(wog.at[0], o_r.at[6])
    for k in range(NZ):
        at = 512 * (k % 2) + 128 * (k // 2)
        woc[:, at : at + 128] = wog[k]
    r_step(3, 3)
    r_step(4, 3)
    r_step(0, 4)
    r_step(5, 3)
    r_step(1, 4)
    r_step(2, 4)

    seq_of = lax.rem(iota((count, 128), 0), NS)
    side = iota((count, 128), 1)

    def scaled_rows(p):
        return (r_total(p) * scale).astype(BF16).astype(F32)

    def heads_of(g):
        wide, narrow = slice(256 * g, 256 * g + 256), slice(128 * g, 128 * g + 128)
        history = jnp.concatenate(
            [past(cx, px)[:, wide], past(cb, pb)[:, narrow], past(cc, pc)[:, narrow]], axis=1
        )
        taps = jnp.concatenate([wtx[:, wide], wtb[:, narrow], wtc[:, narrow]], axis=1)
        own = jnp.concatenate([scaled_rows(3 * g), scaled_rows(3 * g + 1)], axis=1)
        post = tree_conv(history, own, taps.astype(F32))
        post_b, post_c = post[:, 256:384].astype(BF16), post[:, 384:512].astype(BF16)
        post_x = post[:, 0:256].astype(BF16)
        split_c = jnp.concatenate(
            [jnp.where(seq_of == s, post_c.astype(F32), 0.0) for s in range(NS)], axis=1
        ).astype(BF16)
        carried = dot_of(split_c, fresh[g], (1, 1))
        scores = dot_of(post_c, post_b, (1, 1))
        within = []
        for pair in range(2):
            sides = []
            for h in (4 * g + 2 * pair, 4 * g + 2 * pair + 1):
                gap = decay[:, h : h + 1] - decay_t[h : h + 1, :]
                mixing = jnp.exp(jnp.where(is_kin, gap, 0.0)) * step_t[h : h + 1, :]
                mixing = jnp.where(is_kin, scores * mixing, 0.0)
                sides.append(dot(mixing, post_x[:, 128 * pair : 128 * pair + 128]))
            within.append(jnp.where(side < 64, sides[0], sides[1]))
        heads = carried * grown[:, wide] + jnp.concatenate(within, axis=1)
        return heads + skip[:, wide] * post[:, 0:256]

    def gate(g, heads):
        heads = heads * silu(scaled_rows(3 * g + 2))
        spread_of = jnp.sum(heads * heads, axis=1, keepdims=True) / 256.0
        heads = heads * lax.rsqrt(spread_of + EPS) * gain_out[:, 256 * g : 256 * g + 256]
        gated[g] = heads.astype(BF16)

    def g_copy(g, d):
        return remote(
            gated.at[g],
            gg.at[g, d - 1],
            g_s,
            g_r.at[0 if g == 0 else d],
            {"x": wrap(x + d, NX)},
        )

    def product(g, d, columns):
        values = gated[g] if d == 0 else gg[g, d - 1]
        return jnp.dot(
            values, woc[256 * g : 256 * g + 256, columns], preferred_element_type=F32
        )

    def d_copy(d):
        return remote(given.at[d], taken.at[d], d_s, d_r.at[d], {"c": 1 - c})

    def p_copy(d, e):
        to_y = wrap(y + e, NY)
        return remote(
            part.at[d, to_y],
            terms.at[x * NY + y],
            p_s,
            p_r,
            {"x": wrap(x - d, NX), "y": to_y},
        )

    mine = pl.ds(pl.multiple_of(512 * c, 512), 512)
    other = pl.ds(pl.multiple_of(512 * (1 - c), 512), 512)

    r_step(3, 4)
    r_step(4, 4)
    total = r_total(6)
    scale = lax.rsqrt(dot_of(eye, total, (1, 1), HIGH)[:, NH : NH + 1] / (NZ * NX * 128.0) + EPS)
    scale_t = lax.rsqrt(total[NH : NH + 1] / (NZ * NX * 128.0) + EPS)
    step_t = softplus((total[0:NH] * scale_t).astype(BF16).astype(F32) + upright(bias))
    slope_t = step_t * -jnp.exp(upright(alog))
    decay = dot_of(family, slope_t, (1, 1), HIGH)
    decay_t = dot_of(slope_t, family, (1, 1), HIGH)
    grown = widen(jnp.exp(decay))
    skip = widen(jnp.broadcast_to(dskip[...], (NS, NH)))[0:1]
    first = heads_of(0)
    r_step(5, 4)
    gate(0, first)
    for d in order:
        g_copy(0, d).start()
    gate(1, heads_of(1))
    for d in (1, 3, 2):
        g_copy(1, d).start()
    def begin(d):
        hold[d] = product(0, d, other)
        kept[d] = product(0, d, mine)

    def finish(d):
        if d > 0:
            settle(gg.at[1, d - 1], g_r.at[d])
        given[d] = (hold[d] + product(1, d, other)).astype(BF16)
        d_copy(d).start()
        kept[d] = kept[d] + product(1, d, mine)

    def deliver(d):
        settle(taken.at[d], d_r.at[d])
        both = (kept[d] + taken[d].astype(F32)).astype(BF16)
        for to in range(NY):
            part[d, to] = both[:, 128 * to : 128 * to + 128]
        for e in (2, 1, 3, 0):
            if d + e > 0:
                p_copy(d, e).start()

    begin(0)
    finish(0)
    settle(gg.at[0], g_r.at[0])
    for d in order:
        begin(d)
    deliver(0)
    terms[pl.ds(x * NY + y, 1)] = part[0, pl.ds(y, 1)]
    finish(1)
    finish(3)
    deliver(1)
    finish(2)
    deliver(3)
    deliver(2)
    settle(terms.at[pl.ds(0, 15)], p_r)
    for xs in range(NX):
        total = terms[xs * NY].astype(F32)
        for k in range(1, NY):
            total = total + terms[xs * NY + k].astype(F32)
        mixed[:, xs * 128 : (xs + 1) * 128] = total.astype(BF16)

    settle(wog.at[pl.ds(0, 7)], o_s)
    settle(tg.at[pl.ds(0, 3)], t_s)
    settle(wg.at[pl.ds(0, 18)], w_s)
    settle(ring, r_s)
    settle(aring, a_s)
    settle(gg, g_s)
    settle(given, d_s)
    settle(terms.at[pl.ds(0, 15)], p_s)


def mixer(*args):
    vmem = pl.BlockSpec(memory_space=pltpu.VMEM)
    far = pl.BlockSpec(memory_space=pltpu.HBM)
    dma = pltpu.SemaphoreType.DMA
    rows = NQ * NS
    return pl.pallas_call(
        mixer_kernel,
        name="mixer",
        out_shape=(
            jax.ShapeDtypeStruct((rows, 512), BF16),
            jax.ShapeDtypeStruct((NS, 512, 128), F32),
        ),
        in_specs=[far] * 8 + [vmem] * (len(args) - 8),
        out_specs=(vmem, vmem),
        scratch_shapes=[
            pltpu.VMEM((NQ, NZ, NX, NS, 128), BF16),
            pltpu.VMEM((6, 128, 256), BF16),
            pltpu.VMEM((NH, 512), BF16),
            pltpu.VMEM((512, 128), BF16),
            pltpu.VMEM((NS, 512, 128), F32),
            pltpu.VMEM((2, 256, 1024), BF16),
            pltpu.VMEM((NX, NQ, NZ, NS, 128), BF16),
            pltpu.VMEM((NQ, NZ, NS, 512), BF16),
            pltpu.VMEM((24, 128, 256), BF16),
            pltpu.VMEM((NZ, 512, 128), BF16),
            pltpu.VMEM((6, NQ, NZ, NS, 256), F32),
            pltpu.VMEM((NZ, 16, rows), F32),
            pltpu.VMEM((6, 7, NQ, NS, 256), BF16),
            pltpu.VMEM((7, 16, rows), BF16),
            pltpu.VMEM((6, 2, NQ, NS, 256), BF16),
            pltpu.VMEM((2, 16, rows), BF16),
            pltpu.VMEM((2, rows, 256), BF16),
            pltpu.VMEM((2, 3, rows, 256), BF16),
            pltpu.VMEM((512, 1024), BF16),
            pltpu.VMEM((NX, rows, 512), F32),
            pltpu.VMEM((NX, rows, 512), F32),
            pltpu.VMEM((NX, rows, 512), BF16),
            pltpu.VMEM((NX, rows, 512), BF16),
            pltpu.VMEM((NX, NY, rows, 128), BF16),
            pltpu.VMEM((NX * NY, rows, 128), BF16),
            dma((5,)),
            dma((2,)),
            dma,
            dma((3,)),
            dma((3,)),
            dma,
            dma((6, 2)),
            dma,
            dma,
            dma((7, 4)),
            dma,
            dma((7,)),
            dma,
            dma((4,)),
            dma,
            dma((NX,)),
            dma,
            dma,
        ],
        compiler_params=pltpu.CompilerParams(
            collective_id=0, has_side_effects=True, vmem_limit_bytes=VMEM_LIMIT
        ),
    )(*(pltpu.with_memory_space_constraint(a, pltpu.HBM) for a in args))


def finish_kernel(mixed, state, mixed_o, state_o, out_s):
    def save(k):
        if k == NS:
            return pltpu.make_async_copy(mixed, mixed_o, out_s.at[1])
        return pltpu.make_async_copy(state.at[k], state_o.at[k], out_s.at[0])

    for k in range(NS + 1):
        save(k).start()
    settle(state, out_s.at[0])
    save(NS).wait()


def finish(mixed, new_state):
    far = pl.BlockSpec(memory_space=pltpu.HBM)
    near = pl.BlockSpec(memory_space=pltpu.VMEM)
    return pl.pallas_call(
        finish_kernel,
        name="finish",
        out_shape=(
            jax.ShapeDtypeStruct(mixed.shape, mixed.dtype),
            jax.ShapeDtypeStruct(new_state.shape, new_state.dtype),
        ),
        in_specs=[near, near],
        out_specs=(far, far),
        scratch_shapes=[pltpu.SemaphoreType.DMA((2,))],
        compiler_params=pltpu.CompilerParams(vmem_limit_bytes=8 * 1024 * 1024),
    )(mixed, new_state)


def by_place(v):
    v = jnp.transpose(v, (1, 0, 2))
    return v.reshape(v.shape[0] * v.shape[1], v.shape[2])


def shards(
    tokens,
    parents,
    accepted,
    state,
    conv_x,
    conv_b,
    conv_c,
    path_x,
    path_b,
    path_c,
    path_dt,
    gain_in,
    w_x,
    w_z,
    w_b,
    w_c,
    w_dt,
    dt_bias,
    a_log,
    d_skip,
    conv_wx,
    conv_wb,
    conv_wc,
    gain_out,
    w_out,
):
    tok = jnp.transpose(tokens, (1, 0, 2)).reshape(NQ, NZ, NX, NS, 128)
    conv_x, path_x = by_place(conv_x), by_place(path_x)
    conv_b, path_b = by_place(conv_b), by_place(path_b)
    conv_c, path_c = by_place(conv_c), by_place(path_c)
    accepted, dt_bias, a_log = accepted[None, :], dt_bias[None, :], a_log[None, :]
    mixed, new_state = mixer(
        tok,
        w_x,
        w_z,
        w_b,
        w_c,
        w_dt.T,
        w_out,
        state.reshape(NS, 512, 128),
        gain_in.reshape(32, 128),
        parents,
        accepted,
        conv_x,
        path_x,
        conv_b,
        path_b,
        conv_c,
        path_c,
        by_place(path_dt),
        dt_bias,
        a_log,
        d_skip[None, :],
        conv_wx,
        conv_wb,
        conv_wc,
        gain_out[None, :],
    )
    mixed, new_state = finish(mixed, new_state)
    mixed = jnp.transpose(mixed.reshape(NQ, NS, 512), (1, 0, 2))
    return (mixed, new_state.reshape(NS, NH, 64, 128))


def solution(mesh):
    finer = Mesh(mesh.devices.reshape(NZ, NX, NY, NC), ("z", "x", "y", "c"))
    return jax.shard_map(
        shards,
        mesh=finer,
        in_specs=(
            P(None, None, KV),
            P(KV, None),
            P(KV),
            P(KV, TP, None, None),
            P(KV, None, TP),
            P(KV, None, TP),
            P(KV, None, TP),
            P(KV, None, TP),
            P(KV, None, TP),
            P(KV, None, TP),
            P(KV, None, TP),
            P(),
            P(KV, TP),
            P(KV, TP),
            P(KV, TP),
            P(KV, TP),
            P(),
            P(TP),
            P(TP),
            P(TP),
            P(None, TP),
            P(None, TP),
            P(None, TP),
            P(TP),
            P(TP, KV),
        ),
        out_specs=(P(KV, None, TP), P(KV, TP, None, None)),
        check_vma=False,
    )
```

```python
import functools

import jax
import jax.numpy as jnp
from jax import lax
from jax.experimental import pallas as pl
from jax.experimental.pallas import tpu as pltpu
from jax.sharding import Mesh
from jax.sharding import PartitionSpec as P

NZ, NX, NY, NC = 8, 4, 4, 2
NT = NY * NC
MESH = pl.DeviceIdType.MESH
KV = ("z", "x")
TP = ("y", "c")
EPS = 1e-06
HIGH = lax.Precision.HIGHEST
F32 = jnp.float32
BF16 = jnp.bfloat16
NQ, NS, NP, NH = 12, 8, 6, 8
VMEM_LIMIT = 40 * 1024 * 1024


def wrap(i, n):
    return lax.rem(i + n, n)


def remote(src, dst, send_sem, recv_sem, device):
    return pltpu.make_async_remote_copy(
        src_ref=src,
        dst_ref=dst,
        send_sem=send_sem,
        recv_sem=recv_sem,
        device_id=device,
        device_id_type=MESH,
    )


def greet(devices):
    barrier = pltpu.get_barrier_semaphore()
    for device in devices:
        pl.semaphore_signal(barrier, inc=1, device_id=device, device_id_type=MESH)
    pl.semaphore_wait(barrier, len(devices))


def settle(view, sem):
    pltpu.make_async_copy(view, view, sem).wait()


def hops_of(piece, way):
    return 4 if (piece % 2 == 0) == (way == 0) else 3


def slot_of(piece, way, hop):
    return (0, 2, 4, 5)[hop - 1] if hops_of(piece, way) == 4 else (1, 3, 6)[hop - 1]


def sem_of(piece, way, hop):
    return hop - 1 if hop < hops_of(piece, way) else 3


def silu(v):
    return v * (1.0 / (1.0 + jnp.exp(-v)))


def softplus(v):
    return jnp.maximum(v, 0.0) + jnp.log1p(jnp.exp(-jnp.abs(v)))


def iota(shape, dim):
    return lax.broadcasted_iota(jnp.int32, shape, dim)


def dot(a, b):
    return jnp.dot(a.astype(BF16), b.astype(BF16), preferred_element_type=F32)


def dot_of(a, b, dims, precision=None):
    return lax.dot_general(
        a, b, ((dims[:1], dims[1:]), ((), ())), precision=precision, preferred_element_type=F32
    )


def past(first, last):
    return jnp.concatenate([first[...].astype(F32), last[...].astype(F32)], axis=0)


def widen(v):
    spread = (iota((NH, 512), 1) // 64 == iota((NH, 512), 0)).astype(F32)
    return dot_of(v, spread, (1, 0), HIGH)


def upright(row):
    wide = jnp.broadcast_to(row[...].astype(F32), (NS, NS))
    return jnp.sum(
        jnp.where(iota((NS, NS), 0) == iota((NS, NS), 1), wide, 0.0), axis=1, keepdims=True
    )


def mixer_kernel(
    fetches,
    tok_h,
    wx_h,
    wz_h,
    wb_h,
    wc_h,
    wdt_h,
    wo_h,
    state_h,
    gain,
    parents,
    accepted,
    cx,
    px,
    cb,
    pb,
    cc,
    pc,
    pdt,
    bias,
    alog,
    dskip,
    wtx,
    wtb,
    wtc,
    gain_out,
    mixed,
    new_state,
    tok,
    wown,
    wr,
    wo,
    held,
    fresh,
    tg,
    ts,
    wg,
    wog,
    prod,
    aprod,
    ring,
    aring,
    stage,
    astage,
    gated,
    gg,
    woc,
    kept,
    hold,
    given,
    taken,
    part,
    terms,
    l_s,
    s_s,
    t_s,
    t_r,
    f_r,
    w_s,
    w_r,
    r_s,
    a_s,
    r_r,
    o_s,
    o_r,
    g_s,
    g_r,
    d_s,
    d_r,
    p_s,
    p_r,
):
    z, x = lax.axis_index("z"), lax.axis_index("x")
    y, c = lax.axis_index("y"), lax.axis_index("c")
    t = y * NC + c
    count = NQ * NS

    def depth_of(owner):
        return pl.ds(pl.multiple_of(owner * 128, 128), 128)

    lower, upper = slice(0, 128), slice(128, 256)
    loads = [(tok_h, tok, 0), (wo_h, wo, 1)]
    loads.append(
        (
            wdt_h.at[
                pl.ds(pl.multiple_of(t * NH, NH), NH), pl.ds(pl.multiple_of(z * 512, 512), 512)
            ],
            wr,
            2,
        )
    )
    for g in range(2):
        wide, narrow = slice(256 * g, 256 * g + 256), slice(128 * g, 128 * g + 128)
        loads.append((wx_h.at[:, wide], wown.at[3 * g], 3 + g))
        loads.append((wb_h.at[:, narrow], wown.at[3 * g + 1, :, lower], 4))
        loads.append((wc_h.at[:, narrow], wown.at[3 * g + 1, :, upper], 4))
        loads.append((wz_h.at[:, wide], wown.at[3 * g + 2], 4))

    def load(k):
        return pltpu.make_async_copy(loads[k][0], loads[k][1], l_s.at[loads[k][2]])

    def load_state(s):
        return pltpu.make_async_copy(state_h.at[s], held.at[s], s_s.at[s // 4])

    for k in (3, 0, 1, 4, 5, 6, 2, 7, 8, 9, 10):
        load(k).start()
    for fetch in fetches:
        fetch.start()
    for s in range(NS):
        load_state(s).start()
    plane = [(d, e) for d in range(NX) for e in range(NY) if d + e > 0]
    greet(
        [{"x": wrap(x + d, NX), "y": wrap(y + e, NY)} for d, e in plane]
        + [{"z": wrap(z + 1, NZ)}, {"z": wrap(z - 1, NZ)}, {"c": 1 - c}]
    )
    for fetch in fetches:
        fetch.wait()
    half = pl.ds(4 * c, 4)

    def tok_copy(d):
        to = wrap(x + d, NX)
        return remote(
            tok.at[:, half, to], tg.at[x, :, half], t_s, t_r.at[d - 1], {"x": to}
        )

    def tok_share(d):
        block = tg.at[wrap(x - d, NX), :, half]
        return remote(block, block, t_s, f_r.at[d - 1], {"c": 1 - c})

    def w_own(p, way):
        to = wrap(x + (1 if way == 0 else -1), NX)
        last = 0 if way == p % 2 else 1
        return remote(wown.at[p], wg.at[4 * p + x], w_s, w_r.at[p, last], {"x": to})

    def w_pass(p):
        sign = 1 if p % 2 == 0 else -1
        block = wg.at[4 * p + wrap(x - sign, NX)]
        return remote(block, block, w_s, w_r.at[p, 1], {"x": wrap(x + sign, NX)})

    def o_step(hop, side):
        for way in (0, 1):
            if hop == 4:
                side = way
            if hop == 4 or (hop > 1 and way == 0):
                settle(wog.at[0], o_r.at[2 * (hop - 2) + side])
            sign = 1 if way == 0 else -1
            owner = wrap(z - sign * (hop - 1), NZ)
            part = pl.ds(256 * side, 256)
            src = wo.at[part] if hop == 1 else wog.at[owner, part]
            to = {"z": wrap(z + sign, NZ)}
            at = 6 if hop == 4 else 2 * (hop - 1) + side
            sends.append(remote(src, wog.at[owner, part], o_s, o_r.at[at], to))
        for copy in sends[-2:]:
            copy.start()

    sends = []

    def r_copy(p, way, hop):
        to = {"z": wrap(z + (1 if way == 0 else -1), NZ)}
        buffer = aring if p == 6 else ring.at[p]
        dst = buffer.at[slot_of(p, way, hop)]
        if hop > 1:
            src = buffer.at[slot_of(p, way, hop - 1)]
        else:
            src = astage.at[way] if p == 6 else stage.at[p, way]
        return remote(src, dst, a_s if p == 6 else r_s, r_r.at[p, sem_of(p, way, hop)], to)

    def r_wait(p, index):
        buffer = aring if p == 6 else ring.at[p]
        first, many = ((0, 2), (2, 2), (4, 1), (5, 2))[index]
        settle(buffer.at[pl.ds(first, many)], r_r.at[p, index])

    def own_term(p, dest):
        if p == 6:
            return aprod[pl.ds(dest, 1)].reshape(16, count)
        return prod[p, :, pl.ds(dest, 1)].reshape(NQ, NS, 256)

    def r_step(p, hop):
        if hop > 1:
            r_wait(p, hop - 2)
        for way in (0, 1):
            hops = hops_of(p, way)
            if hop > hops:
                continue
            sign = 1 if way == 0 else -1
            term = own_term(p, wrap(z + sign * (hops + 1 - hop), NZ))
            if hop == 1:
                if p == 6:
                    astage[way] = term.astype(BF16)
                else:
                    stage[p, way] = term.astype(BF16)
            else:
                at = slot_of(p, way, hop - 1)
                if p == 6:
                    aring[at] = (aring[at].astype(F32) + term).astype(BF16)
                else:
                    ring[p, at] = (ring[p, at].astype(F32) + term).astype(BF16)
            r_copy(p, way, hop).start()

    def r_total(p):
        r_wait(p, 3)
        if p == 6:
            return own_term(p, z) + aring[5].astype(F32) + aring[6].astype(F32)
        total = own_term(p, z) + ring[p, 5].astype(F32) + ring[p, 6].astype(F32)
        return total.reshape(count, 256)

    order = (2, 1, 3)

    def w_send(p):
        w_own(p, p % 2).start()
        w_own(p, 1 - p % 2).start()

    load(3).wait()
    w_send(0)
    load(0).wait()
    for d in order:
        tok_copy(d).start()
    load(1).wait()
    o_step(1, 0)
    o_step(1, 1)

    up = jnp.concatenate([parents[:, q : q + 1] for q in range(NQ)], axis=0).astype(F32)
    taken_in = jnp.concatenate([upright(accepted)] * NQ, axis=0)
    seq = lax.rem(iota((count, 1), 0), NS).astype(F32)
    is_root = up < 0.0
    nodes = iota((count, 9 * NS + count), 1).astype(F32)

    def reach(back, other):
        return jnp.where(is_root, (taken_in + back) * NS + seq, other)

    at_kin = up * NS + seq
    kin = iota((count, count), 1).astype(F32)
    links = (kin == jnp.where(is_root, -1.0, at_kin)).astype(F32)
    eye = (iota((count, count), 0) == iota((count, count), 1)).astype(F32)
    family = eye + links
    for _ in range(4):
        family = jnp.minimum(dot(family, family), 1.0)
    is_kin = family > 0.5
    one = (nodes == reach(2.0, 9.0 * NS + at_kin)).astype(F32)
    two = dot(links, one) + (nodes == reach(1.0, -1.0)).astype(F32)
    three = dot(links, two) + (nodes == reach(0.0, -1.0)).astype(F32)
    one, two, three = one.astype(BF16), two.astype(BF16), three.astype(BF16)

    def window(history, taps):
        summed = taps[0:1] * history[0 : NP * NS]
        for k in (1, 2, 3):
            summed = summed + taps[k : k + 1] * history[k * NS : (k + NP) * NS]
        return silu(summed)

    rate = -jnp.exp(alog[...])
    path_xs = window(past(cx, px), wtx[...].astype(F32))
    path_bs = window(past(cb, pb), wtb[...].astype(F32))
    path_step = softplus(pdt[...].astype(F32) + bias[...])
    live = ((iota((NP * NS, 1), 0) // NS).astype(F32) < taken_in[0 : NP * NS]).astype(F32)
    path_log = path_step * rate * live
    tails = [jnp.zeros((NS, NH), F32)]
    for j in range(NP - 1, 0, -1):
        tails.insert(0, tails[0] + path_log[j * NS : (j + 1) * NS])
    overall = jnp.exp(tails[0] + path_log[0:NS])
    weights = live * jnp.exp(jnp.concatenate(tails, axis=0)) * path_step
    weighted = (path_xs * widen(weights)).astype(BF16)
    path_seq = lax.rem(iota((NP * NS, 128), 0), NS)

    def forward(p):
        settle(wg.at[0], w_r.at[p, 0])
        w_pass(p).start()

    forward(0)
    settle(wown.at[pl.ds(1, 5)], l_s.at[4])
    w_send(1)
    w_send(2)
    tg[pl.ds(x, 1)] = tok[:, :, pl.ds(x, 1)].reshape(1, NQ, NZ, NS, 128)
    for p in range(6):
        wg[pl.ds(4 * p + x, 1)] = wown[pl.ds(p, 1)]
    wog[pl.ds(z, 1)] = wo[...].reshape(1, 512, 128)
    load(2).wait()

    def rescale(d):
        xs = wrap(x - d, NX)
        values = tg[pl.ds(xs, 1)].reshape(NQ * NZ * NS, 128).astype(F32)
        scaled = (values * gain[pl.ds(z * NX + xs, 1), :]).astype(BF16)
        ts[:, :, :, depth_of(xs)] = scaled.reshape(NQ, NZ, NS, 128)
        return values * values

    squares = rescale(0)
    o_step(2, 0)

    gained = []
    for g in range(2):
        split_b = jnp.concatenate(
            [
                jnp.where(path_seq == s, path_bs[:, 128 * g : 128 * g + 128], 0.0)
                for s in range(NS)
            ],
            axis=1,
        ).astype(BF16)
        gained.append(dot_of(weighted[:, 256 * g : 256 * g + 256], split_b, (0, 0)))
    o_step(2, 1)
    for s in range(NS):
        if s % 4 == 0:
            settle(held.at[pl.ds(s, 4)], s_s.at[s // 4])
        at = slice(128 * s, 128 * s + 128)
        for g in range(2):
            wide = slice(256 * g, 256 * g + 256)
            fade = jnp.concatenate(
                [
                    jnp.broadcast_to(overall[s : s + 1, h : h + 1], (64, 128))
                    for h in range(4 * g, 4 * g + 4)
                ],
                axis=0,
            )
            now = fade * held[s, wide, :] + gained[g][:, at]
            new_state[s, wide, :] = now
            fresh[g, :, at] = now.astype(BF16)

    def tree_conv(history, own, taps):
        values = jnp.concatenate([history, own], axis=0).astype(BF16)
        summed = taps[3:4] * own
        for k, far in ((2, one), (1, two), (0, three)):
            summed = summed + taps[k : k + 1] * dot(far, values)
        return silu(summed)

    for d in order:
        settle(tg.at[0, :, half], t_r.at[d - 1])
        tok_share(d).start()

    def multiply(p):
        settle(wg.at[pl.ds(0, 2)], w_r.at[p, 1])
        prod[p] = jnp.dot(
            ts[...].reshape(NQ * NZ * NS, 512),
            wg[4 * p : 4 * p + 4].reshape(512, 256),
            preferred_element_type=F32,
        ).reshape(NQ, NZ, NS, 256)
        r_step(p, 1)

    for d in order:
        if d == 3:
            forward(1)
            w_send(3)
            o_step(3, 0)
        settle(tg.at[0, :, half], f_r.at[d - 1])
        squares = squares + rescale(d)
    multiply(0)
    o_step(3, 1)
    forward(2)
    w_send(4)
    multiply(1)
    forward(3)
    w_send(5)
    tall = jnp.concatenate([wr[...].astype(F32), jnp.zeros((8, 512), F32)], axis=0).astype(BF16)
    squares = squares.reshape(NQ, NZ, NS, 128)
    for dest in range(NZ):
        rates = dot_of(tall, ts[:, dest].reshape(count, 512), (1, 1))
        square = squares[:, dest].reshape(count, 128)
        above = square.astype(BF16)
        both = jnp.concatenate([above, (square - above.astype(F32)).astype(BF16)], axis=1)
        sums = dot_of(jnp.ones((16, 256), BF16), both, (1, 1))
        aprod[dest] = jnp.where(iota((16, count), 0) == NH, sums, rates)
    r_step(6, 1)
    r_step(0, 2)
    multiply(2)
    forward(4)
    r_step(1, 2)
    multiply(3)
    forward(5)
    o_step(4, 0)
    r_step(2, 2)
    r_step(6, 2)
    multiply(4)
    r_step(3, 2)
    multiply(5)
    r_step(6, 3)
    r_step(0, 3)
    r_step(4, 2)
    r_step(1, 3)
    r_step(5, 2)
    r_step(6, 4)
    r_step(2, 3)
    settle(wog.at[0], o_r.at[6])
    for k in range(NZ):
        at = 512 * (k % 2) + 128 * (k // 2)
        woc[:, at : at + 128] = wog[k]
    r_step(3, 3)
    r_step(4, 3)
    r_step(0, 4)
    r_step(5, 3)
    r_step(1, 4)
    r_step(2, 4)

    seq_of = lax.rem(iota((count, 128), 0), NS)
    side = iota((count, 128), 1)

    def scaled_rows(p):
        return (r_total(p) * scale).astype(BF16).astype(F32)

    def heads_of(g):
        wide, narrow = slice(256 * g, 256 * g + 256), slice(128 * g, 128 * g + 128)
        history = jnp.concatenate(
            [past(cx, px)[:, wide], past(cb, pb)[:, narrow], past(cc, pc)[:, narrow]], axis=1
        )
        taps = jnp.concatenate([wtx[:, wide], wtb[:, narrow], wtc[:, narrow]], axis=1)
        own = jnp.concatenate([scaled_rows(3 * g), scaled_rows(3 * g + 1)], axis=1)
        post = tree_conv(history, own, taps.astype(F32))
        post_b, post_c = post[:, 256:384].astype(BF16), post[:, 384:512].astype(BF16)
        post_x = post[:, 0:256].astype(BF16)
        split_c = jnp.concatenate(
            [jnp.where(seq_of == s, post_c.astype(F32), 0.0) for s in range(NS)], axis=1
        ).astype(BF16)
        carried = dot_of(split_c, fresh[g], (1, 1))
        scores = dot_of(post_c, post_b, (1, 1))
        within = []
        for pair in range(2):
            sides = []
            for h in (4 * g + 2 * pair, 4 * g + 2 * pair + 1):
                gap = decay[:, h : h + 1] - decay_t[h : h + 1, :]
                mixing = jnp.exp(jnp.where(is_kin, gap, 0.0)) * step_t[h : h + 1, :]
                mixing = jnp.where(is_kin, scores * mixing, 0.0)
                sides.append(dot(mixing, post_x[:, 128 * pair : 128 * pair + 128]))
            within.append(jnp.where(side < 64, sides[0], sides[1]))
        heads = carried * grown[:, wide] + jnp.concatenate(within, axis=1)
        return heads + skip[:, wide] * post[:, 0:256]

    def gate(g, heads):
        heads = heads * silu(scaled_rows(3 * g + 2))
        spread_of = jnp.sum(heads * heads, axis=1, keepdims=True) / 256.0
        heads = heads * lax.rsqrt(spread_of + EPS) * gain_out[:, 256 * g : 256 * g + 256]
        gated[g] = heads.astype(BF16)

    def g_copy(g, d):
        return remote(
            gated.at[g],
            gg.at[g, d - 1],
            g_s,
            g_r.at[0 if g == 0 else d],
            {"x": wrap(x + d, NX)},
        )

    def product(g, d, columns):
        values = gated[g] if d == 0 else gg[g, d - 1]
        return jnp.dot(
            values, woc[256 * g : 256 * g + 256, columns], preferred_element_type=F32
        )

    def d_copy(d):
        return remote(given.at[d], taken.at[d], d_s, d_r.at[d], {"c": 1 - c})

    def p_copy(d, e):
        to_y = wrap(y + e, NY)
        return remote(
            part.at[d, to_y],
            terms.at[x * NY + y],
            p_s,
            p_r,
            {"x": wrap(x - d, NX), "y": to_y},
        )

    mine = pl.ds(pl.multiple_of(512 * c, 512), 512)
    other = pl.ds(pl.multiple_of(512 * (1 - c), 512), 512)

    r_step(3, 4)
    r_step(4, 4)
    total = r_total(6)
    scale = lax.rsqrt(dot_of(eye, total, (1, 1), HIGH)[:, NH : NH + 1] / (NZ * NX * 128.0) + EPS)
    scale_t = lax.rsqrt(total[NH : NH + 1] / (NZ * NX * 128.0) + EPS)
    step_t = softplus((total[0:NH] * scale_t).astype(BF16).astype(F32) + upright(bias))
    slope_t = step_t * -jnp.exp(upright(alog))
    decay = dot_of(family, slope_t, (1, 1), HIGH)
    decay_t = dot_of(slope_t, family, (1, 1), HIGH)
    grown = widen(jnp.exp(decay))
    skip = widen(jnp.broadcast_to(dskip[...], (NS, NH)))[0:1]
    first = heads_of(0)
    r_step(5, 4)
    gate(0, first)
    for d in order:
        g_copy(0, d).start()
    gate(1, heads_of(1))
    for d in (1, 3, 2):
        g_copy(1, d).start()
    def begin(d):
        hold[d] = product(0, d, other)
        kept[d] = product(0, d, mine)

    def finish(d):
        if d > 0:
            settle(gg.at[1, d - 1], g_r.at[d])
        given[d] = (hold[d] + product(1, d, other)).astype(BF16)
        d_copy(d).start()
        kept[d] = kept[d] + product(1, d, mine)

    def deliver(d):
        settle(taken.at[d], d_r.at[d])
        both = (kept[d] + taken[d].astype(F32)).astype(BF16)
        for to in range(NY):
            part[d, to] = both[:, 128 * to : 128 * to + 128]
        for e in (2, 1, 3, 0):
            if d + e > 0:
                p_copy(d, e).start()

    begin(0)
    finish(0)
    settle(gg.at[0], g_r.at[0])
    for d in order:
        begin(d)
    deliver(0)
    terms[pl.ds(x * NY + y, 1)] = part[0, pl.ds(y, 1)]
    finish(1)
    finish(3)
    deliver(1)
    deliver(3)
    finish(2)
    deliver(2)
    settle(terms.at[pl.ds(0, 15)], p_r)
    for xs in range(NX):
        total = terms[xs * NY].astype(F32)
        for k in range(1, NY):
            total = total + terms[xs * NY + k].astype(F32)
        mixed[:, xs * 128 : (xs + 1) * 128] = total.astype(BF16)

    settle(wog.at[pl.ds(0, 7)], o_s)
    settle(tg.at[pl.ds(0, 3)], t_s)
    settle(wg.at[pl.ds(0, 18)], w_s)
    settle(ring, r_s)
    settle(aring, a_s)
    settle(gg, g_s)
    settle(given, d_s)
    settle(terms.at[pl.ds(0, 15)], p_s)


def mixer(*args):
    vmem = pl.BlockSpec(memory_space=pltpu.VMEM)
    far = pl.BlockSpec(memory_space=pltpu.HBM)
    dma = pltpu.SemaphoreType.DMA
    small = args[8:]

    def entry(*refs):
        far_refs, rest = refs[8 : len(args)], refs[len(args) :]
        near_refs, near_s = rest[-len(small) - 1 : -1], rest[-1]
        fetches = [
            pltpu.make_async_copy(f, n, near_s.at[k])
            for k, (f, n) in enumerate(zip(far_refs, near_refs))
        ]
        mixer_kernel(fetches, *refs[:8], *near_refs, *rest[: -len(small) - 1])

    rows = NQ * NS
    return pl.pallas_call(
        entry,
        name="mixer",
        out_shape=(
            jax.ShapeDtypeStruct((rows, 512), BF16),
            jax.ShapeDtypeStruct((NS, 512, 128), F32),
        ),
        in_specs=[far] * len(args),
        out_specs=(vmem, vmem),
        scratch_shapes=[
            pltpu.VMEM((NQ, NZ, NX, NS, 128), BF16),
            pltpu.VMEM((6, 128, 256), BF16),
            pltpu.VMEM((NH, 512), BF16),
            pltpu.VMEM((512, 128), BF16),
            pltpu.VMEM((NS, 512, 128), F32),
            pltpu.VMEM((2, 256, 1024), BF16),
            pltpu.VMEM((NX, NQ, NZ, NS, 128), BF16),
            pltpu.VMEM((NQ, NZ, NS, 512), BF16),
            pltpu.VMEM((24, 128, 256), BF16),
            pltpu.VMEM((NZ, 512, 128), BF16),
            pltpu.VMEM((6, NQ, NZ, NS, 256), F32),
            pltpu.VMEM((NZ, 16, rows), F32),
            pltpu.VMEM((6, 7, NQ, NS, 256), BF16),
            pltpu.VMEM((7, 16, rows), BF16),
            pltpu.VMEM((6, 2, NQ, NS, 256), BF16),
            pltpu.VMEM((2, 16, rows), BF16),
            pltpu.VMEM((2, rows, 256), BF16),
            pltpu.VMEM((2, 3, rows, 256), BF16),
            pltpu.VMEM((512, 1024), BF16),
            pltpu.VMEM((NX, rows, 512), F32),
            pltpu.VMEM((NX, rows, 512), F32),
            pltpu.VMEM((NX, rows, 512), BF16),
            pltpu.VMEM((NX, rows, 512), BF16),
            pltpu.VMEM((NX, NY, rows, 128), BF16),
            pltpu.VMEM((NX * NY, rows, 128), BF16),
            dma((5,)),
            dma((2,)),
            dma,
            dma((3,)),
            dma((3,)),
            dma,
            dma((6, 2)),
            dma,
            dma,
            dma((7, 4)),
            dma,
            dma((7,)),
            dma,
            dma((4,)),
            dma,
            dma((NX,)),
            dma,
            dma,
            *[pltpu.VMEM(a.shape, a.dtype) for a in small],
            dma((len(small),)),
        ],
        compiler_params=pltpu.CompilerParams(
            collective_id=0, has_side_effects=True, vmem_limit_bytes=VMEM_LIMIT
        ),
    )(*(pltpu.with_memory_space_constraint(a, pltpu.HBM) for a in args))


def finish_kernel(mixed, state, mixed_o, state_o, out_s):
    def save(k):
        if k == NS:
            return pltpu.make_async_copy(mixed, mixed_o, out_s.at[1])
        return pltpu.make_async_copy(state.at[k], state_o.at[k], out_s.at[0])

    for k in range(NS + 1):
        save(k).start()
    settle(state, out_s.at[0])
    save(NS).wait()


def finish(mixed, new_state):
    far = pl.BlockSpec(memory_space=pltpu.HBM)
    near = pl.BlockSpec(memory_space=pltpu.VMEM)
    return pl.pallas_call(
        finish_kernel,
        name="finish",
        out_shape=(
            jax.ShapeDtypeStruct(mixed.shape, mixed.dtype),
            jax.ShapeDtypeStruct(new_state.shape, new_state.dtype),
        ),
        in_specs=[near, near],
        out_specs=(far, far),
        scratch_shapes=[pltpu.SemaphoreType.DMA((2,))],
        compiler_params=pltpu.CompilerParams(vmem_limit_bytes=8 * 1024 * 1024),
    )(mixed, new_state)


def by_place(v):
    v = jnp.transpose(v, (1, 0, 2))
    return v.reshape(v.shape[0] * v.shape[1], v.shape[2])


def shards(
    tokens,
    parents,
    accepted,
    state,
    conv_x,
    conv_b,
    conv_c,
    path_x,
    path_b,
    path_c,
    path_dt,
    gain_in,
    w_x,
    w_z,
    w_b,
    w_c,
    w_dt,
    dt_bias,
    a_log,
    d_skip,
    conv_wx,
    conv_wb,
    conv_wc,
    gain_out,
    w_out,
):
    tok = jnp.transpose(tokens, (1, 0, 2)).reshape(NQ, NZ, NX, NS, 128)
    conv_x, path_x = by_place(conv_x), by_place(path_x)
    conv_b, path_b = by_place(conv_b), by_place(path_b)
    conv_c, path_c = by_place(conv_c), by_place(path_c)
    accepted, dt_bias, a_log = accepted[None, :], dt_bias[None, :], a_log[None, :]
    mixed, new_state = mixer(
        tok,
        w_x,
        w_z,
        w_b,
        w_c,
        w_dt.T,
        w_out,
        state.reshape(NS, 512, 128),
        gain_in.reshape(32, 128),
        parents,
        accepted,
        conv_x,
        path_x,
        conv_b,
        path_b,
        conv_c,
        path_c,
        by_place(path_dt),
        dt_bias,
        a_log,
        d_skip[None, :],
        conv_wx,
        conv_wb,
        conv_wc,
        gain_out[None, :],
    )
    mixed, new_state = finish(mixed, new_state)
    mixed = jnp.transpose(mixed.reshape(NQ, NS, 512), (1, 0, 2))
    return (mixed, new_state.reshape(NS, NH, 64, 128))


def solution(mesh):
    finer = Mesh(mesh.devices.reshape(NZ, NX, NY, NC), ("z", "x", "y", "c"))
    return jax.shard_map(
        shards,
        mesh=finer,
        in_specs=(
            P(None, None, KV),
            P(KV, None),
            P(KV),
            P(KV, TP, None, None),
            P(KV, None, TP),
            P(KV, None, TP),
            P(KV, None, TP),
            P(KV, None, TP),
            P(KV, None, TP),
            P(KV, None, TP),
            P(KV, None, TP),
            P(),
            P(KV, TP),
            P(KV, TP),
            P(KV, TP),
            P(KV, TP),
            P(),
            P(TP),
            P(TP),
            P(TP),
            P(None, TP),
            P(None, TP),
            P(None, TP),
            P(TP),
            P(TP, KV),
        ),
        out_specs=(P(KV, None, TP), P(KV, TP, None, None)),
        check_vma=False,
    )
```
